256 devices in a mesh: sp: 16 (over y, x), tp: 16 (over z, core).
Axes of the slice: x: 4, y: 4, z: 8, core: 2. Of those that a mesh axis runs over, the one named last changes fastest.
Arguments:
- queries: bfloat16 [8192, 2048], P('sp', 'tp'), may hold values from -16 to 16
- key_vectors: bfloat16 [8192, 2048], P('sp', 'tp'), may hold values from -4 to 4
- value_vectors: bfloat16 [8192, 2048], P('sp', 'tp'), may hold values from -5 to 5
- forget_totals: float32 [8192, 16], P('sp', 'tp'), may hold values from -1368 to 0, as said below
- head_gain: float32 [2048], P('tp'), may hold values from 0.1 to 1.9
- stream: bfloat16 [8192, 2048], P(('sp', 'tp')), may hold values from -6 to 6
- out_weight: bfloat16 [2048, 2048], replicated, may hold values from -0.125 to 0.125
- norm_gain: float32 [2048], replicated, may hold values from 0.1 to 1.9
- routing: int32 [8192, 2], P(('sp', 'tp')), may hold values from 0 to 15, all different within a row; in each aligned block of 32 rows (0 to 31, 32 to 63, ...) at most 8 rows name the same one
- route_weights: float32 [8192, 2], P(('sp', 'tp')), may hold values from 0.2 to 1
- gate_weight: bfloat16 [16, 2048, 4096], P('sp', None, 'tp'), may hold values from -0.125 to 0.125
- up_weight: bfloat16 [16, 2048, 4096], P('sp', None, 'tp'), may hold values from -0.125 to 0.125
- down_weight: bfloat16 [16, 4096, 2048], P('sp', 'tp'), may hold values from -0.09375 to 0.09375
Outputs:
- layer_out: bfloat16 [8192, 2048], P(('sp', 'tp'))
The draws below stay inside these ranges and needn't reach their ends.
Inputs may be any that keep to these rules, and one draw needn't show every extreme that they name: `forget_totals`: along the positions, the values of each head never rise. `routing`: A token's 2 experts differ. Within the tokens of one device (aligned blocks of 32 rows) no expert is named more than 8 times.
All inputs are finite; a program needn't handle non-finite values.
Results may differ from the reference program's by a relative error of at most 0.01145.
Values may be sent and summed in bfloat16 or wider, within the bound.
No kernel may reach another device: no remote copies, remote signals or barrier semaphores. Data moves between devices by JAX's collectives and lax.ppermute only.
A program may use at most 128 MiB of HBM per device.

```python
import math
import jax
import jax.numpy as jnp
import numpy as np
from jax import lax

D = 2048
HEAD_COUNT = 16
HD = 128
FF_E = 4096
TOP = 2
TOK_DEV = 512
SEQUENCE_TOKENS = 8192
EXPERTS = 16
ROWS_DEV = 32
CAP = 8
N_TP = 16


def draw_queries(key, part):
    own_key = jax.random.fold_in(key, 11)
    entries = jnp.clip(jax.random.normal(own_key, (SEQUENCE_TOKENS, HEAD_COUNT * HD), jnp.float32), -4.0, 4.0)
    return entries.astype(jnp.bfloat16)


def draw_key_vectors(key, part):
    own_key = jax.random.fold_in(key, 13)
    entries = jnp.clip(jax.random.normal(own_key, (SEQUENCE_TOKENS, HEAD_COUNT * HD), jnp.float32), -4.0, 4.0)
    return entries.astype(jnp.bfloat16)


def draw_forget_totals(key, part):
    ranking = jax.random.permutation(jax.random.fold_in(key, 21), HEAD_COUNT)
    slow_heads = ranking < HEAD_COUNT // 2
    slow_rate = jax.random.uniform(jax.random.fold_in(key, 22), (HEAD_COUNT,), jnp.float32, 0.3, 0.8) / SEQUENCE_TOKENS
    fast_rate = jnp.exp(-jax.random.uniform(jax.random.fold_in(key, 23), (HEAD_COUNT,), jnp.float32, math.log(30.0), math.log(100.0)))
    head_rate = jnp.where(slow_heads, slow_rate, fast_rate)
    block_factor = jnp.exp(jax.random.uniform(jax.random.fold_in(key, 24), (SEQUENCE_TOKENS // TOK_DEV, HEAD_COUNT), jnp.float32, math.log(0.5), math.log(1.5)))
    block_factor = jnp.repeat(block_factor, TOK_DEV, axis=0)
    step_factor = jnp.exp(jax.random.uniform(jax.random.fold_in(key, 25), (SEQUENCE_TOKENS, HEAD_COUNT), jnp.float32, math.log(0.3), math.log(3.0)))
    gate_logarithms = -head_rate[None, :] * block_factor * step_factor
    cluster_positions = jax.random.randint(jax.random.fold_in(key, 26), (3,), 0, SEQUENCE_TOKENS)
    cluster_sizes = jnp.log(jax.random.uniform(jax.random.fold_in(key, 27), (3, HEAD_COUNT), jnp.float32, 0.5, 0.8))
    gate_logarithms = gate_logarithms.at[cluster_positions].add(cluster_sizes)
    return jnp.cumsum(gate_logarithms, axis=0).astype(jnp.float32)


def block_scale(key, dims, shards, least, largest):
    gain = 1.0
    for axis_at, blocks in shards:
        steps = jax.random.uniform(jax.random.fold_in(jax.random.fold_in(key, 6), axis_at), (blocks,), jnp.float32, least / len(shards), largest / len(shards))
        gain = gain * jnp.repeat(jnp.exp(steps), dims[axis_at] // blocks).reshape((-1,) + (1,) * (len(dims) - 1 - axis_at))
    return gain


def routed_block(stream_key, own, number, rows, amount, top, bound, skew):
    sequence = jax.random.permutation(stream_key, amount)
    heavy_load, usual = portions_of(amount, rows * top, bound, skew, True), portions_of(amount, rows * top, bound, skew, False)
    places = jnp.arange(amount)

    def named(lengths, rotation):
        used = int((lengths > 0).sum())
        fixed = max(1, used // 4)
        shifted = fixed + (places - fixed + rotation * (used - fixed)) % max(1, amount - fixed)
        return jnp.zeros((amount,), jnp.int32).at[sequence[jnp.where(places < fixed, places, shifted)]].set(jnp.asarray(lengths, jnp.int32))

    lengths = jnp.where(number % 4 == 0, named(heavy_load, number // 4), named(usual, number - number // 4 - 1))
    mixed = jax.random.permutation(jax.random.fold_in(own, 3), amount)
    donor, receiver = mixed[0:amount // 2 * 2:2], mixed[1:amount // 2 * 2:2]
    slack = jnp.minimum(lengths[donor] - 1, bound - lengths[receiver]) // 2
    slack = jnp.where((donor == sequence[0]) | (receiver == sequence[0]) | (lengths[receiver] == 0), 0, jnp.maximum(slack, 0))
    shifted = jax.random.randint(jax.random.fold_in(own, 4), (amount // 2,), 0, 1 << 20) % (slack + 1)
    lengths = lengths.at[donor].add(-shifted).at[receiver].add(shifted)
    labels = jnp.searchsorted(jnp.cumsum(lengths), jnp.arange(rows * top), side="right").astype(jnp.int32)
    table = labels.reshape(top, rows).T
    table = table[jax.random.permutation(jax.random.fold_in(own, 1), rows)]
    rotation = jax.random.randint(jax.random.fold_in(own, 2), (rows, 1), 0, top)
    return jnp.take_along_axis(table, (jnp.arange(top)[None, :] + rotation) % top, axis=1)


def portions_of(number_of, total, most, slope, full):
    weights = [(1 << 20) // math.isqrt(rank ** slope) + 1 for rank in range(1, number_of + 1)]
    largest = most if full else min(most, max(-(-total // number_of), total * weights[0] // sum(weights)))
    least = 1 if total - largest >= number_of - 1 else 0
    given, spare = [largest] + [least] * (number_of - 1), total - largest - least * (number_of - 1)
    while spare > 0:
        free = [i for i in range(1, number_of) if given[i] < largest] or [i for i in range(1, number_of) if given[i] < most]
        pool, budget = sum([weights[i] for i in free]), spare
        for i in free:
            addition = min(most - given[i], max(1, budget * weights[i] // pool), spare)
            given[i] = given[i] + addition
            spare = spare - addition
    return np.array(given)


def bell_draw(stream_key, dims, spread, bound, split=(), held_as=jnp.bfloat16):
    factor_of = block_scale(stream_key, dims, split, -0.22, 0.18) if split else 1.0
    values = jax.random.normal(stream_key, dims, jnp.float32) * spread * factor_of
    return jnp.minimum(jnp.maximum(values, -bound), bound).astype(held_as)


def setup_inputs(seed: int = 0) -> dict:
    seeds = jax.random.split(jax.random.key(seed), 14)
    queries = draw_queries(jax.random.fold_in(seeds[13], 71), 0)
    key_vectors = draw_key_vectors(jax.random.fold_in(seeds[13], 71), 0)
    value_vectors = bell_draw(seeds[2], (SEQUENCE_TOKENS, HEAD_COUNT * HD), 1.0, 5.0, ((0, 16), (1, 16)))
    forget_totals = draw_forget_totals(jax.random.fold_in(seeds[13], 71), 0)
    head_gain = jnp.clip(1.0 + 0.18 * jax.random.normal(seeds[4], (HEAD_COUNT * HD,), jnp.float32), 0.1, 1.9)
    stream = bell_draw(seeds[5], (SEQUENCE_TOKENS, D), 1.0, 6.0, ((0, 256),))
    out_weight = bell_draw(seeds[6], (HEAD_COUNT * HD, D), (HEAD_COUNT * HD) ** -0.5, 0.125)
    norm_gain = jnp.clip(1.0 + 0.18 * jax.random.normal(seeds[7], (D,), jnp.float32), 0.1, 1.9)
    routing_keys = jax.random.split(jax.random.fold_in(seeds[8], 1), SEQUENCE_TOKENS // ROWS_DEV)
    routing_turns = jax.random.permutation(jax.random.fold_in(seeds[8], 3), SEQUENCE_TOKENS // ROWS_DEV)
    routing = jax.vmap(lambda own, number: routed_block(jax.random.fold_in(seeds[8], 2), own, number, ROWS_DEV, EXPERTS, TOP, CAP, 1))(routing_keys, routing_turns).reshape((SEQUENCE_TOKENS, TOP))
    route_weights = jnp.clip(0.2 + 0.8 * jax.random.uniform(seeds[9], (SEQUENCE_TOKENS, TOP), jnp.float32) ** block_scale(seeds[9], (SEQUENCE_TOKENS, TOP), ((0, 256),), -0.2, 0.2), 0.2, 1.0)
    gate_weight = bell_draw(seeds[10], (EXPERTS, D, FF_E), D ** -0.5, 0.125, ((0, 16), (2, 16)))
    up_weight = bell_draw(seeds[11], (EXPERTS, D, FF_E), D ** -0.5, 0.125, ((0, 16), (2, 16)))
    down_weight = bell_draw(seeds[12], (EXPERTS, FF_E, D), FF_E ** -0.5, 0.09375, ((0, 16), (1, 16)))
    return {"queries": queries, "key_vectors": key_vectors, "value_vectors": value_vectors, "forget_totals": forget_totals, "head_gain": head_gain, "stream": stream, "out_weight": out_weight, "norm_gain": norm_gain, "routing": routing, "route_weights": route_weights, "gate_weight": gate_weight, "up_weight": up_weight, "down_weight": down_weight}


def attention_rows(queries, key_vectors, value_vectors, forget_totals, head_gain):
    seq_len = queries.shape[0]
    query_block = 512 if seq_len % 512 == 0 else seq_len
    query_complete = queries.astype(jnp.float32).reshape(seq_len, HEAD_COUNT, HD)
    key_all = key_vectors.astype(jnp.float32).reshape(seq_len, HEAD_COUNT, HD)
    value_all = value_vectors.astype(jnp.float32).reshape(seq_len, HEAD_COUNT, HD)
    gate_rows = jnp.transpose(forget_totals)
    key_pos = jnp.arange(seq_len, dtype=jnp.int32)
    gain_grid = head_gain.reshape(HEAD_COUNT, 1, HD)

    def one_block(block_index):
        first_row = block_index * query_block
        query_rows = lax.dynamic_slice_in_dim(query_complete, first_row, query_block, 0)
        query_gate = lax.dynamic_slice_in_dim(gate_rows, first_row, query_block, 1)
        scores = jnp.einsum('qhd,khd->hqk', query_rows, key_all) * HD ** (-0.5) + query_gate[:, :, None] - gate_rows[:, None, :]
        query_pos = first_row + jnp.arange(query_block, dtype=jnp.int32)
        visible = (key_pos[None, :] <= query_pos[:, None])[None]
        scores = jnp.where(visible, scores, -jnp.inf)
        row_peak = lax.optimization_barrier(jnp.max(scores, axis=2, keepdims=True))
        lifted = jnp.exp(scores - row_peak)
        row_total = lax.optimization_barrier(jnp.sum(lifted, axis=2))
        rounded = lax.optimization_barrier(lifted.astype(jnp.bfloat16))
        numerator = jnp.einsum('hqk,khd->hqd', rounded.astype(jnp.float32), value_all)
        attended = numerator / row_total[:, :, None]
        inverse_rms = lax.rsqrt(lax.optimization_barrier(jnp.mean(attended * attended, axis=2, keepdims=True)) + 1e-06)
        normed = attended * inverse_rms * gain_grid
        return jnp.transpose(normed, (1, 0, 2)).reshape(query_block, HEAD_COUNT * HD).astype(jnp.bfloat16)
    block_count = seq_len // query_block
    head_out = lax.map(one_block, jnp.arange(block_count, dtype=jnp.int32))
    return head_out.reshape(seq_len, HEAD_COUNT * HD)

def expert_rows(normed_rows, routing, route_weights, gate_weight, up_weight, down_weight):
    token_count = normed_rows.shape[0]
    row_block = 128
    flat_expert = routing.reshape(-1).astype(jnp.int32)
    pair_count = flat_expert.shape[0]
    flat_token = (jnp.arange(pair_count, dtype=jnp.int32) // TOP).astype(jnp.int32)
    flat_weight = route_weights.reshape(-1)
    ordering = jnp.argsort(flat_expert, stable=True)
    sorted_expert = flat_expert[ordering]
    per_expert = lax.optimization_barrier(jnp.sum((flat_expert[:, None] == jnp.arange(EXPERTS, dtype=jnp.int32)[None, :]).astype(jnp.int32), axis=0)).astype(jnp.int32)
    padded = ((per_expert + row_block - 1) // row_block * row_block).astype(jnp.int32)
    pad_end = jnp.cumsum(padded).astype(jnp.int32)
    pad_start = (pad_end - padded).astype(jnp.int32)
    run_start = (jnp.cumsum(per_expert) - per_expert).astype(jnp.int32)
    target = (pad_start[sorted_expert] + jnp.arange(pair_count, dtype=jnp.int32) - run_start[sorted_expert]).astype(jnp.int32)
    block_count = -(-pair_count // row_block) + EXPERTS
    slot_total = block_count * row_block
    slot_token = jnp.full((slot_total,), token_count, jnp.int32).at[target].set(flat_token[ordering])
    slot_weight = jnp.zeros((slot_total,), jnp.float32).at[target].set(flat_weight[ordering])
    block_starts = (jnp.arange(block_count, dtype=jnp.int32) * row_block).astype(jnp.int32)
    block_expert = jnp.minimum(jnp.searchsorted(pad_end, block_starts, side='right').astype(jnp.int32), EXPERTS - 1).astype(jnp.int32)
    padded_rows = jnp.concatenate([normed_rows, jnp.zeros((1, normed_rows.shape[1]), normed_rows.dtype)], axis=0)[slot_token]
    units_dev = FF_E // N_TP

    def expert_block(block_args):
        block_in, expert_id = block_args
        gate_pre = jnp.dot(block_in, gate_weight[expert_id], preferred_element_type=jnp.float32)
        up_pre = jnp.dot(block_in, up_weight[expert_id], preferred_element_type=jnp.float32)
        hidden = lax.optimization_barrier((jax.nn.silu(gate_pre) * up_pre).astype(jnp.bfloat16))
        grouped_rows = jnp.transpose(hidden.reshape(row_block, N_TP, units_dev), (1, 0, 2)).astype(jnp.float32)
        down_groups = down_weight[expert_id].reshape(N_TP, units_dev, -1).astype(jnp.float32)
        partial_value = lax.optimization_barrier(jnp.einsum('gbf,gfd->gbd', grouped_rows, down_groups).astype(jnp.bfloat16))
        return lax.optimization_barrier(jnp.sum(partial_value.astype(jnp.float32), axis=0)).astype(jnp.bfloat16)
    expert_out = lax.map(expert_block, (padded_rows.reshape(block_count, row_block, -1), block_expert))
    expert_out = expert_out.reshape(slot_total, -1)
    weighted = expert_out.astype(jnp.float32) * slot_weight[:, None]
    return jax.ops.segment_sum(weighted, slot_token, num_segments=token_count + 1)[:token_count]

def reference(queries, key_vectors, value_vectors, forget_totals, head_gain, stream, out_weight, norm_gain, routing, route_weights, gate_weight, up_weight, down_weight):
    head_out = attention_rows(queries, key_vectors, value_vectors, forget_totals, head_gain)
    mixed_rows = jnp.dot(head_out, out_weight, preferred_element_type=jnp.float32)
    resid_sum = stream.astype(jnp.float32) + mixed_rows
    center = resid_sum - lax.optimization_barrier(jnp.mean(resid_sum, axis=1, keepdims=True))
    normed_rows = (center * lax.rsqrt(lax.optimization_barrier(jnp.mean(center * center, axis=1, keepdims=True)) + 1e-05) * norm_gain).astype(jnp.bfloat16)
    routed = expert_rows(normed_rows, routing, route_weights, gate_weight, up_weight, down_weight)
    return (resid_sum + routed).astype(jnp.bfloat16)
```

```python
from functools import partial

import jax
import jax.numpy as jnp
from jax import lax
from jax.experimental import pallas as pl
from jax.experimental.pallas import tpu as pltpu
from jax.sharding import PartitionSpec as P

HD = 128
TOP = 2
LOG2E = 1.4426950408889634
low_score = -1e30
GATE_ROWS = 16


def sp_perm(dy, dx):
    return [
        (y * 4 + x, ((y + dy) % 4) * 4 + (x + dx) % 4) for y in range(4) for x in range(4)
    ]


def z_perm(dz):
    return [(z * 2 + c, ((z + dz) % 8) * 2 + c) for z in range(8) for c in range(2)]


core_swap = [(i, i ^ 1) for i in range(16)]


def three_parts(gates):
    first = lax.reduce_precision(gates, 8, 7)
    rest = gates - first
    second = lax.reduce_precision(rest, 8, 7)
    third = rest - second
    return jnp.stack([first, second, third]).astype(jnp.bfloat16)


def make_piece(keys, values, gates):
    rows = keys.shape[0]
    both = jnp.concatenate([keys, values], axis=1)
    parts = three_parts(gates[:, 0])
    parts = jnp.pad(parts, ((0, GATE_ROWS - 3), (0, 2 * HD - rows)))
    return jnp.concatenate([both, parts], axis=0)


def attend_kernel(
    *refs, layout, first, last, piece_rows, row_block, tok_count
):
    refs = list(refs)
    meta = refs.pop(0)
    gate_ref = refs.pop(0)
    query = refs.pop(0)
    bundles = [refs.pop(0) for _ in layout]
    if not first:
        max_in, sum_in, acc_in = refs.pop(0), refs.pop(0), refs.pop(0)
    if last:
        gain = refs.pop(0)
        head_out = refs.pop(0)
        run_max, run_sum, run_acc = refs
    else:
        run_max, run_sum, run_acc = refs
    keys_each = piece_rows - GATE_ROWS
    scale = HD ** (-0.5) * LOG2E
    own = meta[0]
    if first:
        run_max[...] = jnp.full_like(run_max, low_score)
        run_sum[...] = jnp.zeros_like(run_sum)
        run_acc[...] = jnp.zeros_like(run_acc)
    else:
        run_max[...] = max_in[...]
        run_sum[...] = sum_in[...]
        run_acc[...] = acc_in[...]
    start_gate = gate_ref[0, 0]

    def fold(bundle, pieces, key_offset=None):
        biases = []
        for piece in pieces:
            at = piece * piece_rows + keys_each
            parts = bundle[at : at + GATE_ROWS, :].astype(jnp.float32)
            total = parts[0:1, :] + parts[1:2, :] + parts[2:3, :]
            biases.append((start_gate - total) * LOG2E)
        for block in range(tok_count // row_block):
            rows = pl.ds(block * row_block, row_block)
            query_rows = query[rows, :]
            scores = []
            for piece, bias in zip(pieces, biases):
                at = piece * piece_rows
                keys = bundle[at : at + keys_each, 0:HD]
                raw = lax.dot_general(
                    query_rows, keys, (((1,), (1,)), ((), ())), preferred_element_type=jnp.float32
                )
                score = raw * scale + bias
                if key_offset is not None:
                    row_at = lax.broadcasted_iota(jnp.int32, score.shape, 0) + block * row_block
                    key_at = lax.broadcasted_iota(jnp.int32, score.shape, 1) + key_offset
                    score = jnp.where(key_at <= row_at, score, low_score)
                scores.append(score)
            old_max = run_max[rows, :]
            peak = scores[0]
            for score in scores[1:]:
                peak = jnp.maximum(peak, score)
            new_max = jnp.maximum(old_max, jnp.max(peak, axis=1, keepdims=True))
            rescale = jnp.exp2(old_max - new_max)
            wide_max = jnp.concatenate([new_max] * (keys_each // HD), axis=1)
            total = run_sum[rows, :] * rescale
            acc = run_acc[rows, :] * rescale
            for piece, score in zip(pieces, scores):
                at = piece * piece_rows
                lifted = jnp.exp2(score - wide_max)
                for part in range(keys_each // HD):
                    total = total + lifted[:, part * HD : (part + 1) * HD]
                acc = acc + jnp.dot(
                    lifted.astype(jnp.bfloat16),
                    bundle[at : at + keys_each, HD : 2 * HD],
                    preferred_element_type=jnp.float32,
                )
            run_max[rows, :] = new_max
            run_sum[rows, :] = total
            run_acc[rows, :] = acc

    spot = 1
    for bundle, (count, own_offset) in zip(bundles, layout):
        if own_offset is not None:
            fold(bundle, [0], key_offset=own_offset)
            spot += count
            continue
        if count == 1:
            pl.when(meta[spot] < own)(partial(fold, bundle, [0]))
        else:
            seen = [meta[spot + i] < own for i in range(count)]
            every = seen[0]
            some = seen[0]
            for flag in seen[1:]:
                every = jnp.logical_and(every, flag)
                some = jnp.logical_or(some, flag)
            pl.when(every)(partial(fold, bundle, list(range(count))))

            @pl.when(jnp.logical_and(some, jnp.logical_not(every)))
            def _():
                for i in range(count):
                    pl.when(seen[i])(partial(fold, bundle, [i]))

        spot += count
    if last:
        for block in range(tok_count // row_block):
            rows = pl.ds(block * row_block, row_block)
            total = jnp.sum(run_sum[rows, :], axis=1, keepdims=True)
            attended = run_acc[rows, :] / total
            mean_square = jnp.mean(attended * attended, axis=1, keepdims=True)
            normed = attended * lax.rsqrt(mean_square + 1e-06) * gain[...]
            head_out[rows, :] = normed.astype(jnp.bfloat16)


def attend(meta, start_gate, query, bundles, layout, state=None, gain=None):
    tok_count = query.shape[0]
    piece_rows = bundles[0].shape[0] // layout[0][0]
    first, last = state is None, gain is not None
    operands = [meta, start_gate, query, *bundles]
    vmem = pl.BlockSpec(memory_space=pltpu.VMEM)
    smem = pl.BlockSpec(memory_space=pltpu.SMEM)
    specs = [smem, smem] + [vmem] * (1 + len(bundles))
    if not first:
        operands += list(state)
        specs += [vmem] * 3
    wide = jax.ShapeDtypeStruct((tok_count, HD), jnp.float32)
    if last:
        operands.append(gain)
        specs.append(vmem)
        outs = jax.ShapeDtypeStruct((tok_count, HD), jnp.bfloat16)
        out_specs = vmem
        scratch = [pltpu.VMEM((tok_count, HD), jnp.float32)] * 3
    else:
        outs = (wide, wide, wide)
        out_specs = (vmem, vmem, vmem)
        scratch = []
    pieces = sum(count for count, _ in layout)
    flops = 4 * tok_count * HD * (piece_rows - GATE_ROWS) * pieces
    return pl.pallas_call(
        partial(
            attend_kernel,
            layout=tuple(layout),
            first=first,
            last=last,
            piece_rows=piece_rows,
            row_block=min(128, tok_count),
            tok_count=tok_count,
        ),
        out_shape=outs,
        in_specs=specs,
        out_specs=out_specs,
        scratch_shapes=scratch,
        compiler_params=pltpu.CompilerParams(vmem_limit_bytes=24 * 1024 * 1024),
        cost_estimate=pl.CostEstimate(
            flops=flops, transcendentals=flops // (4 * HD), bytes_accessed=1 << 20
        ),
    )(*operands)


def attention(queries, key_vectors, value_vectors, forget_totals, head_gain):
    tok_count = queries.shape[0]
    half = tok_count // 2
    sp_index = lax.axis_index("sp").astype(jnp.int32)
    row_y, col_x = sp_index // 4, sp_index % 4

    def place(dy, dx):
        return ((row_y + dy) % 4) * 4 + (col_x + dx) % 4

    def shift(array, dy, dx):
        return lax.ppermute(array, "sp", sp_perm(dy, dx))

    first_a = make_piece(key_vectors[:half], value_vectors[:half], forget_totals[:half])
    first_b = make_piece(key_vectors[half:], value_vectors[half:], forget_totals[half:])
    cut = first_a.shape[0] // 32 * 16
    a_low = shift(first_a, 0, 1)
    a_high = shift(first_a, 0, -1)
    b_low = shift(first_b, 1, 0)
    b_high = shift(first_b, -1, 0)
    a_far = jnp.concatenate([shift(a_low[:cut], 0, 1), shift(a_high[cut:], 0, -1)])
    b_far = jnp.concatenate([shift(b_low[:cut], 1, 0), shift(b_high[cut:], -1, 0)])
    a_row = jnp.concatenate([first_a, a_low, a_high, a_far])
    b_col = jnp.concatenate([first_b, b_low, b_high, b_far])
    rel = (0, -1, 1, 2)
    a_row_low = shift(a_row, 1, 0)
    a_row_high = shift(a_row, -1, 0)
    b_col_low = shift(b_col, 0, 1)
    b_col_high = shift(b_col, 0, -1)
    mid = a_row.shape[0] // 2
    a_row_far1 = shift(a_row_low[:mid], 1, 0)
    a_row_far2 = shift(a_row_high[mid:], -1, 0)
    b_col_far1 = shift(b_col_low[:mid], 0, 1)
    b_col_far2 = shift(b_col_high[mid:], 0, -1)

    start_gate = forget_totals[:1, :1]
    gain = head_gain.reshape(1, HD)

    def meta_of(places):
        return jnp.stack([sp_index] + places).astype(jnp.int32)

    places = [sp_index, sp_index]
    layout = [(1, 0), (1, half), (1, None), (1, None), (1, None), (1, None), (1, None), (1, None)]
    places += [place(0, -1), place(0, 1), place(0, 2), place(-1, 0), place(1, 0), place(2, 0)]
    state = attend(
        meta_of(places),
        start_gate,
        queries,
        [first_a, first_b, a_low, a_high, a_far, b_low, b_high, b_far],
        layout,
    )
    places = [place(-1, d) for d in rel] + [place(1, d) for d in rel]
    places += [place(d, -1) for d in rel] + [place(d, 1) for d in rel]
    state = attend(
        meta_of(places),
        start_gate,
        queries,
        [a_row_low, a_row_high, b_col_low, b_col_high],
        [(4, None)] * 4,
        state=state,
    )
    places = [place(2, d) for d in rel] + [place(d, 2) for d in rel]
    return attend(
        meta_of(places),
        start_gate,
        queries,
        [a_row_far1, a_row_far2, b_col_far1, b_col_far2],
        [(2, None)] * 4,
        state=state,
        gain=gain,
    )


def expert_kernel(*refs, count):
    rows = refs[:count]
    gate_a, gate_b, up_a, up_b, down_a, down_b = refs[count : count + 6]
    outs = refs[count + 6 : 2 * count + 6]
    joined = refs[-1] if count > 1 else rows[0]
    each = rows[0].shape[0]
    if count > 1:
        for i, part in enumerate(rows):
            joined[i * each : (i + 1) * each, :] = part[...]
    hidden = []
    for gate, up in ((gate_a, up_a), (gate_b, up_b)):
        gate_pre = jnp.dot(joined[...], gate[...], preferred_element_type=jnp.float32)
        up_pre = jnp.dot(joined[...], up[...], preferred_element_type=jnp.float32)
        silu = gate_pre / (1.0 + jnp.exp(-gate_pre))
        hidden.append((silu * up_pre).astype(jnp.bfloat16))
    width = outs[0].shape[1]
    step = 512
    for col in range(0, width, step):
        part = jnp.dot(
            hidden[0], down_a[:, col : col + step], preferred_element_type=jnp.float32
        ) + jnp.dot(hidden[1], down_b[:, col : col + step], preferred_element_type=jnp.float32)
        part = part.astype(jnp.bfloat16)
        for i, out in enumerate(outs):
            out[:, col : col + step] = part[i * each : (i + 1) * each]


def expert_rows(rows, weights):
    count = len(rows)
    each, width = rows[0].shape
    hidden = weights[0].shape[1] * 2
    vmem = pl.BlockSpec(memory_space=pltpu.VMEM)
    flops = 2 * count * each * width * hidden * 3
    return pl.pallas_call(
        partial(expert_kernel, count=count),
        out_shape=tuple(jax.ShapeDtypeStruct((each, width), jnp.bfloat16) for _ in rows),
        in_specs=[vmem] * (count + 6),
        out_specs=tuple(vmem for _ in rows),
        scratch_shapes=[pltpu.VMEM((count * each, width), jnp.bfloat16)] if count > 1 else [],
        compiler_params=pltpu.CompilerParams(vmem_limit_bytes=28 * 1024 * 1024),
        cost_estimate=pl.CostEstimate(flops=flops, transcendentals=0, bytes_accessed=6 << 20),
    )(*rows, *weights)


def added(left, right):
    return (left.astype(jnp.float32) + right.astype(jnp.float32)).astype(jnp.bfloat16)


def expert_sum(own, weights):
    def up(array):
        return lax.ppermute(array, "tp", z_perm(1))

    def down(array):
        return lax.ppermute(array, "tp", z_perm(-1))

    half = own.shape[0] // 2
    low1, high1 = up(own), down(own)
    (part0,) = expert_rows([own], weights)
    low2, high2 = up(low1), down(high1)
    part_low1, part_high1 = expert_rows([low1, high1], weights)
    low3, high3 = up(low2), down(high2)
    part_low2, part_high2 = expert_rows([low2, high2], weights)
    far_top, far_bottom = up(low3[:half]), down(high3[half:])
    part_low3, part_high3 = expert_rows([low3, high3], weights)
    far_top, far_bottom = expert_rows([far_top, far_bottom], weights)
    from_top, from_bottom = up(far_top), down(far_bottom)
    sum_high = jnp.concatenate([added(part_high3[:half], from_top), part_high3[half:]])
    sum_low = jnp.concatenate([part_low3[:half], added(part_low3[half:], from_bottom)])
    sum_high, sum_low = added(up(sum_high), part_high2), added(down(sum_low), part_low2)
    sum_high, sum_low = added(up(sum_high), part_high1), added(down(sum_low), part_low1)
    sum_high, sum_low = up(sum_high), down(sum_low)
    total = (
        sum_high.astype(jnp.float32) + sum_low.astype(jnp.float32) + part0.astype(jnp.float32)
    )
    return total.astype(jnp.bfloat16)


def on_device(
    queries,
    key_vectors,
    value_vectors,
    forget_totals,
    head_gain,
    stream,
    out_weight,
    norm_gain,
    routing,
    route_weights,
    gate_weight,
    up_weight,
    down_weight,
):
    sp_count = lax.axis_size("sp")
    weights = []
    for weight in (gate_weight[0], up_weight[0], down_weight[0]):
        weights += [weight, lax.ppermute(weight, "tp", core_swap)]
    head_out = attention(queries, key_vectors, value_vectors, forget_totals, head_gain)
    token_heads = lax.all_to_all(head_out, "tp", split_axis=0, concat_axis=1, tiled=True)
    mixed_rows = jnp.dot(token_heads, out_weight, preferred_element_type=jnp.float32)
    resid_sum = stream.astype(jnp.float32) + mixed_rows
    center = resid_sum - jnp.mean(resid_sum, axis=1, keepdims=True)
    normed_rows = (
        center * lax.rsqrt(jnp.mean(center * center, axis=1, keepdims=True) + 1e-05) * norm_gain
    ).astype(jnp.bfloat16)
    row_count = normed_rows.shape[0]
    capacity = max(2, 2 * TOP * row_count // sp_count)
    flat_expert = routing.reshape(-1)
    onehot = (flat_expert[:, None] == jnp.arange(sp_count, dtype=jnp.int32)[None, :]).astype(
        jnp.int32
    )
    earlier = jnp.cumsum(onehot, axis=0) - onehot
    slot_index = flat_expert * capacity + jnp.sum(earlier * onehot, axis=1)
    slot_grid = slot_index.reshape(row_count, TOP)
    slot_ids = jnp.arange(sp_count * capacity, dtype=jnp.int32)
    placing = jnp.sum(
        (slot_grid[None, :, :] == slot_ids[:, None, None]).astype(jnp.float32), axis=2
    ).astype(jnp.bfloat16)
    outgoing = jnp.dot(placing, normed_rows, preferred_element_type=jnp.float32).astype(
        jnp.bfloat16
    )
    outgoing = outgoing.reshape(sp_count, capacity, normed_rows.shape[1])
    arrived = lax.all_to_all(outgoing, "sp", split_axis=0, concat_axis=0, tiled=True)
    summed = expert_sum(arrived.reshape(-1, arrived.shape[2]), weights)
    expert_out = summed.reshape(sp_count, capacity, -1)
    returned = lax.all_to_all(expert_out, "sp", split_axis=0, concat_axis=0, tiled=True)
    picked = returned.reshape(sp_count * capacity, -1)[slot_index].astype(jnp.float32)
    weighted = picked * route_weights.reshape(-1)[:, None]
    routed = jnp.sum(weighted.reshape(row_count, TOP, -1), axis=1)
    return (resid_sum + routed).astype(jnp.bfloat16)


def solution(mesh):
    in_specs = (
        P("sp", "tp"),
        P("sp", "tp"),
        P("sp", "tp"),
        P("sp", "tp"),
        P("tp"),
        P(("sp", "tp"), None),
        P(),
        P(),
        P(("sp", "tp"), None),
        P(("sp", "tp"), None),
        P("sp", None, "tp"),
        P("sp", None, "tp"),
        P("sp", "tp", None),
    )
    out_specs = P(("sp", "tp"), None)
    return jax.shard_map(
        on_device, mesh=mesh, in_specs=in_specs, out_specs=out_specs, check_vma=False
    )
```

```python
from functools import partial

import jax
import jax.numpy as jnp
from jax import lax
from jax.experimental import pallas as pl
from jax.experimental.pallas import tpu as pltpu
from jax.sharding import PartitionSpec as P

HD = 128
TOP = 2
LOG2E = 1.4426950408889634
low_score = -1e30
GATE_ROWS = 16
KEYS = 256
PIECE = KEYS + GATE_ROWS


def sp_perm(dy, dx):
    return [
        (y * 4 + x, ((y + dy) % 4) * 4 + (x + dx) % 4) for y in range(4) for x in range(4)
    ]


def z_perm(dz):
    return [(z * 2 + c, ((z + dz) % 8) * 2 + c) for z in range(8) for c in range(2)]


core_swap = [(i, i ^ 1) for i in range(16)]


vmem = pl.BlockSpec(memory_space=pltpu.VMEM)
smem = pl.BlockSpec(memory_space=pltpu.SMEM)


def three_parts(wide):
    first = wide.astype(jnp.bfloat16)
    rest = wide - first.astype(jnp.float32)
    second = rest.astype(jnp.bfloat16)
    third = (rest - second.astype(jnp.float32)).astype(jnp.bfloat16)
    return first, second, third


def piece_kernel(queries, keys, values, gates, piece_a, piece_b, query_cols, gate_mix):
    stretched = gates[...] * HD**0.5
    tok_count = stretched.shape[1]
    query_cols[...] = jnp.transpose(queries[...])
    row = lax.broadcasted_iota(jnp.int32, (GATE_ROWS, KEYS), 0)
    for i, piece in enumerate((piece_a, piece_b)):
        rows = slice(i * KEYS, (i + 1) * KEYS)
        piece[0:HD, :] = jnp.transpose(values[rows, :])
        piece[HD:KEYS, 0:HD] = keys[i * KEYS : i * KEYS + HD, :]
        piece[HD:KEYS, HD:KEYS] = keys[i * KEYS + HD : (i + 1) * KEYS, :]
        parts = [part.astype(jnp.float32) for part in three_parts(-stretched[:, rows])]
        block = jnp.where((row >= 3) & (row < 6), 1.0, 0.0)
        for at, part in enumerate(parts):
            block = jnp.where(row == at, part, block)
        piece[KEYS:PIECE, :] = block.astype(jnp.bfloat16)
    wide_row = lax.broadcasted_iota(jnp.int32, (GATE_ROWS, tok_count), 0)
    mix = jnp.where(wide_row < 3, 1.0, 0.0)
    parts = [part.astype(jnp.float32) for part in three_parts(stretched[:, 0:1])]
    for at, part in enumerate(parts):
        mix = jnp.where(wide_row == 3 + at, part, mix)
    mix = jnp.where(wide_row == 6, low_score, mix)
    gate_mix[...] = mix.astype(jnp.bfloat16)


def make_pieces(queries, keys, values, gates):
    tok_count = queries.shape[0]
    piece = jax.ShapeDtypeStruct((PIECE, 2 * HD), jnp.bfloat16)
    return pl.pallas_call(
        piece_kernel,
        out_shape=(
            piece,
            piece,
            jax.ShapeDtypeStruct((HD, tok_count), jnp.bfloat16),
            jax.ShapeDtypeStruct((GATE_ROWS, tok_count), jnp.bfloat16),
        ),
        in_specs=[vmem] * 4,
        out_specs=(vmem,) * 4,
        compiler_params=pltpu.CompilerParams(vmem_limit_bytes=6 << 20),
        name="make_pieces",
    )(queries, keys, values, gates.reshape(1, tok_count))


def bundle_kernel(*refs):
    for i in range(2):
        at = 0
        out = refs[10 + i]
        for part in refs[5 * i : 5 * i + 5]:
            out[at : at + part.shape[0], :] = part[...]
            at += part.shape[0]


def make_bundles(parts_a, parts_b):
    bundle = jax.ShapeDtypeStruct((4 * PIECE, 2 * HD), jnp.bfloat16)
    return pl.pallas_call(
        bundle_kernel,
        out_shape=(bundle, bundle),
        in_specs=[vmem] * 10,
        out_specs=(vmem, vmem),
        compiler_params=pltpu.CompilerParams(vmem_limit_bytes=6 << 20),
        name="make_bundles",
    )(*parts_a, *parts_b)


def attend_kernel(*refs, stage):
    own_ref, query_cols, gate_mix = refs[:3]
    refs = list(refs[3:])
    bundles = [refs.pop(0) for _ in range(2 if stage == 0 else 4)]
    if stage > 0:
        state_in = [refs.pop(0) for _ in range(3)]
    if stage == 2:
        gain, head_out = refs.pop(0), refs.pop(0)
    run_max, run_sum, run_acc = refs
    tok_count = query_cols.shape[1]
    scale = HD ** (-0.5) * LOG2E
    own = own_ref[0]
    own_y, own_x = own >> 2, own & 3
    if stage == 0:
        run_max[...] = jnp.full_like(run_max, low_score)
        run_sum[...] = jnp.zeros_like(run_sum)
        run_acc[...] = jnp.zeros_like(run_acc)
    else:
        for into, came in zip((run_max, run_sum, run_acc), state_in):
            into[...] = came[...]
    hide = jnp.where(lax.broadcasted_iota(jnp.int32, (GATE_ROWS, KEYS), 0) == 6, 1.0, 0.0)

    def seen(dy, dx):
        return ((own_y + dy) & 3) * 4 + ((own_x + dx) & 3) < own

    def fold(pieces, flags=None, own_block=False):
        scores = []
        for i, (bundle, at) in enumerate(pieces):
            gates = bundle[pl.ds(at + KEYS, GATE_ROWS), :]
            if flags is not None:
                gates = jnp.where(flags[i], gates.astype(jnp.float32), hide).astype(jnp.bfloat16)
            bias = lax.dot_general(
                gates, gate_mix[...], (((0,), (0,)), ((), ())), preferred_element_type=jnp.float32
            )
            for part in range(KEYS // HD):
                keys = bundle[pl.ds(at + HD, HD), part * HD : (part + 1) * HD]
                score = jnp.dot(keys, query_cols[...], preferred_element_type=jnp.float32)
                score = score + bias[part * HD : (part + 1) * HD]
                if own_block:
                    key_at = lax.broadcasted_iota(jnp.int32, score.shape, 0)
                    key_at = key_at + (i * KEYS + part * HD)
                    query_at = lax.broadcasted_iota(jnp.int32, score.shape, 1)
                    score = jnp.where(key_at <= query_at, score, low_score)
                scores.append(score)
        old_max = run_max[0:1, :]
        peak = scores[0]
        for score in scores[1:]:
            peak = jnp.maximum(peak, score)
        new_max = jnp.maximum(old_max, jnp.max(peak, axis=0, keepdims=True))
        rescale = jnp.exp2((old_max - new_max) * scale)
        scaled_max = new_max * scale
        total = run_sum[...] * rescale
        acc = run_acc[...] * rescale
        for i, (bundle, at) in enumerate(pieces):
            rounded = []
            for score in scores[2 * i : 2 * i + 2]:
                lifted = jnp.exp2(score * scale - scaled_max)
                total = total + jnp.sum(lifted.reshape(HD // 8, 8, tok_count), axis=0)
                rounded.append(lifted.astype(jnp.bfloat16))
            acc = acc + jnp.dot(
                bundle[pl.ds(at, HD), :],
                jnp.concatenate(rounded, axis=0),
                preferred_element_type=jnp.float32,
            )
        run_sum[...] = total
        run_acc[...] = acc
        run_max[...] = jnp.broadcast_to(new_max, run_max.shape)

    def fold_seen(pieces, flags):
        pl.when(jnp.logical_or(*flags))(partial(fold, pieces, flags))

    if stage == 0:
        row, col = bundles
        fold([(row, 0), (col, 0)], own_block=True)
        fold_seen([(row, PIECE), (row, 2 * PIECE)], (seen(0, -1), seen(0, 1)))
        fold_seen([(col, PIECE), (col, 2 * PIECE)], (seen(-1, 0), seen(1, 0)))
        fold_seen([(row, 3 * PIECE), (col, 3 * PIECE)], (seen(0, 2), seen(2, 0)))
    elif stage == 1:
        for bundle, (dy, dx) in zip(bundles, ((-1, None), (1, None), (None, -1), (None, 1))):

            def pair(i, carry, bundle=bundle, dy=dy, dx=dx):
                flags = []
                for rel in (i, 3 * i - 1):
                    flags.append(seen(rel if dy is None else dy, rel if dx is None else dx))
                at = pl.multiple_of(i * (2 * PIECE), 32)
                fold_seen([(bundle, at), (bundle, at + PIECE)], flags)
                return carry

            lax.fori_loop(0, 2, pair, 0)
    else:
        sides = ((2, 0), (2, -1)), ((2, 1), (2, 2)), ((0, 2), (-1, 2)), ((1, 2), (2, 2))
        for bundle, side in zip(bundles, sides):
            fold_seen([(bundle, 0), (bundle, PIECE)], [seen(dy, dx) for dy, dx in side])
        total = jnp.sum(run_sum[...], axis=0, keepdims=True)
        attended = run_acc[...] / total
        mean_square = jnp.mean(attended * attended, axis=0, keepdims=True)
        normed = jnp.transpose(attended * lax.rsqrt(mean_square + 1e-06))
        head_out[...] = (normed * gain[...]).astype(jnp.bfloat16)


def attend(own, query_cols, gate_mix, bundles, stage, state=(), gain=None):
    tok_count = query_cols.shape[1]
    operands = [own, query_cols, gate_mix, *bundles, *state]
    narrow = ((8, tok_count), jnp.float32)
    shapes = (narrow, narrow, ((HD, tok_count), jnp.float32))
    if stage == 2:
        operands.append(gain)
        outs = jax.ShapeDtypeStruct((tok_count, HD), jnp.bfloat16)
        out_specs = vmem
        scratch = [pltpu.VMEM(*shape) for shape in shapes]
    else:
        outs = tuple(jax.ShapeDtypeStruct(*shape) for shape in shapes)
        out_specs = (vmem,) * 3
        scratch = []
    pieces = sum(bundle.shape[0] // PIECE for bundle in bundles)
    flops = 8 * tok_count * HD * KEYS * pieces
    return pl.pallas_call(
        partial(attend_kernel, stage=stage),
        out_shape=outs,
        in_specs=[smem] + [vmem] * (len(operands) - 1),
        out_specs=out_specs,
        scratch_shapes=scratch,
        compiler_params=pltpu.CompilerParams(vmem_limit_bytes=12 << 20),
        cost_estimate=pl.CostEstimate(
            flops=flops, transcendentals=tok_count * KEYS * pieces, bytes_accessed=1 << 20
        ),
        name="attend%d" % stage,
    )(*operands)


def attention(queries, key_vectors, value_vectors, forget_totals, head_gain, early):
    own = lax.axis_index("sp").astype(jnp.int32).reshape(1)

    def shift(array, dy, dx):
        return lax.ppermute(array, "sp", sp_perm(dy, dx))

    first_a, first_b, query_cols, gate_mix = make_pieces(
        queries, key_vectors, value_vectors, forget_totals
    )
    a_low = shift(first_a, 0, 1)
    a_high = shift(first_a, 0, -1)
    b_low = shift(first_b, 1, 0)
    b_high = shift(first_b, -1, 0)
    cut = HD
    a_far = shift(a_low[:cut], 0, 1), shift(a_high[cut:], 0, -1)
    b_far = shift(b_low[:cut], 1, 0), shift(b_high[cut:], -1, 0)
    a_row, b_col = make_bundles(
        (first_a, a_low, a_high, *a_far), (first_b, b_low, b_high, *b_far)
    )
    near = (
        shift(a_row, 1, 0),
        shift(a_row, -1, 0),
        shift(b_col, 0, 1),
        shift(b_col, 0, -1),
    )
    state = attend(own, query_cols, gate_mix, [a_row, b_col], 0)
    near, state, early = lax.optimization_barrier((near, state, early))
    mid = 2 * PIECE
    far = (
        shift(near[0][:mid], 1, 0),
        shift(near[1][mid:], -1, 0),
        shift(near[2][:mid], 0, 1),
        shift(near[3][mid:], 0, -1),
    )
    state = attend(own, query_cols, gate_mix, near, 1, state)
    far, state = lax.optimization_barrier((far, state))
    head_out = attend(own, query_cols, gate_mix, far, 2, state, head_gain.reshape(1, HD))
    return head_out, early


def expert_kernel(*refs, count):
    rows = refs[:count]
    gate_a, gate_b, up_a, up_b, down_a, down_b = refs[count : count + 6]
    outs = refs[count + 6 : 2 * count + 6]
    joined = refs[-1] if count > 1 else rows[0]
    each = rows[0].shape[0]
    if count > 1:
        for i, part in enumerate(rows):
            joined[i * each : (i + 1) * each, :] = part[...]
    hidden = []
    for gate, up in ((gate_a, up_a), (gate_b, up_b)):
        gate_pre = jnp.dot(joined[...], gate[...], preferred_element_type=jnp.float32)
        up_pre = jnp.dot(joined[...], up[...], preferred_element_type=jnp.float32)
        silu = gate_pre / (1.0 + jnp.exp(-gate_pre))
        hidden.append((silu * up_pre).astype(jnp.bfloat16))
    width = outs[0].shape[1]
    step = 512
    for col in range(0, width, step):
        part = jnp.dot(
            hidden[0], down_a[:, col : col + step], preferred_element_type=jnp.float32
        ) + jnp.dot(hidden[1], down_b[:, col : col + step], preferred_element_type=jnp.float32)
        part = part.astype(jnp.bfloat16)
        for i, out in enumerate(outs):
            out[:, col : col + step] = part[i * each : (i + 1) * each]


def expert_rows(rows, weights):
    count = len(rows)
    each, width = rows[0].shape
    hidden = weights[0].shape[1] * 2
    flops = 2 * count * each * width * hidden * 3
    return pl.pallas_call(
        partial(expert_kernel, count=count),
        out_shape=tuple(jax.ShapeDtypeStruct((each, width), jnp.bfloat16) for _ in rows),
        in_specs=[vmem] * (count + 6),
        out_specs=tuple(vmem for _ in rows),
        scratch_shapes=[pltpu.VMEM((count * each, width), jnp.bfloat16)] if count > 1 else [],
        compiler_params=pltpu.CompilerParams(vmem_limit_bytes=16 << 20),
        cost_estimate=pl.CostEstimate(flops=flops, transcendentals=0, bytes_accessed=6 << 20),
        name="expert%d" % count,
    )(*rows, *weights)


def added(left, right):
    return (left.astype(jnp.float32) + right.astype(jnp.float32)).astype(jnp.bfloat16)


def expert_sum(own, weights):
    def up(array):
        return lax.ppermute(array, "tp", z_perm(1))

    def down(array):
        return lax.ppermute(array, "tp", z_perm(-1))

    half = own.shape[0] // 2
    low1, high1 = up(own), down(own)
    (part0,) = expert_rows([own], weights)
    low2, high2 = up(low1), down(high1)
    part_low1, part_high1 = expert_rows([low1, high1], weights)
    low3, high3 = up(low2), down(high2)
    part_low2, part_high2 = expert_rows([low2, high2], weights)
    far_top, far_bottom = up(low3[:half]), down(high3[half:])
    part_low3, part_high3 = expert_rows([low3, high3], weights)
    far_top, far_bottom = expert_rows([far_top, far_bottom], weights)
    from_top, from_bottom = up(far_top), down(far_bottom)
    sum_high = jnp.concatenate([added(part_high3[:half], from_top), part_high3[half:]])
    sum_low = jnp.concatenate([part_low3[:half], added(part_low3[half:], from_bottom)])
    sum_high, sum_low = added(up(sum_high), part_high2), added(down(sum_low), part_low2)
    sum_high, sum_low = added(up(sum_high), part_high1), added(down(sum_low), part_low1)
    sum_high, sum_low = up(sum_high), down(sum_low)
    total = (
        sum_high.astype(jnp.float32) + sum_low.astype(jnp.float32) + part0.astype(jnp.float32)
    )
    return total.astype(jnp.bfloat16)


def project_kernel(heads, out_weight, stream, norm_gain, placing, resid_sum, outgoing, joined):
    for head in range(heads.shape[0]):
        joined[:, head * HD : (head + 1) * HD] = heads[head]
    mixed_rows = jnp.dot(joined[...], out_weight[...], preferred_element_type=jnp.float32)
    resid = stream[...].astype(jnp.float32) + mixed_rows
    resid_sum[...] = resid
    center = resid - jnp.mean(resid, axis=1, keepdims=True)
    spread = jnp.mean(center * center, axis=1, keepdims=True)
    normed = (center * lax.rsqrt(spread + 1e-05) * norm_gain[...]).astype(jnp.bfloat16)
    outgoing[...] = jnp.dot(
        placing[...], normed, preferred_element_type=jnp.float32
    ).astype(jnp.bfloat16)


def project(heads, out_weight, stream, norm_gain, placing):
    rows, width = stream.shape
    return pl.pallas_call(
        project_kernel,
        out_shape=(
            jax.ShapeDtypeStruct((rows, width), jnp.float32),
            jax.ShapeDtypeStruct((placing.shape[0], width), jnp.bfloat16),
        ),
        in_specs=[vmem] * 5,
        out_specs=(vmem, vmem),
        scratch_shapes=[pltpu.VMEM((rows, heads.shape[0] * HD), jnp.bfloat16)],
        compiler_params=pltpu.CompilerParams(vmem_limit_bytes=14 << 20),
        name="project",
    )(heads, out_weight, stream, norm_gain.reshape(1, width), placing)


def combine_kernel(resid_sum, returned, mixing, out):
    total = resid_sum[...]
    for part in three_parts(mixing[...]):
        total = total + jnp.dot(part, returned[...], preferred_element_type=jnp.float32)
    out[...] = total.astype(jnp.bfloat16)


def combine(resid_sum, returned, mixing):
    return pl.pallas_call(
        combine_kernel,
        out_shape=jax.ShapeDtypeStruct(resid_sum.shape, jnp.bfloat16),
        in_specs=[vmem] * 3,
        out_specs=vmem,
        compiler_params=pltpu.CompilerParams(vmem_limit_bytes=6 << 20),
        name="combine",
    )(resid_sum, returned, mixing)


def on_device(
    queries,
    key_vectors,
    value_vectors,
    forget_totals,
    head_gain,
    stream,
    out_weight,
    norm_gain,
    routing,
    route_weights,
    gate_weight,
    up_weight,
    down_weight,
):
    sp_count = lax.axis_size("sp")
    own_weights = (gate_weight[0], up_weight[0], down_weight[0])
    other_weights = tuple(lax.ppermute(weight, "tp", core_swap) for weight in own_weights)
    head_out, other_weights = attention(
        queries, key_vectors, value_vectors, forget_totals, head_gain, other_weights
    )
    weights = []
    for mine, other in zip(own_weights, other_weights):
        weights += [mine, other]
    row_count, width = stream.shape
    capacity = max(2, 2 * TOP * row_count // sp_count)
    flat_expert = routing.reshape(-1)
    onehot = (flat_expert[:, None] == jnp.arange(sp_count, dtype=jnp.int32)[None, :]).astype(
        jnp.int32
    )
    earlier = jnp.cumsum(onehot, axis=0) - onehot
    slot_index = flat_expert * capacity + jnp.sum(earlier * onehot, axis=1)
    slot_grid = slot_index.reshape(row_count, TOP)
    slot_ids = jnp.arange(sp_count * capacity, dtype=jnp.int32)
    placing = jnp.sum(
        (slot_grid[None, :, :] == slot_ids[:, None, None]).astype(jnp.float32), axis=2
    ).astype(jnp.bfloat16)
    mixing = jnp.sum(
        jnp.where(slot_grid[:, :, None] == slot_ids[None, None, :], route_weights[:, :, None], 0.0),
        axis=1,
    )
    heads = head_out.reshape(-1, row_count, HD)
    heads = lax.all_to_all(heads, "tp", split_axis=0, concat_axis=0, tiled=True)
    resid_sum, outgoing = project(heads, out_weight, stream, norm_gain, placing)
    outgoing = outgoing.reshape(sp_count, capacity, width)
    arrived = lax.all_to_all(outgoing, "sp", split_axis=0, concat_axis=0, tiled=True)
    summed = expert_sum(arrived.reshape(-1, width), weights)
    expert_out = summed.reshape(sp_count, capacity, width)
    returned = lax.all_to_all(expert_out, "sp", split_axis=0, concat_axis=0, tiled=True)
    return combine(resid_sum, returned.reshape(-1, width), mixing)


def solution(mesh):
    in_specs = (
        P("sp", "tp"),
        P("sp", "tp"),
        P("sp", "tp"),
        P("sp", "tp"),
        P("tp"),
        P(("sp", "tp"), None),
        P(),
        P(),
        P(("sp", "tp"), None),
        P(("sp", "tp"), None),
        P("sp", None, "tp"),
        P("sp", None, "tp"),
        P("sp", "tp", None),
    )
    out_specs = P(("sp", "tp"), None)
    return jax.shard_map(
        on_device, mesh=mesh, in_specs=in_specs, out_specs=out_specs, check_vma=False
    )
```

```python
from functools import partial

import jax
import jax.numpy as jnp
from jax import lax
from jax.experimental import pallas as pl
from jax.experimental.pallas import tpu as pltpu
from jax.sharding import PartitionSpec as P

HD = 128
TOP = 2
LOG2E = 1.4426950408889634
low_score = -1e30
GATE_ROWS = 16
KEYS = 256
PIECE = KEYS + GATE_ROWS


def sp_perm(dy, dx, needed):
    pairs = []
    for y in range(4):
        for x in range(4):
            into = (y + dy) % 4, (x + dx) % 4
            if needed(*into):
                pairs.append((y * 4 + x, into[0] * 4 + into[1]))
    return pairs


def z_perm(dz):
    return [(z * 2 + c, ((z + dz) % 8) * 2 + c) for z in range(8) for c in range(2)]


core_swap = [(i, i ^ 1) for i in range(16)]


vmem = pl.BlockSpec(memory_space=pltpu.VMEM)


def three_parts(wide):
    first = wide.astype(jnp.bfloat16)
    rest = wide - first.astype(jnp.float32)
    second = rest.astype(jnp.bfloat16)
    third = (rest - second.astype(jnp.float32)).astype(jnp.bfloat16)
    return first, second, third


def piece_kernel(*refs):
    sources, outs, staged, sems = refs[:4], refs[4:8], refs[8:12], refs[12]
    copies = [
        pltpu.make_async_copy(source, into, sems.at[i])
        for i, (source, into) in enumerate(zip(sources, staged))
    ]
    for copy in copies:
        copy.start()
    for copy in copies:
        copy.wait()
    queries, keys, values, gates = staged
    piece_a, piece_b, query_cols, gate_mix = outs
    stretched = gates[...] * HD**0.5
    tok_count = stretched.shape[1]
    row = lax.broadcasted_iota(jnp.int32, (GATE_ROWS, KEYS), 0)
    for i, piece in enumerate((piece_a, piece_b)):
        rows = slice(i * KEYS, (i + 1) * KEYS)
        piece[0:HD, :] = jnp.transpose(values[rows, :])
        piece[HD:KEYS, 0:HD] = keys[i * KEYS : i * KEYS + HD, :]
        piece[HD:KEYS, HD:KEYS] = keys[i * KEYS + HD : (i + 1) * KEYS, :]
        parts = [part.astype(jnp.float32) for part in three_parts(-stretched[:, rows])]
        block = jnp.where((row >= 3) & (row < 6), 1.0, 0.0)
        for at, part in enumerate(parts):
            block = jnp.where(row == at, part, block)
        piece[KEYS:PIECE, :] = block.astype(jnp.bfloat16)
    wide_row = lax.broadcasted_iota(jnp.int32, (GATE_ROWS, tok_count), 0)
    mix = jnp.where(wide_row < 3, 1.0, 0.0)
    parts = [part.astype(jnp.float32) for part in three_parts(stretched[:, 0:1])]
    for at, part in enumerate(parts):
        mix = jnp.where(wide_row == 3 + at, part, mix)
    mix = jnp.where(wide_row == 6, low_score, mix)
    gate_mix[...] = mix.astype(jnp.bfloat16)
    query_cols[...] = jnp.transpose(queries[...])


def make_pieces(queries, keys, values, gates):
    tok_count = queries.shape[0]
    piece = jax.ShapeDtypeStruct((PIECE, 2 * HD), jnp.bfloat16)
    return pl.pallas_call(
        piece_kernel,
        out_shape=(
            piece,
            piece,
            jax.ShapeDtypeStruct((HD, tok_count), jnp.bfloat16),
            jax.ShapeDtypeStruct((GATE_ROWS, tok_count), jnp.bfloat16),
        ),
        in_specs=[pl.BlockSpec(memory_space=pltpu.HBM)] * 4,
        out_specs=(vmem,) * 4,
        scratch_shapes=[pltpu.VMEM((tok_count, HD), jnp.bfloat16)] * 3
        + [pltpu.VMEM((1, tok_count), jnp.float32), pltpu.SemaphoreType.DMA((4,))],
        compiler_params=pltpu.CompilerParams(vmem_limit_bytes=6 << 20),
        name="make_pieces",
    )(queries, keys, values, gates.reshape(1, tok_count))


def bundle_kernel(*refs):
    for i in range(2):
        for at, part in enumerate(refs[4 * i : 4 * i + 4]):
            refs[8 + i][at * PIECE : (at + 1) * PIECE, :] = part[...]


def make_bundles(parts_a, parts_b):
    bundle = jax.ShapeDtypeStruct((4 * PIECE, 2 * HD), jnp.bfloat16)
    return pl.pallas_call(
        bundle_kernel,
        out_shape=(bundle, bundle),
        in_specs=[vmem] * 8,
        out_specs=(vmem, vmem),
        compiler_params=pltpu.CompilerParams(vmem_limit_bytes=6 << 20),
        name="make_bundles",
    )(*parts_a, *parts_b)


order = (0, -1, 1, 2)
near_places = {0: ((0, -1), (0, 1), (-1, 0), (1, 0), (0, 2), (2, 0))}
near_places[1] = tuple((d, r) for d in (-1, 1) for r in order)
near_places[1] += tuple((r, d) for d in (-1, 1) for r in order)
near_places[2] = tuple((2, r) for r in order) + tuple((r, 2) for r in order)


def attend_kernel(*refs, stage):
    query_cols, gate_mix = refs[:2]
    refs = list(refs[2:])
    bundles = [refs.pop(0) for _ in range((8, 4, 4)[stage])]
    if stage > 0:
        state_in = [refs.pop(0) for _ in range(3)]
    if stage == 2:
        gain, head_out = refs.pop(0), refs.pop(0)
    stack = refs.pop() if stage != 1 else None
    run_max, run_sum, run_acc = refs
    tok_count = query_cols.shape[1]
    scale = HD ** (-0.5) * LOG2E
    own = lax.axis_index("sp")
    own_y, own_x = own >> 2, own & 3
    if stage == 0:
        run_max[...] = jnp.full_like(run_max, low_score)
        run_sum[...] = jnp.zeros_like(run_sum)
        run_acc[...] = jnp.zeros_like(run_acc)
    else:
        for into, came in zip((run_max, run_sum, run_acc), state_in):
            into[...] = came[...]
    hide = jnp.where(lax.broadcasted_iota(jnp.int32, (GATE_ROWS, KEYS), 0) == 6, 1.0, 0.0)

    def fold(pieces, flags=None, own_block=False):
        scores = []
        for i, (bundle, at) in enumerate(pieces):
            gates = bundle[pl.ds(at + KEYS, GATE_ROWS), :]
            if flags is not None:
                gates = jnp.where(flags[i], gates.astype(jnp.float32), hide).astype(jnp.bfloat16)
            bias = lax.dot_general(
                gates, gate_mix[...], (((0,), (0,)), ((), ())), preferred_element_type=jnp.float32
            )
            for part in range(KEYS // HD):
                keys = bundle[pl.ds(at + HD, HD), part * HD : (part + 1) * HD]
                score = jnp.dot(keys, query_cols[...], preferred_element_type=jnp.float32)
                score = score + bias[part * HD : (part + 1) * HD]
                if own_block:
                    key_at = lax.broadcasted_iota(jnp.int32, score.shape, 0)
                    key_at = key_at + (i * KEYS + part * HD)
                    query_at = lax.broadcasted_iota(jnp.int32, score.shape, 1)
                    score = jnp.where(key_at <= query_at, score, low_score)
                scores.append(score)
        old_max = run_max[0:1, :]
        peak = scores[0]
        for score in scores[1:]:
            peak = jnp.maximum(peak, score)
        new_max = jnp.maximum(old_max, jnp.max(peak, axis=0, keepdims=True))
        rescale = jnp.exp2((old_max - new_max) * scale)
        scaled_max = new_max * scale
        total = run_sum[...] * rescale
        acc = run_acc[...] * rescale
        for i, (bundle, at) in enumerate(pieces):
            rounded = []
            for score in scores[2 * i : 2 * i + 2]:
                lifted = jnp.exp2(score * scale - scaled_max)
                total = total + jnp.sum(lifted.reshape(HD // 8, 8, tok_count), axis=0)
                rounded.append(lifted.astype(jnp.bfloat16))
            acc = acc + jnp.dot(
                bundle[pl.ds(at, HD), :],
                jnp.concatenate(rounded, axis=0),
                preferred_element_type=jnp.float32,
            )
        run_sum[...] = total
        run_acc[...] = acc
        run_max[...] = jnp.broadcast_to(new_max, run_max.shape)

    def fold_seen(pieces, flags):
        pl.when(jnp.logical_or(*flags))(partial(fold, pieces, flags))

    if stage == 0:
        fold([(bundles.pop(0), 0), (bundles.pop(0), 0)], own_block=True)
    places = near_places[stage]

    def fold_pairs(source, first, count):
        def pair(i, carry):
            flags = []
            for side in range(2):
                spots = places[first + side : first + 2 * count : 2]
                dy, dx = spots[0]
                for at in range(1, count):
                    dy = jnp.where(i == at, spots[at][0], dy)
                    dx = jnp.where(i == at, spots[at][1], dx)
                flags.append(((own_y + dy) & 3) * 4 + ((own_x + dx) & 3) < own)
            at = pl.multiple_of(i * (2 * PIECE), 32)
            fold_seen([(source, at), (source, at + PIECE)], flags)
            return carry

        lax.fori_loop(0, count, pair, 0)

    if stage == 1:
        for i, bundle in enumerate(bundles):
            fold_pairs(bundle, 4 * i, 2)
    else:
        at = 0
        for bundle in bundles:
            stack[at : at + bundle.shape[0], :] = bundle[...]
            at += bundle.shape[0]
        fold_pairs(stack, 0, at // (2 * PIECE))
    if stage == 2:
        total = jnp.sum(run_sum[...], axis=0, keepdims=True)
        attended = run_acc[...] / total
        mean_square = jnp.mean(attended * attended, axis=0, keepdims=True)
        normed = jnp.transpose(attended * lax.rsqrt(mean_square + 1e-06))
        head_out[...] = (normed * gain[...]).astype(jnp.bfloat16)


def attend(query_cols, gate_mix, bundles, stage, state=(), gain=None):
    tok_count = query_cols.shape[1]
    operands = [query_cols, gate_mix, *bundles, *state]
    narrow = ((8, tok_count), jnp.float32)
    shapes = (narrow, narrow, ((HD, tok_count), jnp.float32))
    if stage == 2:
        operands.append(gain)
        outs = jax.ShapeDtypeStruct((tok_count, HD), jnp.bfloat16)
        out_specs = vmem
        scratch = [pltpu.VMEM(*shape) for shape in shapes]
    else:
        outs = tuple(jax.ShapeDtypeStruct(*shape) for shape in shapes)
        out_specs = (vmem,) * 3
        scratch = []
    if stage != 1:
        scratch.append(pltpu.VMEM((8 * PIECE, 2 * HD), jnp.bfloat16))
    pieces = sum(bundle.shape[0] // PIECE for bundle in bundles)
    flops = 8 * tok_count * HD * KEYS * pieces
    return pl.pallas_call(
        partial(attend_kernel, stage=stage),
        out_shape=outs,
        in_specs=[vmem] * len(operands),
        out_specs=out_specs,
        scratch_shapes=scratch,
        compiler_params=pltpu.CompilerParams(vmem_limit_bytes=12 << 20),
        cost_estimate=pl.CostEstimate(
            flops=flops, transcendentals=tok_count * KEYS * pieces, bytes_accessed=1 << 20
        ),
        name="attend%d" % stage,
    )(*operands)


def attention(queries, key_vectors, value_vectors, forget_totals, head_gain, early):
    def shift(array, dy, dx, needed):
        return lax.ppermute(array, "sp", sp_perm(dy, dx, needed))

    own_a, own_b, query_cols, gate_mix = make_pieces(
        queries, key_vectors, value_vectors, forget_totals
    )
    a_low = shift(own_a, 0, 1, lambda y, x: y < 3 or x > 0)
    a_high = shift(own_a, 0, -1, lambda y, x: y < 3 or x == 3)
    a_far = shift(own_a, 0, 2, lambda y, x: y < 3 or x > 1)
    b_low = shift(own_b, 1, 0, lambda y, x: y > 0)
    b_high = shift(own_b, -1, 0, lambda y, x: y == 3)
    b_far = shift(own_b, 2, 0, lambda y, x: y > 1)
    row, col = make_bundles((own_a, a_low, a_high, a_far), (own_b, b_low, b_high, b_far))
    near = (
        shift(row, 1, 0, lambda y, x: y > 0),
        shift(row, -1, 0, lambda y, x: y in (0, 3)),
        shift(col, 0, 1, lambda y, x: True),
        shift(col, 0, -1, lambda y, x: True),
    )
    first = [own_a, own_b, a_low, a_high, b_low, b_high, a_far, b_far]
    state = attend(query_cols, gate_mix, first, 0)
    near, state = lax.optimization_barrier((near, state))
    mid = 2 * PIECE
    far = (
        shift(near[0][:mid], 1, 0, lambda y, x: y > 1),
        shift(near[1][mid:], -1, 0, lambda y, x: y > 1),
        shift(near[2][:mid], 0, 1, lambda y, x: True),
        shift(near[3][mid:], 0, -1, lambda y, x: y > 1),
    )
    state = attend(query_cols, gate_mix, near, 1, state)
    far, state, early = lax.optimization_barrier((far, state, early))
    head_out = attend(query_cols, gate_mix, far, 2, state, head_gain.reshape(1, HD))
    return head_out, early


def expert_kernel(*refs, sizes):
    count = len(sizes)
    rows = refs[:count]
    gate_a, gate_b, up_a, up_b, down_a, down_b = refs[count : count + 6]
    out, joined = refs[count + 6 :]
    at = 0
    for part, size in zip(rows, sizes):
        joined[at : at + size, :] = part[...]
        at += size

    def block(i, carry):
        spot = pl.ds(pl.multiple_of(i * 128, 128), 128)
        mine = joined[spot, :]
        hidden = []
        for gate, up in ((gate_a, up_a), (gate_b, up_b)):
            gate_pre = jnp.dot(mine, gate[...], preferred_element_type=jnp.float32)
            up_pre = jnp.dot(mine, up[...], preferred_element_type=jnp.float32)
            silu = gate_pre / (1.0 + jnp.exp(-gate_pre))
            hidden.append((silu * up_pre).astype(jnp.bfloat16))
        step = 512
        for col in range(0, out.shape[1], step):
            part = jnp.dot(
                hidden[0], down_a[:, col : col + step], preferred_element_type=jnp.float32
            ) + jnp.dot(hidden[1], down_b[:, col : col + step], preferred_element_type=jnp.float32)
            out[spot, col : col + step] = part.astype(jnp.bfloat16)
        return carry

    lax.fori_loop(0, at // 128, block, 0)


def expert_rows(rows, weights):
    sizes = tuple(part.shape[0] for part in rows)
    total, width = sum(sizes), rows[0].shape[1]
    hidden = weights[0].shape[1] * 2
    flops = 2 * total * width * hidden * 3
    return pl.pallas_call(
        partial(expert_kernel, sizes=sizes),
        out_shape=jax.ShapeDtypeStruct((total, width), jnp.bfloat16),
        in_specs=[vmem] * (len(rows) + 6),
        out_specs=vmem,
        scratch_shapes=[pltpu.VMEM((total, width), jnp.bfloat16)],
        compiler_params=pltpu.CompilerParams(vmem_limit_bytes=16 << 20),
        cost_estimate=pl.CostEstimate(flops=flops, transcendentals=0, bytes_accessed=6 << 20),
        name="experts%d" % total,
    )(*rows, *weights)


def added(left, right):
    return (left.astype(jnp.float32) + right.astype(jnp.float32)).astype(jnp.bfloat16)


def expert_sum(own, weights):
    def up(array):
        return lax.ppermute(array, "tp", z_perm(1))

    def down(array):
        return lax.ppermute(array, "tp", z_perm(-1))

    count = own.shape[0]
    half = count // 2
    low1, high1 = up(own), down(own)
    low2, high2 = up(low1), down(high1)
    parts_near = expert_rows([own, low1, high1], weights)
    low3, high3 = up(low2), down(high2)
    far_top, far_bottom = up(low3[:half]), down(high3[half:])
    parts_mid = expert_rows([low2, high2, low3, high3], weights)
    parts_far = expert_rows([far_top, far_bottom], weights)

    def block(parts, i):
        return parts[i * count : (i + 1) * count]

    from_top, from_bottom = up(parts_far[:half]), down(parts_far[half:])
    low, high = block(parts_mid, 2), block(parts_mid, 3)
    sum_high = jnp.concatenate([added(high[:half], from_top), high[half:]])
    sum_low = jnp.concatenate([low[:half], added(low[half:], from_bottom)])
    sum_high = added(up(sum_high), block(parts_mid, 1))
    sum_low = added(down(sum_low), block(parts_mid, 0))
    sum_high = added(up(sum_high), block(parts_near, 2))
    sum_low = added(down(sum_low), block(parts_near, 1))
    sum_high, sum_low = up(sum_high), down(sum_low)
    total = sum_high.astype(jnp.float32) + sum_low.astype(jnp.float32)
    return (total + block(parts_near, 0).astype(jnp.float32)).astype(jnp.bfloat16)


def place_rows(routing, slot_count, capacity):
    expert_count, row_count = slot_count // capacity, routing.shape[1]
    expert_id = lax.broadcasted_iota(jnp.int32, (expert_count, row_count), 0)
    chosen = [(routing[k : k + 1, :] == expert_id).astype(jnp.float32) for k in range(TOP)]
    before = lax.broadcasted_iota(jnp.int32, (row_count, row_count), 0)
    before = before < lax.broadcasted_iota(jnp.int32, (row_count, row_count), 1)
    before = before.astype(jnp.float32).astype(jnp.bfloat16)
    counts = jnp.dot(
        sum(chosen).astype(jnp.bfloat16), before, preferred_element_type=jnp.float32
    )
    slot_id = lax.broadcasted_iota(jnp.int32, (slot_count, row_count), 0)
    here = []
    for k in range(TOP):
        rank = jnp.sum(counts * chosen[k], axis=0, keepdims=True).astype(jnp.int32)
        here.append(slot_id == routing[k : k + 1, :] * capacity + rank)
    return here


def project_kernel(
    heads, out_weight, stream, norm_gain, routing, route_weights, resid_sum, outgoing, mixing, *scratch
):
    joined, held_weight, held_stream, held_gain, held_routing, held_routes, sems = scratch
    sources = ((stream, held_stream), (norm_gain, held_gain))
    sources += ((routing, held_routing), (route_weights, held_routes))
    pieces = sems.shape[0] - len(sources)
    tall = out_weight.shape[0] // pieces
    copies = []
    for i in range(pieces):
        spot = pl.ds(i * tall, tall)
        copies.append(
            pltpu.make_async_copy(out_weight.at[spot], held_weight.at[spot], sems.at[i])
        )
    for source, into in sources:
        copies.append(pltpu.make_async_copy(source, into, sems.at[len(copies)]))
    for copy in copies[pieces:] + copies[:pieces]:
        copy.start()
    for head in range(heads.shape[0]):
        joined[:, head * HD : (head + 1) * HD] = heads[head]
    for copy in copies[pieces:]:
        copy.wait()
    slot_count = mixing.shape[0]
    experts = slot_count // max(2, 2 * TOP * stream.shape[0] // lax.axis_size("sp"))
    here = place_rows(held_routing[...], slot_count, slot_count // experts)
    mix = jnp.zeros(mixing.shape, jnp.float32)
    place = jnp.zeros(mixing.shape, jnp.float32)
    for k in range(TOP):
        mix = jnp.where(here[k], held_routes[k : k + 1, :], mix)
        place = jnp.where(here[k], 1.0, place)
    mixing[...] = mix
    mixed_rows = None
    for i in range(pieces):
        copies[i].wait()
        part = jnp.dot(
            joined[:, i * tall : (i + 1) * tall],
            held_weight[i * tall : (i + 1) * tall, :],
            preferred_element_type=jnp.float32,
        )
        mixed_rows = part if mixed_rows is None else mixed_rows + part
    resid = held_stream[...].astype(jnp.float32) + mixed_rows
    resid_sum[...] = resid
    center = resid - jnp.mean(resid, axis=1, keepdims=True)
    spread = jnp.mean(center * center, axis=1, keepdims=True)
    normed = (center * lax.rsqrt(spread + 1e-05) * held_gain[...]).astype(jnp.bfloat16)
    outgoing[...] = jnp.dot(
        place.astype(jnp.bfloat16), normed, preferred_element_type=jnp.float32
    ).astype(jnp.bfloat16)


def project(heads, out_weight, stream, norm_gain, routing, route_weights, slot_count):
    rows, width = stream.shape
    anywhere = pl.BlockSpec(memory_space=pltpu.HBM)
    return pl.pallas_call(
        project_kernel,
        out_shape=(
            jax.ShapeDtypeStruct((rows, width), jnp.float32),
            jax.ShapeDtypeStruct((slot_count, width), jnp.bfloat16),
            jax.ShapeDtypeStruct((slot_count, rows), jnp.float32),
        ),
        in_specs=[vmem] + [anywhere] * 5,
        out_specs=(vmem,) * 3,
        scratch_shapes=[
            pltpu.VMEM((rows, heads.shape[0] * HD), jnp.bfloat16),
            pltpu.VMEM(out_weight.shape, jnp.bfloat16),
            pltpu.VMEM(stream.shape, jnp.bfloat16),
            pltpu.VMEM((1, width), jnp.float32),
            pltpu.VMEM((TOP, rows), jnp.int32),
            pltpu.VMEM((TOP, rows), jnp.float32),
            pltpu.SemaphoreType.DMA((12,)),
        ],
        compiler_params=pltpu.CompilerParams(vmem_limit_bytes=14 << 20),
        name="project",
    )(
        heads,
        out_weight,
        stream,
        norm_gain.reshape(1, width),
        jnp.transpose(routing),
        jnp.transpose(route_weights),
    )


def combine_kernel(resid_sum, returned, mixing, out):
    total = resid_sum[...]
    for part in three_parts(mixing[...]):
        total = total + lax.dot_general(
            part, returned[...], (((0,), (0,)), ((), ())), preferred_element_type=jnp.float32
        )
    out[...] = total.astype(jnp.bfloat16)


def combine(resid_sum, returned, mixing):
    return pl.pallas_call(
        combine_kernel,
        out_shape=jax.ShapeDtypeStruct(resid_sum.shape, jnp.bfloat16),
        in_specs=[vmem] * 3,
        out_specs=vmem,
        compiler_params=pltpu.CompilerParams(vmem_limit_bytes=6 << 20),
        name="combine",
    )(resid_sum, returned, mixing)


def on_device(
    queries,
    key_vectors,
    value_vectors,
    forget_totals,
    head_gain,
    stream,
    out_weight,
    norm_gain,
    routing,
    route_weights,
    gate_weight,
    up_weight,
    down_weight,
):
    sp_count = lax.axis_size("sp")
    own_weights = (gate_weight[0], up_weight[0], down_weight[0])
    other_weights = tuple(lax.ppermute(weight, "tp", core_swap) for weight in own_weights)
    head_out, other_weights = attention(
        queries, key_vectors, value_vectors, forget_totals, head_gain, other_weights
    )
    weights = []
    for mine, other in zip(own_weights, other_weights):
        weights += [mine, other]
    row_count, width = stream.shape
    capacity = max(2, 2 * TOP * row_count // sp_count)
    heads = head_out.reshape(-1, row_count, HD)
    heads = lax.all_to_all(heads, "tp", split_axis=0, concat_axis=0, tiled=True)
    resid_sum, outgoing, mixing = project(
        heads, out_weight, stream, norm_gain, routing, route_weights, sp_count * capacity
    )
    outgoing = outgoing.reshape(sp_count, capacity, width)
    arrived = lax.all_to_all(outgoing, "sp", split_axis=0, concat_axis=0, tiled=True)
    summed = expert_sum(arrived.reshape(-1, width), weights)
    expert_out = summed.reshape(sp_count, capacity, width)
    returned = lax.all_to_all(expert_out, "sp", split_axis=0, concat_axis=0, tiled=True)
    return combine(resid_sum, returned.reshape(-1, width), mixing)


def solution(mesh):
    in_specs = (
        P("sp", "tp"),
        P("sp", "tp"),
        P("sp", "tp"),
        P("sp", "tp"),
        P("tp"),
        P(("sp", "tp"), None),
        P(),
        P(),
        P(("sp", "tp"), None),
        P(("sp", "tp"), None),
        P("sp", None, "tp"),
        P("sp", None, "tp"),
        P("sp", "tp", None),
    )
    out_specs = P(("sp", "tp"), None)
    return jax.shard_map(
        on_device, mesh=mesh, in_specs=in_specs, out_specs=out_specs, check_vma=False
    )
```

```python
from functools import partial

import jax
import jax.numpy as jnp
from jax import lax
from jax.experimental import pallas as pl
from jax.experimental.pallas import tpu as pltpu
from jax.sharding import PartitionSpec as P


HD = 128
TOP = 2
LOG2E = 1.4426950408889634
low_score = -1e30
GATE_ROWS = 16
KEYS = 256
PIECE = KEYS + GATE_ROWS
BLOCK = 2 * PIECE
PACK = HD + GATE_ROWS


def sp_perm(dy, dx, needed):
    pairs = []
    for y in range(4):
        for x in range(4):
            into = (y + dy) % 4, (x + dx) % 4
            if needed(*into):
                pairs.append((y * 4 + x, into[0] * 4 + into[1]))
    return pairs


def z_perm(dz):
    return [(z * 2 + c, ((z + dz) % 8) * 2 + c) for z in range(8) for c in range(2)]


core_swap = [(i, i ^ 1) for i in range(16)]


vmem = pl.BlockSpec(memory_space=pltpu.VMEM)


def three_parts(wide):
    first = wide.astype(jnp.bfloat16)
    rest = wide - first.astype(jnp.float32)
    second = rest.astype(jnp.bfloat16)
    third = (rest - second.astype(jnp.float32)).astype(jnp.bfloat16)
    return first, second, third


def piece_kernel(*refs):
    sources, outs, staged, sems = refs[:4], refs[4:6], refs[6:10], refs[10]
    copies = [
        pltpu.make_async_copy(source, into, sems.at[i])
        for i, (source, into) in enumerate(zip(sources, staged))
    ]
    for copy in copies:
        copy.start()
    for copy in copies:
        copy.wait()
    queries, keys, values, gates = staged
    keys_own, query_pack = outs
    stretched = gates[...] * HD**0.5
    tok_count = stretched.shape[1]
    row = lax.broadcasted_iota(jnp.int32, (GATE_ROWS, KEYS), 0)
    for i in range(2):
        at_row = i * PIECE
        rows = slice(i * KEYS, (i + 1) * KEYS)
        keys_own[at_row : at_row + HD, :] = jnp.transpose(values[rows, :])
        keys_own[at_row + HD : at_row + KEYS, 0:HD] = keys[i * KEYS : i * KEYS + HD, :]
        keys_own[at_row + HD : at_row + KEYS, HD:KEYS] = keys[i * KEYS + HD : (i + 1) * KEYS, :]
        parts = [part.astype(jnp.float32) for part in three_parts(-stretched[:, rows])]
        block = jnp.where((row >= 3) & (row < 6), 1.0, 0.0)
        for at, part in enumerate(parts):
            block = jnp.where(row == at, part, block)
        keys_own[at_row + KEYS : at_row + PIECE, :] = block.astype(jnp.bfloat16)
    wide_row = lax.broadcasted_iota(jnp.int32, (GATE_ROWS, tok_count), 0)
    mix = jnp.where(wide_row < 3, 1.0, 0.0)
    parts = [part.astype(jnp.float32) for part in three_parts(stretched[:, 0:1])]
    for at, part in enumerate(parts):
        mix = jnp.where(wide_row == 3 + at, part, mix)
    mix = jnp.where(wide_row == 6, low_score, mix)
    query_pack[HD:PACK, :] = mix.astype(jnp.bfloat16)
    query_pack[0:HD, :] = jnp.transpose(queries[...])


def make_pieces(queries, keys, values, gates):
    tok_count = queries.shape[0]
    return pl.pallas_call(
        piece_kernel,
        out_shape=(
            jax.ShapeDtypeStruct((BLOCK, 2 * HD), jnp.bfloat16),
            jax.ShapeDtypeStruct((PACK, tok_count), jnp.bfloat16),
        ),
        in_specs=[pl.BlockSpec(memory_space=pltpu.HBM)] * 4,
        out_specs=(vmem,) * 2,
        scratch_shapes=[pltpu.VMEM((tok_count, HD), jnp.bfloat16)] * 3
        + [pltpu.VMEM((1, tok_count), jnp.float32), pltpu.SemaphoreType.DMA((4,))],
        compiler_params=pltpu.CompilerParams(vmem_limit_bytes=6 << 20),
        name="make_pieces",
    )(queries, keys, values, gates.reshape(1, tok_count))


def fold(query_pack, state, pieces, own_block=False):
    run_max, run_sum, run_acc = state
    tok_count = query_pack.shape[1]
    scale = HD ** (-0.5) * LOG2E
    scores = []
    for i, (keys_in, at) in enumerate(pieces):
        bias = lax.dot_general(
            keys_in[pl.ds(at + KEYS, GATE_ROWS), :],
            query_pack[HD:PACK, :],
            (((0,), (0,)), ((), ())),
            preferred_element_type=jnp.float32,
        )
        for part in range(KEYS // HD):
            keys = keys_in[pl.ds(at + HD, HD), part * HD : (part + 1) * HD]
            score = jnp.dot(keys, query_pack[0:HD, :], preferred_element_type=jnp.float32)
            score = score + bias[part * HD : (part + 1) * HD]
            if own_block:
                key_at = lax.broadcasted_iota(jnp.int32, score.shape, 0)
                key_at = key_at + (i * KEYS + part * HD)
                query_at = lax.broadcasted_iota(jnp.int32, score.shape, 1)
                score = jnp.where(key_at <= query_at, score, low_score)
            scores.append(score)
    old_max = run_max[0:1, :]
    peak = scores[0]
    for score in scores[1:]:
        peak = jnp.maximum(peak, score)
    new_max = jnp.maximum(old_max, jnp.max(peak, axis=0, keepdims=True))
    rescale = jnp.exp2((old_max - new_max) * scale)
    scaled_max = new_max * scale
    total = run_sum[...] * rescale
    acc = run_acc[...] * rescale
    for i, (keys_in, at) in enumerate(pieces):
        rounded = []
        for score in scores[2 * i : 2 * i + 2]:
            lifted = jnp.exp2(score * scale - scaled_max)
            total = total + jnp.sum(lifted.reshape(HD // 8, 8, tok_count), axis=0)
            rounded.append(lifted.astype(jnp.bfloat16))
        acc = acc + jnp.dot(
            keys_in[pl.ds(at, HD), :],
            jnp.concatenate(rounded, axis=0),
            preferred_element_type=jnp.float32,
        )
    run_sum[...] = total
    run_acc[...] = acc
    run_max[...] = jnp.broadcast_to(new_max, run_max.shape)


def clear(state):
    run_max, run_sum, run_acc = state
    run_max[...] = jnp.full_like(run_max, low_score)
    run_sum[...] = jnp.zeros_like(run_sum)
    run_acc[...] = jnp.zeros_like(run_acc)


def fold_blocks(query_pack, state, stack, first, count, seen=None):
    def block(i, carry):
        at = pl.multiple_of(i * BLOCK, 32)

        def run():
            fold(query_pack, state, [(stack, at), (stack, at + PIECE)])

        if seen is None:
            run()
        else:
            pl.when(seen(i))(run)
        return carry

    lax.fori_loop(first, first + count, block, 0)


def pack_result(state, out):
    run_max, run_sum, run_acc = state
    total = jnp.sum(run_sum[...], axis=0, keepdims=True)
    out[0:HD, :] = (run_acc[...] / total).astype(jnp.bfloat16)
    row = lax.broadcasted_iota(jnp.int32, (GATE_ROWS, total.shape[1]), 0)
    block = jnp.zeros(row.shape, jnp.float32)
    for at, part in enumerate(three_parts(run_max[0:1, :]) + three_parts(total)):
        block = jnp.where(row == at, part.astype(jnp.float32), block)
    out[HD:PACK, :] = block.astype(jnp.bfloat16)


def fill(stack, parts):
    at = 0
    for part in parts:
        stack[at : at + part.shape[0], :] = part[...]
        at += part.shape[0]


def distant_kernel(*refs):
    packs, keys, states, stack = refs[:2], refs[2:5], (refs[5:8], refs[8:11]), refs[11]
    own_y = lax.axis_index("sp") >> 2
    fill(stack, keys)
    for pack, state, above in zip(packs, states, (3, 2)):

        @pl.when(own_y + above <= 3)
        def _():
            clear(state)
            fold_blocks(pack, state, stack, 0, 3)


def distant_end_kernel(*refs):
    packs, far, states_in, outs = refs[:2], refs[2:4], (refs[4:7], refs[7:10]), refs[10:12]
    state = refs[12:15]
    own_y = lax.axis_index("sp") >> 2
    for pack, state_in, out, above in zip(packs, states_in, outs, (3, 2)):

        @pl.when(own_y + above <= 3)
        def _():
            for into, came in zip(state, state_in):
                into[...] = came[...]
            fold(pack, state, [(far[0], 0), (far[1], 0)])
            pack_result(state, out)


def close_kernel(*refs):
    next_pack, own_pack = refs[:2]
    keys, out, own_state = refs[2:7], refs[7], refs[8:11]
    state, stack = refs[11:14], refs[14]
    own = lax.axis_index("sp")
    own_x = own & 3
    fill(stack, keys)

    @pl.when(own < 12)
    def _():
        clear(state)
        fold_blocks(next_pack, state, stack, 0, 4)
        pack_result(state, out)

    clear(own_state)
    fold(own_pack, own_state, [(keys[0], 0), (keys[0], PIECE)], own_block=True)

    def seen(i):
        move = jnp.where(i == 1, -1, jnp.where(i == 2, 1, 2))
        return ((own_x + move) & 3) < own_x

    fold_blocks(own_pack, own_state, stack, 1, 3, seen)


def merge_kernel(*refs):
    came, own_state, gain, head_out = refs[:3], refs[3:6], refs[6], refs[7]
    own_y = lax.axis_index("sp") >> 2
    scale = HD ** (-0.5) * LOG2E
    peaks = [own_state[0][0:1, :]]
    totals = [jnp.sum(own_state[1][...], axis=0, keepdims=True)]
    for above, pack in enumerate(came):
        rows = pack[HD:PACK, :].astype(jnp.float32)
        parts = [rows[at : at + 1, :] for at in range(6)]
        valid = own_y > above
        peaks.append(jnp.where(valid, parts[0] + parts[1] + parts[2], low_score))
        totals.append(jnp.where(valid, parts[3] + parts[4] + parts[5], 0.0))
    top = peaks[0]
    for peak in peaks[1:]:
        top = jnp.maximum(top, peak)
    weight = jnp.exp2((peaks[0] - top) * scale)
    total = totals[0] * weight
    acc = own_state[2][...] * weight
    for pack, peak, share in zip(came, peaks[1:], totals[1:]):
        weight = share * jnp.exp2((peak - top) * scale)
        total = total + weight
        acc = acc + pack[0:HD, :].astype(jnp.float32) * weight
    attended = acc / total
    mean_square = jnp.mean(attended * attended, axis=0, keepdims=True)
    normed = jnp.transpose(attended * lax.rsqrt(mean_square + 1e-06))
    head_out[...] = (normed * gain[...]).astype(jnp.bfloat16)


def attend(kernel, operands, outs, scratch, folds):
    tok_count = 2 * KEYS
    return pl.pallas_call(
        kernel,
        out_shape=tuple(jax.ShapeDtypeStruct(*out) for out in outs),
        in_specs=[vmem] * len(operands),
        out_specs=(vmem,) * len(outs),
        scratch_shapes=[pltpu.VMEM(*shape) for shape in scratch],
        compiler_params=pltpu.CompilerParams(vmem_limit_bytes=12 << 20),
        cost_estimate=pl.CostEstimate(
            flops=8 * tok_count * tok_count * HD * folds,
            transcendentals=tok_count * tok_count * folds,
            bytes_accessed=1 << 20,
        ),
    )(*operands)


def attention(queries, key_vectors, value_vectors, forget_totals, head_gain, early):
    tok_count = queries.shape[0]

    def shift(array, dy, dx, needed):
        return lax.ppermute(array, "sp", sp_perm(dy, dx, needed))

    keys_own, own_pack = make_pieces(queries, key_vectors, value_vectors, forget_totals)
    low = shift(keys_own, 0, 1, lambda y, x: y < 3 or x > 0)
    high = shift(keys_own, 0, -1, lambda y, x: y < 3 or x in (0, 3))
    pack3 = shift(own_pack, 1, 0, lambda y, x: y == 0)
    pack2 = shift(own_pack, 2, 0, lambda y, x: y < 2)
    pack1 = shift(own_pack, -1, 0, lambda y, x: y < 3)
    far_a = shift(low[:PIECE], 0, 1, lambda y, x: y < 3 or x > 1)
    far_b = shift(high[PIECE:], 0, -1, lambda y, x: y < 3 or x > 1)

    narrow = ((8, tok_count), jnp.float32)
    state = [narrow, narrow, ((HD, tok_count), jnp.float32)]
    result = ((PACK, tok_count), jnp.bfloat16)

    def stack(count):
        return ((count * BLOCK, 2 * HD), jnp.bfloat16)

    near = attend(distant_kernel, [pack3, pack2, keys_own, low, high], state * 2, [stack(3)], 6)
    far_a, far_b, near, early = lax.optimization_barrier((far_a, far_b, near, early))
    part3, part2 = attend(
        distant_end_kernel, [pack3, pack2, far_a, far_b, *near], [result] * 2, state, 2
    )
    part3, part2, pack1 = lax.optimization_barrier((part3, part2, pack1))
    back3 = shift(part3, -1, 0, lambda y, x: y == 3)
    back2 = shift(part2, 2, 0, lambda y, x: y > 1)
    part1, *own_state = attend(
        close_kernel,
        [pack1, own_pack, keys_own, low, high, far_a, far_b],
        [result] + state,
        state + [stack(4)],
        8,
    )
    back1 = shift(part1, 1, 0, lambda y, x: y > 0)
    (head_out,) = attend(
        merge_kernel,
        [back1, back2, back3, *own_state, head_gain.reshape(1, HD)],
        [((tok_count, HD), jnp.bfloat16)],
        [],
        0,
    )
    return head_out, early


def expert_kernel(*refs, count):
    rows = refs[:count]
    gate_a, gate_b, up_a, up_b, down_a, down_b = refs[count : count + 6]
    outs = refs[count + 6 : 2 * count + 6]
    joined, made = refs[2 * count + 6 :]
    each = rows[0].shape[0]
    for i, part in enumerate(rows):
        joined[i * each : (i + 1) * each, :] = part[...]
    tall, wide = 128, 512

    def block(i, carry):
        spot = pl.ds(pl.multiple_of(i * tall, tall), tall)
        mine = joined[spot, :]
        hidden = []
        for gate, up in ((gate_a, up_a), (gate_b, up_b)):
            gate_pre = jnp.dot(mine, gate[...], preferred_element_type=jnp.float32)
            up_pre = jnp.dot(mine, up[...], preferred_element_type=jnp.float32)
            silu = gate_pre / (1.0 + jnp.exp(-gate_pre))
            hidden.append((silu * up_pre).astype(jnp.bfloat16))

        def column(j, inner):
            cols = pl.ds(pl.multiple_of(j * wide, wide), wide)
            part = jnp.dot(
                hidden[0], down_a[:, cols], preferred_element_type=jnp.float32
            ) + jnp.dot(hidden[1], down_b[:, cols], preferred_element_type=jnp.float32)
            made[spot, cols] = part.astype(jnp.bfloat16)
            return inner

        return lax.fori_loop(0, made.shape[1] // wide, column, carry)

    lax.fori_loop(0, joined.shape[0] // tall, block, 0)
    for i, out in enumerate(outs):
        out[...] = made[i * each : (i + 1) * each, :]


def expert_rows(rows, weights):
    count = len(rows)
    each, width = rows[0].shape
    hidden = weights[0].shape[1] * 2
    flops = 2 * count * each * width * hidden * 3
    joined = pltpu.VMEM((count * each, width), jnp.bfloat16)
    return pl.pallas_call(
        partial(expert_kernel, count=count),
        out_shape=tuple(jax.ShapeDtypeStruct((each, width), jnp.bfloat16) for _ in rows),
        in_specs=[vmem] * (count + 6),
        out_specs=(vmem,) * count,
        scratch_shapes=[joined, joined],
        compiler_params=pltpu.CompilerParams(vmem_limit_bytes=16 << 20),
        cost_estimate=pl.CostEstimate(flops=flops, transcendentals=0, bytes_accessed=6 << 20),
    )(*rows, *weights)


def added(left, right):
    return (left.astype(jnp.float32) + right.astype(jnp.float32)).astype(jnp.bfloat16)


def expert_sum(own, weights):
    def up(array):
        return lax.ppermute(array, "tp", z_perm(1))

    def down(array):
        return lax.ppermute(array, "tp", z_perm(-1))

    half = own.shape[0] // 2
    top, end = own[:half], own[half:]
    up_top, down_end, up_end, down_top = [up(top)], [down(end)], [up(end)], [down(top)]
    for _ in range(2):
        up_top.append(up(up_top[-1]))
        down_end.append(down(down_end[-1]))
        up_end.append(up(up_end[-1]))
        down_top.append(down(down_top[-1]))
    up_top.append(up(up_top[-1]))
    down_end.append(down(down_end[-1]))
    chains = (up_top, up_end, down_top, down_end)
    near = expert_rows([top, end] + [chain[0] for chain in chains], weights)
    mid = expert_rows([chain[i] for i in (1, 2) for chain in chains], weights)
    far_top, far_end = expert_rows([up_top[3], down_end[3]], weights)
    done = [near[2:], mid[:4], mid[4:]]

    low_top, high_end = down(done[2][0]), up(done[2][3])
    high_top, low_end = up(far_top), down(far_end)
    high_top = up(added(high_top, done[2][2]))
    low_end = down(added(low_end, done[2][1]))
    for i in (1, 0):
        low_top = down(added(low_top, done[i][0]))
        high_end = up(added(high_end, done[i][3]))
        high_top = up(added(high_top, done[i][2]))
        low_end = down(added(low_end, done[i][1]))
    sums = []
    for parts in ((low_top, high_top, near[0]), (low_end, high_end, near[1])):
        low, high, mine = (part.astype(jnp.float32) for part in parts)
        sums.append((low + high + mine).astype(jnp.bfloat16))
    return jnp.concatenate(sums)


def place_rows(routing, slot_count, capacity):
    expert_count, row_count = slot_count // capacity, routing.shape[1]
    expert_id = lax.broadcasted_iota(jnp.int32, (expert_count, row_count), 0)
    chosen = [(routing[k : k + 1, :] == expert_id).astype(jnp.float32) for k in range(TOP)]
    before = lax.broadcasted_iota(jnp.int32, (row_count, row_count), 0)
    before = before < lax.broadcasted_iota(jnp.int32, (row_count, row_count), 1)
    before = before.astype(jnp.float32).astype(jnp.bfloat16)
    counts = jnp.dot(
        sum(chosen).astype(jnp.bfloat16), before, preferred_element_type=jnp.float32
    )
    slot_id = lax.broadcasted_iota(jnp.int32, (slot_count, row_count), 0)
    here = []
    for k in range(TOP):
        rank = jnp.sum(counts * chosen[k], axis=0, keepdims=True).astype(jnp.int32)
        here.append(slot_id == routing[k : k + 1, :] * capacity + rank)
    return here


def project_kernel(
    heads, out_weight, stream, norm_gain, routing, route_weights, resid_sum, outgoing, mixing, joined
):
    for head in range(heads.shape[0]):
        joined[:, head * HD : (head + 1) * HD] = heads[head]
    slot_count = mixing.shape[0]
    experts = slot_count // max(2, 2 * TOP * stream.shape[0] // lax.axis_size("sp"))
    here = place_rows(routing[...], slot_count, slot_count // experts)
    mix = jnp.zeros(mixing.shape, jnp.float32)
    place = jnp.zeros(mixing.shape, jnp.float32)
    for k in range(TOP):
        mix = jnp.where(here[k], route_weights[k : k + 1, :], mix)
        place = jnp.where(here[k], 1.0, place)
    mixing[...] = mix
    wide = 512

    def column(j, carry):
        cols = pl.ds(pl.multiple_of(j * wide, wide), wide)
        mixed_rows = jnp.dot(joined[...], out_weight[:, cols], preferred_element_type=jnp.float32)
        resid_sum[:, cols] = stream[:, cols].astype(jnp.float32) + mixed_rows
        return carry

    lax.fori_loop(0, resid_sum.shape[1] // wide, column, 0)
    resid = resid_sum[...]
    center = resid - jnp.mean(resid, axis=1, keepdims=True)
    spread = jnp.mean(center * center, axis=1, keepdims=True)
    normed = (center * lax.rsqrt(spread + 1e-05) * norm_gain[...]).astype(jnp.bfloat16)
    outgoing[...] = jnp.dot(
        place.astype(jnp.bfloat16), normed, preferred_element_type=jnp.float32
    ).astype(jnp.bfloat16)


def project(heads, out_weight, stream, norm_gain, routing, route_weights, slot_count):
    rows, width = stream.shape
    return pl.pallas_call(
        project_kernel,
        out_shape=(
            jax.ShapeDtypeStruct((rows, width), jnp.float32),
            jax.ShapeDtypeStruct((slot_count, width), jnp.bfloat16),
            jax.ShapeDtypeStruct((slot_count, rows), jnp.float32),
        ),
        in_specs=[vmem] * 6,
        out_specs=(vmem,) * 3,
        scratch_shapes=[pltpu.VMEM((rows, heads.shape[0] * HD), jnp.bfloat16)],
        compiler_params=pltpu.CompilerParams(vmem_limit_bytes=14 << 20),
        name="project",
    )(
        heads,
        out_weight,
        stream,
        norm_gain.reshape(1, width),
        jnp.transpose(routing),
        jnp.transpose(route_weights),
    )


def combine_kernel(resid_sum, returned, mixing, out):
    total = resid_sum[...]
    for part in three_parts(mixing[...]):
        total = total + lax.dot_general(
            part, returned[...], (((0,), (0,)), ((), ())), preferred_element_type=jnp.float32
        )
    out[...] = total.astype(jnp.bfloat16)


def combine(resid_sum, returned, mixing):
    return pl.pallas_call(
        combine_kernel,
        out_shape=jax.ShapeDtypeStruct(resid_sum.shape, jnp.bfloat16),
        in_specs=[vmem] * 3,
        out_specs=vmem,
        compiler_params=pltpu.CompilerParams(vmem_limit_bytes=6 << 20),
        name="combine",
    )(resid_sum, returned, mixing)


def on_device(
    queries,
    key_vectors,
    value_vectors,
    forget_totals,
    head_gain,
    stream,
    out_weight,
    norm_gain,
    routing,
    route_weights,
    gate_weight,
    up_weight,
    down_weight,
):
    sp_count = lax.axis_size("sp")
    own_weights = (gate_weight[0], up_weight[0], down_weight[0])
    other_weights = tuple(lax.ppermute(weight, "tp", core_swap) for weight in own_weights)
    head_out, other_weights = attention(
        queries, key_vectors, value_vectors, forget_totals, head_gain, other_weights
    )
    weights = []
    for mine, other in zip(own_weights, other_weights):
        weights += [mine, other]
    row_count, width = stream.shape
    capacity = max(2, 2 * TOP * row_count // sp_count)
    heads = head_out.reshape(-1, row_count, HD)
    heads = lax.all_to_all(heads, "tp", split_axis=0, concat_axis=0, tiled=True)
    resid_sum, outgoing, mixing = project(
        heads, out_weight, stream, norm_gain, routing, route_weights, sp_count * capacity
    )
    outgoing = outgoing.reshape(sp_count, capacity, width)
    arrived = lax.all_to_all(outgoing, "sp", split_axis=0, concat_axis=0, tiled=True)
    summed = expert_sum(arrived.reshape(-1, width), weights)
    expert_out = summed.reshape(sp_count, capacity, width)
    returned = lax.all_to_all(expert_out, "sp", split_axis=0, concat_axis=0, tiled=True)
    return combine(resid_sum, returned.reshape(-1, width), mixing)


def solution(mesh):
    in_specs = (
        P("sp", "tp"),
        P("sp", "tp"),
        P("sp", "tp"),
        P("sp", "tp"),
        P("tp"),
        P(("sp", "tp"), None),
        P(),
        P(),
        P(("sp", "tp"), None),
        P(("sp", "tp"), None),
        P("sp", None, "tp"),
        P("sp", None, "tp"),
        P("sp", "tp", None),
    )
    out_specs = P(("sp", "tp"), None)
    return jax.shard_map(
        on_device, mesh=mesh, in_specs=in_specs, out_specs=out_specs, check_vma=False
    )
```

```python
from functools import partial

import jax
import jax.numpy as jnp
from jax import lax
from jax.experimental import pallas as pl
from jax.experimental.pallas import tpu as pltpu
from jax.sharding import PartitionSpec as P


HD = 128
TOP = 2
LOG2E = 1.4426950408889634
low_score = -1e30
GATE_ROWS = 16
KEYS = 256
PIECE = KEYS + GATE_ROWS
BLOCK = 2 * PIECE
PACK = HD + GATE_ROWS


def sp_perm(dy, dx, needed):
    pairs = []
    for y in range(4):
        for x in range(4):
            into = (y + dy) % 4, (x + dx) % 4
            if needed(*into):
                pairs.append((y * 4 + x, into[0] * 4 + into[1]))
    return pairs


def z_perm(dz):
    return [(z * 2 + c, ((z + dz) % 8) * 2 + c) for z in range(8) for c in range(2)]


core_swap = [(i, i ^ 1) for i in range(16)]


vmem = pl.BlockSpec(memory_space=pltpu.VMEM)


def in_hbm(*arrays):
    return [pltpu.with_memory_space_constraint(array, pltpu.HBM) for array in arrays]


def three_parts(wide):
    first = wide.astype(jnp.bfloat16)
    rest = wide - first.astype(jnp.float32)
    second = rest.astype(jnp.bfloat16)
    third = (rest - second.astype(jnp.float32)).astype(jnp.bfloat16)
    return first, second, third


def piece_kernel(*refs):
    sources, outs, staged, sems = refs[:4], refs[4:6], refs[6:10], refs[10]
    copies = [
        pltpu.make_async_copy(source, into, sems.at[i])
        for i, (source, into) in enumerate(zip(sources, staged))
    ]
    for copy in copies:
        copy.start()
    for copy in copies:
        copy.wait()
    queries, keys, values, gates = staged
    keys_own, query_pack = outs
    stretched = gates[...] * HD**0.5
    tok_count = stretched.shape[1]
    row = lax.broadcasted_iota(jnp.int32, (GATE_ROWS, KEYS), 0)
    for i in range(2):
        at_row = i * PIECE
        rows = slice(i * KEYS, (i + 1) * KEYS)
        keys_own[at_row : at_row + HD, :] = jnp.transpose(values[rows, :])
        keys_own[at_row + HD : at_row + KEYS, 0:HD] = keys[i * KEYS : i * KEYS + HD, :]
        keys_own[at_row + HD : at_row + KEYS, HD:KEYS] = keys[i * KEYS + HD : (i + 1) * KEYS, :]
        parts = [part.astype(jnp.float32) for part in three_parts(-stretched[:, rows])]
        block = jnp.where((row >= 3) & (row < 6), 1.0, 0.0)
        for at, part in enumerate(parts):
            block = jnp.where(row == at, part, block)
        keys_own[at_row + KEYS : at_row + PIECE, :] = block.astype(jnp.bfloat16)
    wide_row = lax.broadcasted_iota(jnp.int32, (GATE_ROWS, tok_count), 0)
    mix = jnp.where(wide_row < 3, 1.0, 0.0)
    parts = [part.astype(jnp.float32) for part in three_parts(stretched[:, 0:1])]
    for at, part in enumerate(parts):
        mix = jnp.where(wide_row == 3 + at, part, mix)
    mix = jnp.where(wide_row == 6, low_score, mix)
    query_pack[HD:PACK, :] = mix.astype(jnp.bfloat16)
    query_pack[0:HD, :] = jnp.transpose(queries[...])


def make_pieces(queries, keys, values, gates):
    tok_count = queries.shape[0]
    return pl.pallas_call(
        piece_kernel,
        out_shape=(
            jax.ShapeDtypeStruct((BLOCK, 2 * HD), jnp.bfloat16),
            jax.ShapeDtypeStruct((PACK, tok_count), jnp.bfloat16),
        ),
        in_specs=[pl.BlockSpec(memory_space=pltpu.HBM)] * 4,
        out_specs=(vmem,) * 2,
        scratch_shapes=[pltpu.VMEM((tok_count, HD), jnp.bfloat16)] * 3
        + [pltpu.VMEM((1, tok_count), jnp.float32), pltpu.SemaphoreType.DMA((4,))],
        compiler_params=pltpu.CompilerParams(vmem_limit_bytes=6 << 20),
        name="make_pieces",
    )(*in_hbm(queries, keys, values, gates.reshape(1, tok_count)))


def fold(query_pack, state, pieces, own_block=False):
    run_max, run_sum, run_acc = state
    tok_count = query_pack.shape[1]
    scale = HD ** (-0.5) * LOG2E
    scores = []
    for i, (keys_in, at) in enumerate(pieces):
        bias = lax.dot_general(
            keys_in[pl.ds(at + KEYS, GATE_ROWS), :],
            query_pack[HD:PACK, :],
            (((0,), (0,)), ((), ())),
            preferred_element_type=jnp.float32,
        )
        for part in range(KEYS // HD):
            keys = keys_in[pl.ds(at + HD, HD), part * HD : (part + 1) * HD]
            score = jnp.dot(keys, query_pack[0:HD, :], preferred_element_type=jnp.float32)
            score = score + bias[part * HD : (part + 1) * HD]
            if own_block:
                key_at = lax.broadcasted_iota(jnp.int32, score.shape, 0)
                key_at = key_at + (i * KEYS + part * HD)
                query_at = lax.broadcasted_iota(jnp.int32, score.shape, 1)
                score = jnp.where(key_at <= query_at, score, low_score)
            scores.append(score)
    old_max = run_max[0:1, :]
    peak = scores[0]
    for score in scores[1:]:
        peak = jnp.maximum(peak, score)
    new_max = jnp.maximum(old_max, jnp.max(peak, axis=0, keepdims=True))
    rescale = jnp.exp2((old_max - new_max) * scale)
    scaled_max = new_max * scale
    total = run_sum[...] * rescale
    acc = run_acc[...] * rescale
    for i, (keys_in, at) in enumerate(pieces):
        rounded = []
        for score in scores[2 * i : 2 * i + 2]:
            lifted = jnp.exp2(score * scale - scaled_max)
            total = total + jnp.sum(lifted.reshape(HD // 8, 8, tok_count), axis=0)
            rounded.append(lifted.astype(jnp.bfloat16))
        acc = acc + jnp.dot(
            keys_in[pl.ds(at, HD), :],
            jnp.concatenate(rounded, axis=0),
            preferred_element_type=jnp.float32,
        )
    run_sum[...] = total
    run_acc[...] = acc
    run_max[...] = jnp.broadcast_to(new_max, run_max.shape)


def clear(state):
    run_max, run_sum, run_acc = state
    run_max[...] = jnp.full_like(run_max, low_score)
    run_sum[...] = jnp.zeros_like(run_sum)
    run_acc[...] = jnp.zeros_like(run_acc)


def fold_blocks(query_pack, state, stack, first, count, seen=None):
    def block(i, carry):
        at = pl.multiple_of(i * BLOCK, 32)

        def run():
            fold(query_pack, state, [(stack, at), (stack, at + PIECE)])

        if seen is None:
            run()
        else:
            pl.when(seen(i))(run)
        return carry

    lax.fori_loop(first, first + count, block, 0)


def pack_result(state, out):
    run_max, run_sum, run_acc = state
    total = jnp.sum(run_sum[...], axis=0, keepdims=True)
    out[0:HD, :] = (run_acc[...] / total).astype(jnp.bfloat16)
    row = lax.broadcasted_iota(jnp.int32, (GATE_ROWS, total.shape[1]), 0)
    block = jnp.zeros(row.shape, jnp.float32)
    for at, part in enumerate(three_parts(run_max[0:1, :]) + three_parts(total)):
        block = jnp.where(row == at, part.astype(jnp.float32), block)
    out[HD:PACK, :] = block.astype(jnp.bfloat16)


def fill(stack, parts):
    at = 0
    for part in parts:
        stack[at : at + part.shape[0], :] = part[...]
        at += part.shape[0]


def distant_kernel(*refs):
    packs, keys, states, stack = refs[:2], refs[2:5], (refs[5:8], refs[8:11]), refs[11]
    own_y = lax.axis_index("sp") >> 2
    fill(stack, keys)
    for pack, state, above in zip(packs, states, (3, 2)):

        @pl.when(own_y + above <= 3)
        def _():
            clear(state)
            fold_blocks(pack, state, stack, 0, 3)


def distant_end_kernel(*refs):
    packs, far, states_in, outs = refs[:2], refs[2:4], (refs[4:7], refs[7:10]), refs[10:12]
    state = refs[12:15]
    own_y = lax.axis_index("sp") >> 2
    for pack, state_in, out, above in zip(packs, states_in, outs, (3, 2)):

        @pl.when(own_y + above <= 3)
        def _():
            for into, came in zip(state, state_in):
                into[...] = came[...]
            fold(pack, state, [(far[0], 0), (far[1], 0)])
            pack_result(state, out)


def close_kernel(*refs):
    next_pack, own_pack = refs[:2]
    keys, out, own_state = refs[2:7], refs[7], refs[8:11]
    state, stack = refs[11:14], refs[14]
    own = lax.axis_index("sp")
    own_x = own & 3
    fill(stack, keys)

    @pl.when(own < 12)
    def _():
        clear(state)
        fold_blocks(next_pack, state, stack, 0, 4)
        pack_result(state, out)

    clear(own_state)
    fold(own_pack, own_state, [(keys[0], 0), (keys[0], PIECE)], own_block=True)

    def seen(i):
        move = jnp.where(i == 1, -1, jnp.where(i == 2, 1, 2))
        return ((own_x + move) & 3) < own_x

    fold_blocks(own_pack, own_state, stack, 1, 3, seen)


def merge_kernel(*refs):
    came, own_state, gain, head_out = refs[:3], refs[3:6], refs[6], refs[7]
    own_y = lax.axis_index("sp") >> 2
    scale = HD ** (-0.5) * LOG2E
    peaks = [own_state[0][0:1, :]]
    totals = [jnp.sum(own_state[1][...], axis=0, keepdims=True)]
    for above, pack in enumerate(came):
        rows = pack[HD:PACK, :].astype(jnp.float32)
        parts = [rows[at : at + 1, :] for at in range(6)]
        valid = own_y > above
        peaks.append(jnp.where(valid, parts[0] + parts[1] + parts[2], low_score))
        totals.append(jnp.where(valid, parts[3] + parts[4] + parts[5], 0.0))
    top = peaks[0]
    for peak in peaks[1:]:
        top = jnp.maximum(top, peak)
    weight = jnp.exp2((peaks[0] - top) * scale)
    total = totals[0] * weight
    acc = own_state[2][...] * weight
    for pack, peak, share in zip(came, peaks[1:], totals[1:]):
        weight = share * jnp.exp2((peak - top) * scale)
        total = total + weight
        acc = acc + pack[0:HD, :].astype(jnp.float32) * weight
    attended = acc / total
    mean_square = jnp.mean(attended * attended, axis=0, keepdims=True)
    normed = jnp.transpose(attended * lax.rsqrt(mean_square + 1e-06))
    head_out[...] = (normed * gain[...]).astype(jnp.bfloat16)


def attend(kernel, operands, outs, scratch, folds):
    tok_count = 2 * KEYS
    return pl.pallas_call(
        kernel,
        out_shape=tuple(jax.ShapeDtypeStruct(*out) for out in outs),
        in_specs=[vmem] * len(operands),
        out_specs=(vmem,) * len(outs),
        scratch_shapes=[pltpu.VMEM(*shape) for shape in scratch],
        compiler_params=pltpu.CompilerParams(vmem_limit_bytes=12 << 20),
        cost_estimate=pl.CostEstimate(
            flops=8 * tok_count * tok_count * HD * folds,
            transcendentals=tok_count * tok_count * folds,
            bytes_accessed=1 << 20,
        ),
    )(*operands)


def attention(queries, key_vectors, value_vectors, forget_totals, head_gain, weights):
    tok_count = queries.shape[0]

    def shift(array, dy, dx, needed):
        return lax.ppermute(array, "sp", sp_perm(dy, dx, needed))

    keys_own, own_pack = make_pieces(queries, key_vectors, value_vectors, forget_totals)
    low = shift(keys_own, 0, 1, lambda y, x: y < 3 or x > 0)
    high = shift(keys_own, 0, -1, lambda y, x: y < 3 or x in (0, 3))
    pack3 = shift(own_pack, 1, 0, lambda y, x: y == 0)
    pack2 = shift(own_pack, 2, 0, lambda y, x: y < 2)
    pack1 = shift(own_pack, -1, 0, lambda y, x: y < 3)
    far_a = shift(low[:PIECE], 0, 1, lambda y, x: y < 3 or x > 1)
    far_b = shift(high[PIECE:], 0, -1, lambda y, x: y < 3 or x > 1)

    narrow = ((8, tok_count), jnp.float32)
    state = [narrow, narrow, ((HD, tok_count), jnp.float32)]
    result = ((PACK, tok_count), jnp.bfloat16)

    def stack(count):
        return ((count * BLOCK, 2 * HD), jnp.bfloat16)

    near = attend(distant_kernel, [pack3, pack2, keys_own, low, high], state * 2, [stack(3)], 6)
    far_a, far_b, near = lax.optimization_barrier((far_a, far_b, near))
    part3, part2 = attend(
        distant_end_kernel, [pack3, pack2, far_a, far_b, *near], [result] * 2, state, 2
    )
    part3, part2, pack1 = lax.optimization_barrier((part3, part2, pack1))
    back3 = shift(part3, -1, 0, lambda y, x: y == 3)
    back2 = shift(part2, 2, 0, lambda y, x: y > 1)
    part1, *own_state = attend(
        close_kernel,
        [pack1, own_pack, keys_own, low, high, far_a, far_b],
        [result] + state,
        state + [stack(4)],
        8,
    )
    back1 = shift(part1, 1, 0, lambda y, x: y > 0)
    part1, weights = lax.optimization_barrier((part1, weights))
    staged = stage_weights(*weights)
    (head_out,) = attend(
        merge_kernel,
        [back1, back2, back3, *own_state, head_gain.reshape(1, HD)],
        [((tok_count, HD), jnp.bfloat16)],
        [],
        0,
    )
    return head_out, staged


def staging_kernel(gate, up, down, out, sems):
    tall, wide = gate.shape
    copies = [
        pltpu.make_async_copy(gate, out.at[pl.ds(0, tall)], sems.at[0]),
        pltpu.make_async_copy(up, out.at[pl.ds(tall, tall)], sems.at[1]),
    ]
    for i in range(down.shape[1] // wide):
        source = down.at[:, pl.ds(i * wide, wide)]
        into = out.at[pl.ds(2 * tall + i * down.shape[0], down.shape[0])]
        copies.append(pltpu.make_async_copy(source, into, sems.at[2 + i]))
    for copy in copies:
        copy.start()
    for copy in copies:
        copy.wait()


def stage_weights(gate, up, down):
    blocks = down.shape[1] // gate.shape[1]
    rows = 2 * gate.shape[0] + blocks * down.shape[0]
    return pl.pallas_call(
        staging_kernel,
        out_shape=jax.ShapeDtypeStruct((rows, gate.shape[1]), jnp.bfloat16),
        in_specs=[pl.BlockSpec(memory_space=pltpu.HBM)] * 3,
        out_specs=vmem,
        scratch_shapes=[pltpu.SemaphoreType.DMA((2 + blocks,))],
        compiler_params=pltpu.CompilerParams(vmem_limit_bytes=4 << 20),
        name="stage_weights",
    )(*in_hbm(gate, up, down))


def expert_kernel(*refs, count):
    rows, halves = refs[:count], refs[count : count + 2]
    outs = refs[count + 2 : 2 * count + 2]
    joined, made = refs[2 * count + 2 :]
    each, width = rows[0].shape
    units = halves[0].shape[1]
    for i, part in enumerate(rows):
        joined[i * each : (i + 1) * each, :] = part[...]
    tall = 128

    def block(i, carry):
        spot = pl.ds(pl.multiple_of(i * tall, tall), tall)
        mine = joined[spot, :]
        hidden = []
        for half in halves:
            gate_pre = jnp.dot(mine, half[0:width, :], preferred_element_type=jnp.float32)
            up_pre = jnp.dot(mine, half[width : 2 * width, :], preferred_element_type=jnp.float32)
            silu = gate_pre / (1.0 + jnp.exp(-gate_pre))
            hidden.append((silu * up_pre).astype(jnp.bfloat16))
        for col in range(0, width, units):
            at = 2 * width + col
            part = jnp.dot(
                hidden[0], halves[0][at : at + units, :], preferred_element_type=jnp.float32
            ) + jnp.dot(
                hidden[1], halves[1][at : at + units, :], preferred_element_type=jnp.float32
            )
            made[spot, col : col + units] = part.astype(jnp.bfloat16)
        return carry

    lax.fori_loop(0, joined.shape[0] // tall, block, 0)
    for i, out in enumerate(outs):
        out[...] = made[i * each : (i + 1) * each, :]


def expert_rows(rows, halves):
    count = len(rows)
    each, width = rows[0].shape
    flops = 2 * count * each * width * halves[0].shape[1] * 2 * 3
    joined = pltpu.VMEM((count * each, width), jnp.bfloat16)
    return pl.pallas_call(
        partial(expert_kernel, count=count),
        out_shape=tuple(jax.ShapeDtypeStruct((each, width), jnp.bfloat16) for _ in rows),
        in_specs=[vmem] * (count + 2),
        out_specs=(vmem,) * count,
        scratch_shapes=[joined, joined],
        compiler_params=pltpu.CompilerParams(vmem_limit_bytes=16 << 20),
        cost_estimate=pl.CostEstimate(flops=flops, transcendentals=0, bytes_accessed=6 << 20),
    )(*rows, *halves)


def added(left, right):
    return (left.astype(jnp.float32) + right.astype(jnp.float32)).astype(jnp.bfloat16)


def expert_sum(own, weights):
    def up(array):
        return lax.ppermute(array, "tp", z_perm(1))

    def down(array):
        return lax.ppermute(array, "tp", z_perm(-1))

    half = own.shape[0] // 2
    top, end = own[:half], own[half:]
    up_top, down_end, up_end, down_top = [top], [end], [end], [top]
    for _ in range(1, 4):
        up_top.append(up(up_top[-1]))
        down_end.append(down(down_end[-1]))
        up_end.append(up(up_end[-1]))
        down_top.append(down(down_top[-1]))
    up_top.append(up(up_top[-1]))
    down_end.append(down(down_end[-1]))
    chains = (up_top, up_end, down_top, down_end)
    made = []
    for i in range(1, 4):
        rows = [chain[i] for chain in chains]
        made.append(expert_rows(([top, end] if i == 1 else []) + rows, weights))
    mine, done = made[0][:2], [made[0][2:], made[1], made[2]]
    far_top, far_end = expert_rows([up_top[4], down_end[4]], weights)

    low_top, high_end = down(done[2][0]), up(done[2][3])
    high_top, low_end = up(far_top), down(far_end)
    high_top = up(added(high_top, done[2][2]))
    low_end = down(added(low_end, done[2][1]))
    for i in (1, 0):
        low_top = down(added(low_top, done[i][0]))
        high_end = up(added(high_end, done[i][3]))
        high_top = up(added(high_top, done[i][2]))
        low_end = down(added(low_end, done[i][1]))
    sums = []
    for parts in ((low_top, high_top, mine[0]), (low_end, high_end, mine[1])):
        low, high, own_part = (part.astype(jnp.float32) for part in parts)
        sums.append((low + high + own_part).astype(jnp.bfloat16))
    return jnp.concatenate(sums)


def place_rows(routing, slot_count, capacity):
    expert_count, row_count = slot_count // capacity, routing.shape[1]
    expert_id = lax.broadcasted_iota(jnp.int32, (expert_count, row_count), 0)
    chosen = [(routing[k : k + 1, :] == expert_id).astype(jnp.float32) for k in range(TOP)]
    before = lax.broadcasted_iota(jnp.int32, (row_count, row_count), 0)
    before = before < lax.broadcasted_iota(jnp.int32, (row_count, row_count), 1)
    before = before.astype(jnp.float32).astype(jnp.bfloat16)
    counts = jnp.dot(
        sum(chosen).astype(jnp.bfloat16), before, preferred_element_type=jnp.float32
    )
    slot_id = lax.broadcasted_iota(jnp.int32, (slot_count, row_count), 0)
    here = []
    for k in range(TOP):
        rank = jnp.sum(counts * chosen[k], axis=0, keepdims=True).astype(jnp.int32)
        here.append(slot_id == routing[k : k + 1, :] * capacity + rank)
    return here


def project_kernel(
    heads, out_weight, stream, norm_gain, routing, route_weights, resid_sum, outgoing, mixing, joined
):
    for head in range(heads.shape[0]):
        joined[:, head * HD : (head + 1) * HD] = heads[head]
    slot_count = mixing.shape[0]
    experts = slot_count // max(2, 2 * TOP * stream.shape[0] // lax.axis_size("sp"))
    here = place_rows(routing[...], slot_count, slot_count // experts)
    mix = jnp.zeros(mixing.shape, jnp.float32)
    place = jnp.zeros(mixing.shape, jnp.float32)
    for k in range(TOP):
        mix = jnp.where(here[k], route_weights[k : k + 1, :], mix)
        place = jnp.where(here[k], 1.0, place)
    mixing[...] = mix
    wide = 512

    def column(j, carry):
        cols = pl.ds(pl.multiple_of(j * wide, wide), wide)
        mixed_rows = jnp.dot(joined[...], out_weight[:, cols], preferred_element_type=jnp.float32)
        resid_sum[:, cols] = stream[:, cols].astype(jnp.float32) + mixed_rows
        return carry

    lax.fori_loop(0, resid_sum.shape[1] // wide, column, 0)
    resid = resid_sum[...]
    center = resid - jnp.mean(resid, axis=1, keepdims=True)
    spread = jnp.mean(center * center, axis=1, keepdims=True)
    normed = (center * lax.rsqrt(spread + 1e-05) * norm_gain[...]).astype(jnp.bfloat16)
    outgoing[...] = jnp.dot(
        place.astype(jnp.bfloat16), normed, preferred_element_type=jnp.float32
    ).astype(jnp.bfloat16)


def project(heads, out_weight, stream, norm_gain, routing, route_weights, slot_count):
    rows, width = stream.shape
    return pl.pallas_call(
        project_kernel,
        out_shape=(
            jax.ShapeDtypeStruct((rows, width), jnp.float32),
            jax.ShapeDtypeStruct((slot_count, width), jnp.bfloat16),
            jax.ShapeDtypeStruct((slot_count, rows), jnp.float32),
        ),
        in_specs=[vmem] * 6,
        out_specs=(vmem,) * 3,
        scratch_shapes=[pltpu.VMEM((rows, heads.shape[0] * HD), jnp.bfloat16)],
        compiler_params=pltpu.CompilerParams(vmem_limit_bytes=14 << 20),
        name="project",
    )(
        heads,
        out_weight,
        stream,
        norm_gain.reshape(1, width),
        jnp.transpose(routing),
        jnp.transpose(route_weights),
    )


def combine_kernel(resid_sum, returned, mixing, out):
    total = resid_sum[...]
    for part in three_parts(mixing[...]):
        total = total + lax.dot_general(
            part, returned[...], (((0,), (0,)), ((), ())), preferred_element_type=jnp.float32
        )
    out[...] = total.astype(jnp.bfloat16)


def combine(resid_sum, returned, mixing):
    return pl.pallas_call(
        combine_kernel,
        out_shape=jax.ShapeDtypeStruct(resid_sum.shape, jnp.bfloat16),
        in_specs=[vmem] * 3,
        out_specs=vmem,
        compiler_params=pltpu.CompilerParams(vmem_limit_bytes=6 << 20),
        name="combine",
    )(resid_sum, returned, mixing)


def on_device(
    queries,
    key_vectors,
    value_vectors,
    forget_totals,
    head_gain,
    stream,
    out_weight,
    norm_gain,
    routing,
    route_weights,
    gate_weight,
    up_weight,
    down_weight,
):
    sp_count = lax.axis_size("sp")
    head_out, own_half = attention(
        queries,
        key_vectors,
        value_vectors,
        forget_totals,
        head_gain,
        (gate_weight[0], up_weight[0], down_weight[0]),
    )
    weights = own_half, lax.ppermute(own_half, "tp", core_swap)
    row_count, width = stream.shape
    capacity = max(2, 2 * TOP * row_count // sp_count)
    heads = head_out.reshape(-1, row_count, HD)
    heads = lax.all_to_all(heads, "tp", split_axis=0, concat_axis=0, tiled=True)
    resid_sum, outgoing, mixing = project(
        heads, out_weight, stream, norm_gain, routing, route_weights, sp_count * capacity
    )
    outgoing = outgoing.reshape(sp_count, capacity, width)
    arrived = lax.all_to_all(outgoing, "sp", split_axis=0, concat_axis=0, tiled=True)
    summed = expert_sum(arrived.reshape(-1, width), weights)
    expert_out = summed.reshape(sp_count, capacity, width)
    returned = lax.all_to_all(expert_out, "sp", split_axis=0, concat_axis=0, tiled=True)
    return combine(resid_sum, returned.reshape(-1, width), mixing)


def solution(mesh):
    in_specs = (
        P("sp", "tp"),
        P("sp", "tp"),
        P("sp", "tp"),
        P("sp", "tp"),
        P("tp"),
        P(("sp", "tp"), None),
        P(),
        P(),
        P(("sp", "tp"), None),
        P(("sp", "tp"), None),
        P("sp", None, "tp"),
        P("sp", None, "tp"),
        P("sp", "tp", None),
    )
    out_specs = P(("sp", "tp"), None)
    return jax.shard_map(
        on_device, mesh=mesh, in_specs=in_specs, out_specs=out_specs, check_vma=False
    )
```

```python
from functools import partial

import jax
import jax.numpy as jnp
from jax import lax
from jax.experimental import pallas as pl
from jax.experimental.pallas import tpu as pltpu
from jax.sharding import PartitionSpec as P


HD = 128
TOP = 2
LOG2E = 1.4426950408889634
low_score = -1e30
GATE_ROWS = 16
KEYS = 256
PIECE = KEYS + GATE_ROWS
BLOCK = 2 * PIECE
PACK = HD + GATE_ROWS


def sp_perm(dy, dx, needed):
    pairs = []
    for y in range(4):
        for x in range(4):
            into = (y + dy) % 4, (x + dx) % 4
            if needed(*into):
                pairs.append((y * 4 + x, into[0] * 4 + into[1]))
    return pairs


def z_perm(dz):
    return [(z * 2 + c, ((z + dz) % 8) * 2 + c) for z in range(8) for c in range(2)]


core_swap = [(i, i ^ 1) for i in range(16)]


vmem = pl.BlockSpec(memory_space=pltpu.VMEM)


def in_hbm(*arrays):
    return [pltpu.with_memory_space_constraint(array, pltpu.HBM) for array in arrays]


def three_parts(wide):
    first = wide.astype(jnp.bfloat16)
    rest = wide - first.astype(jnp.float32)
    second = rest.astype(jnp.bfloat16)
    third = (rest - second.astype(jnp.float32)).astype(jnp.bfloat16)
    return first, second, third


def piece_kernel(*refs):
    sources, outs, staged, sems = refs[:4], refs[4:6], refs[6:10], refs[10]
    copies = [
        pltpu.make_async_copy(source, into, sems.at[i])
        for i, (source, into) in enumerate(zip(sources, staged))
    ]
    for copy in copies:
        copy.start()
    for copy in copies:
        copy.wait()
    queries, keys, values, gates = staged
    keys_own, query_pack = outs
    stretched = gates[...] * HD**0.5
    tok_count = stretched.shape[1]
    row = lax.broadcasted_iota(jnp.int32, (GATE_ROWS, KEYS), 0)
    for i in range(2):
        at_row = i * PIECE
        rows = slice(i * KEYS, (i + 1) * KEYS)
        keys_own[at_row : at_row + HD, :] = jnp.transpose(values[rows, :])
        keys_own[at_row + HD : at_row + KEYS, 0:HD] = keys[i * KEYS : i * KEYS + HD, :]
        keys_own[at_row + HD : at_row + KEYS, HD:KEYS] = keys[i * KEYS + HD : (i + 1) * KEYS, :]
        parts = [part.astype(jnp.float32) for part in three_parts(-stretched[:, rows])]
        block = jnp.where((row >= 3) & (row < 6), 1.0, 0.0)
        for at, part in enumerate(parts):
            block = jnp.where(row == at, part, block)
        keys_own[at_row + KEYS : at_row + PIECE, :] = block.astype(jnp.bfloat16)
    wide_row = lax.broadcasted_iota(jnp.int32, (GATE_ROWS, tok_count), 0)
    mix = jnp.where(wide_row < 3, 1.0, 0.0)
    parts = [part.astype(jnp.float32) for part in three_parts(stretched[:, 0:1])]
    for at, part in enumerate(parts):
        mix = jnp.where(wide_row == 3 + at, part, mix)
    mix = jnp.where(wide_row == 6, low_score, mix)
    query_pack[HD:PACK, :] = mix.astype(jnp.bfloat16)
    query_pack[0:HD, :] = jnp.transpose(queries[...])


def make_pieces(queries, keys, values, gates):
    tok_count = queries.shape[0]
    return pl.pallas_call(
        piece_kernel,
        out_shape=(
            jax.ShapeDtypeStruct((BLOCK, 2 * HD), jnp.bfloat16),
            jax.ShapeDtypeStruct((PACK, tok_count), jnp.bfloat16),
        ),
        in_specs=[pl.BlockSpec(memory_space=pltpu.HBM)] * 4,
        out_specs=(vmem,) * 2,
        scratch_shapes=[pltpu.VMEM((tok_count, HD), jnp.bfloat16)] * 3
        + [pltpu.VMEM((1, tok_count), jnp.float32), pltpu.SemaphoreType.DMA((4,))],
        compiler_params=pltpu.CompilerParams(vmem_limit_bytes=6 << 20),
        name="make_pieces",
    )(*in_hbm(queries, keys, values, gates.reshape(1, tok_count)))


def fold(query_wide, state, stack, keys_wide, block, own_block=False):
    run_max, run_sum, run_acc = state
    tok_count = query_wide.shape[1]
    scale = HD ** (-0.5) * LOG2E
    scores = []
    for part in range(2 * KEYS // HD):
        spot = pl.ds(pl.multiple_of(block * (2 * KEYS) + part * HD, HD), HD)
        score = jnp.dot(
            keys_wide[spot, :], query_wide[...], preferred_element_type=jnp.float32
        )
        if own_block:
            key_at = lax.broadcasted_iota(jnp.int32, score.shape, 0) + part * HD
            query_at = lax.broadcasted_iota(jnp.int32, score.shape, 1)
            score = jnp.where(key_at <= query_at, score, low_score)
        scores.append(score)
    old_max = run_max[0:1, :]
    peak = scores[0]
    for score in scores[1:]:
        peak = jnp.maximum(peak, score)
    new_max = jnp.maximum(old_max, jnp.max(peak, axis=0, keepdims=True))
    rescale = jnp.exp2((old_max - new_max) * scale)
    scaled_max = new_max * scale
    total = run_sum[...] * rescale
    acc = run_acc[...] * rescale
    for i in range(2):
        at = pl.multiple_of(block * BLOCK + i * PIECE, GATE_ROWS)
        rounded = []
        for score in scores[2 * i : 2 * i + 2]:
            lifted = jnp.exp2(score * scale - scaled_max)
            total = total + jnp.sum(lifted.reshape(HD // 8, 8, tok_count), axis=0)
            rounded.append(lifted.astype(jnp.bfloat16))
        acc = acc + jnp.dot(
            stack[pl.ds(at, HD), :],
            jnp.concatenate(rounded, axis=0),
            preferred_element_type=jnp.float32,
        )
    run_sum[...] = total
    run_acc[...] = acc
    run_max[...] = jnp.broadcast_to(new_max, run_max.shape)


def clear(state):
    run_max, run_sum, run_acc = state
    run_max[...] = jnp.full(run_max.shape, low_score, jnp.float32)
    run_sum[...] = jnp.zeros(run_sum.shape, jnp.float32)
    run_acc[...] = jnp.zeros(run_acc.shape, jnp.float32)


def nth_state(state, i):
    found = []
    for ref in state:
        rows = ref.shape[0] // 2
        found.append(ref.at[pl.ds(pl.multiple_of(i * rows, 8), rows)])
    return found


def fold_blocks(query_wide, state, stack, keys_wide, first, count, seen=None):
    def block(i, carry):
        run = partial(fold, query_wide, state, stack, keys_wide, i)
        if seen is None:
            run()
        else:
            pl.when(seen(i))(run)
        return carry

    lax.fori_loop(first, first + count, block, 0)


def load_blocks(stack, keys_wide, parts):
    at = 0
    for part in parts:
        stack[at : at + part.shape[0], :] = part[...]
        at += part.shape[0]
    for piece in range(at // PIECE):
        row, at = piece * KEYS, piece * PIECE
        for half in range(KEYS // HD):
            keys_wide[row + half * HD : row + (half + 1) * HD, 0:HD] = stack[
                at + HD : at + 2 * HD, half * HD : (half + 1) * HD
            ]
        gates = stack[at + KEYS : at + PIECE, :].astype(jnp.float32)
        rest = jnp.zeros((HD - GATE_ROWS, KEYS), jnp.float32)
        columns = jnp.transpose(jnp.concatenate([gates, rest], axis=0))
        keys_wide[row : row + KEYS, HD : 2 * HD] = columns.astype(jnp.bfloat16)


def load_query(query_wide, pack):
    query_wide[0:PACK, :] = pack[...]
    query_wide[PACK : 2 * HD, :] = jnp.zeros((2 * HD - PACK, pack.shape[1]), jnp.bfloat16)


def pack_result(state, out):
    run_max, run_sum, run_acc = state
    total = jnp.sum(run_sum[...], axis=0, keepdims=True)
    out[0:HD, :] = (run_acc[...] / total).astype(jnp.bfloat16)
    row = lax.broadcasted_iota(jnp.int32, (GATE_ROWS, total.shape[1]), 0)
    block = jnp.zeros(row.shape, jnp.float32)
    for at, part in enumerate(three_parts(run_max[0:1, :]) + three_parts(total)):
        block = jnp.where(row == at, part.astype(jnp.float32), block)
    out[HD:PACK, :] = block.astype(jnp.bfloat16)


def distant_kernel(*refs):
    packs, keys, states = refs[:2], refs[2:5], refs[5:8]
    stack, keys_wide, query_wide = refs[8:]
    own_y = lax.axis_index("sp") >> 2

    @pl.when(own_y < 2)
    def _():
        load_blocks(stack, keys_wide, keys)

    def each(i, carry):
        @pl.when(own_y <= i)
        def _():
            for at, pack in enumerate(packs):
                pl.when(i == at)(partial(load_query, query_wide, pack))
            state = nth_state(states, i)
            clear(state)
            fold_blocks(query_wide, state, stack, keys_wide, 0, 3)

        return carry

    lax.fori_loop(0, 2, each, 0)


def distant_end_kernel(*refs):
    packs, far, states, outs = refs[:2], refs[2:4], refs[4:7], refs[7:9]
    state, (stack, keys_wide, query_wide) = refs[9:12], refs[12:]
    own_y = lax.axis_index("sp") >> 2

    @pl.when(own_y < 2)
    def _():
        load_blocks(stack, keys_wide, far)

    def each(i, carry):
        @pl.when(own_y <= i)
        def _():
            for into, came in zip(state, nth_state(states, i)):
                into[...] = came[...]
            for at, pack in enumerate(packs):
                pl.when(i == at)(partial(load_query, query_wide, pack))
            fold(query_wide, state, stack, keys_wide, 0)
            for at, out in enumerate(outs):
                pl.when(i == at)(partial(pack_result, state, out))

        return carry

    lax.fori_loop(0, 2, each, 0)


def next_kernel(*refs):
    pack, keys, out, state = refs[0], refs[1:6], refs[6], refs[7:10]
    stack, keys_wide, query_wide = refs[10:]

    @pl.when(lax.axis_index("sp") < 12)
    def _():
        load_blocks(stack, keys_wide, keys)
        load_query(query_wide, pack)
        clear(state)
        fold_blocks(query_wide, state, stack, keys_wide, 0, 4)
        pack_result(state, out)


def own_kernel(*refs):
    pack, keys, state = refs[0], refs[1:6], refs[6:9]
    stack, keys_wide, query_wide = refs[9:]
    own_x = lax.axis_index("sp") & 3
    load_blocks(stack, keys_wide, keys)
    load_query(query_wide, pack)
    clear(state)
    fold(query_wide, state, stack, keys_wide, 0, own_block=True)

    def seen(i):
        move = jnp.where(i == 1, -1, jnp.where(i == 2, 1, 2))
        return ((own_x + move) & 3) < own_x

    fold_blocks(query_wide, state, stack, keys_wide, 1, 3, seen)


def merge_kernel(*refs):
    came, own_state, gain, head_out = refs[:3], refs[3:6], refs[6], refs[7]
    own_y = lax.axis_index("sp") >> 2
    scale = HD ** (-0.5) * LOG2E
    peaks = [own_state[0][0:1, :]]
    totals = [jnp.sum(own_state[1][...], axis=0, keepdims=True)]
    for above, pack in enumerate(came):
        rows = pack[HD:PACK, :].astype(jnp.float32)
        parts = [rows[at : at + 1, :] for at in range(6)]
        valid = own_y > above
        peaks.append(jnp.where(valid, parts[0] + parts[1] + parts[2], low_score))
        totals.append(jnp.where(valid, parts[3] + parts[4] + parts[5], 0.0))
    top = peaks[0]
    for peak in peaks[1:]:
        top = jnp.maximum(top, peak)
    weight = jnp.exp2((peaks[0] - top) * scale)
    total = totals[0] * weight
    acc = own_state[2][...] * weight
    for pack, peak, share in zip(came, peaks[1:], totals[1:]):
        weight = share * jnp.exp2((peak - top) * scale)
        total = total + weight
        acc = acc + pack[0:HD, :].astype(jnp.float32) * weight
    attended = acc / total
    mean_square = jnp.mean(attended * attended, axis=0, keepdims=True)
    normed = jnp.transpose(attended * lax.rsqrt(mean_square + 1e-06))
    head_out[...] = (normed * gain[...]).astype(jnp.bfloat16)


def attend(kernel, operands, outs, scratch, folds):
    tok_count = 2 * KEYS
    return pl.pallas_call(
        kernel,
        out_shape=tuple(jax.ShapeDtypeStruct(*out) for out in outs),
        in_specs=[vmem] * len(operands),
        out_specs=(vmem,) * len(outs),
        scratch_shapes=[pltpu.VMEM(*shape) for shape in scratch],
        compiler_params=pltpu.CompilerParams(vmem_limit_bytes=12 << 20),
        cost_estimate=pl.CostEstimate(
            flops=8 * tok_count * tok_count * HD * folds,
            transcendentals=tok_count * tok_count * folds,
            bytes_accessed=1 << 20,
        ),
    )(*operands)


def attention(queries, key_vectors, value_vectors, forget_totals, head_gain, weights):
    tok_count = queries.shape[0]

    def shift(array, dy, dx, needed):
        return lax.ppermute(array, "sp", sp_perm(dy, dx, needed))

    keys_own, own_pack = make_pieces(queries, key_vectors, value_vectors, forget_totals)
    low = shift(keys_own, 0, 1, lambda y, x: y < 3 or x > 0)
    high = shift(keys_own, 0, -1, lambda y, x: y < 3 or x in (0, 3))
    pack3 = shift(own_pack, 1, 0, lambda y, x: y == 0)
    pack2 = shift(own_pack, 2, 0, lambda y, x: y < 2)
    pack1 = shift(own_pack, -1, 0, lambda y, x: y < 3)
    far_a = shift(low[:PIECE], 0, 1, lambda y, x: y < 3 or x > 1)
    far_b = shift(high[PIECE:], 0, -1, lambda y, x: y < 3 or x > 1)

    narrow = ((8, tok_count), jnp.float32)
    state = [narrow, narrow, ((HD, tok_count), jnp.float32)]
    both = [((2 * shape[0], tok_count), kind) for shape, kind in state]
    result = ((PACK, tok_count), jnp.bfloat16)

    def loaded(count):
        shapes = (count * BLOCK, 2 * HD), (count * 2 * KEYS, 2 * HD), (2 * HD, tok_count)
        return [(shape, jnp.bfloat16) for shape in shapes]

    near = attend(distant_kernel, [pack3, pack2, keys_own, low, high], both, loaded(3), 6)
    far_a, far_b, near = lax.optimization_barrier((far_a, far_b, near))
    part3, part2 = attend(
        distant_end_kernel, [pack3, pack2, far_a, far_b, *near], [result] * 2, state + loaded(1), 2
    )
    part3, part2, pack1 = lax.optimization_barrier((part3, part2, pack1))
    back3 = shift(part3, -1, 0, lambda y, x: y == 3)
    back2 = shift(part2, 2, 0, lambda y, x: y > 1)
    keys = [keys_own, low, high, far_a, far_b]
    (part1,) = attend(next_kernel, [pack1, *keys], [result], state + loaded(4), 4)
    part1, own_pack, keys, weights = lax.optimization_barrier((part1, own_pack, keys, weights))
    back1 = shift(part1, 1, 0, lambda y, x: y > 0)
    own_state = attend(own_kernel, [own_pack, *keys], state, loaded(4), 4)
    staged = stage_weights(*weights)
    (head_out,) = attend(
        merge_kernel,
        [back1, back2, back3, *own_state, head_gain.reshape(1, HD)],
        [((tok_count, HD), jnp.bfloat16)],
        [],
        0,
    )
    return head_out, staged


def staging_kernel(gate, up, down, out, sems):
    tall, wide = gate.shape
    copies = [
        pltpu.make_async_copy(gate, out.at[pl.ds(0, tall)], sems.at[0]),
        pltpu.make_async_copy(up, out.at[pl.ds(tall, tall)], sems.at[1]),
    ]
    for i in range(down.shape[1] // wide):
        source = down.at[:, pl.ds(i * wide, wide)]
        into = out.at[pl.ds(2 * tall + i * down.shape[0], down.shape[0])]
        copies.append(pltpu.make_async_copy(source, into, sems.at[2 + i]))
    for copy in copies:
        copy.start()
    for copy in copies:
        copy.wait()


def stage_weights(gate, up, down):
    blocks = down.shape[1] // gate.shape[1]
    rows = 2 * gate.shape[0] + blocks * down.shape[0]
    return pl.pallas_call(
        staging_kernel,
        out_shape=jax.ShapeDtypeStruct((rows, gate.shape[1]), jnp.bfloat16),
        in_specs=[pl.BlockSpec(memory_space=pltpu.HBM)] * 3,
        out_specs=vmem,
        scratch_shapes=[pltpu.SemaphoreType.DMA((2 + blocks,))],
        compiler_params=pltpu.CompilerParams(vmem_limit_bytes=4 << 20),
        name="stage_weights",
    )(*in_hbm(gate, up, down))


def expert_kernel(*refs, count):
    rows, halves = refs[:count], refs[count : count + 2]
    outs = refs[count + 2 : 2 * count + 2]
    joined, made = refs[2 * count + 2 :]
    each, width = rows[0].shape
    units = halves[0].shape[1]
    for i, part in enumerate(rows):
        joined[i * each : (i + 1) * each, :] = part[...]
    tall = 128

    def block(i, carry):
        spot = pl.ds(pl.multiple_of(i * tall, tall), tall)
        mine = joined[spot, :]
        hidden = []
        for half in halves:
            gate_pre = jnp.dot(mine, half[0:width, :], preferred_element_type=jnp.float32)
            up_pre = jnp.dot(mine, half[width : 2 * width, :], preferred_element_type=jnp.float32)
            silu = gate_pre / (1.0 + jnp.exp(-gate_pre))
            hidden.append((silu * up_pre).astype(jnp.bfloat16))
        for col in range(0, width, units):
            at = 2 * width + col
            part = jnp.dot(
                hidden[0], halves[0][at : at + units, :], preferred_element_type=jnp.float32
            ) + jnp.dot(
                hidden[1], halves[1][at : at + units, :], preferred_element_type=jnp.float32
            )
            made[spot, col : col + units] = part.astype(jnp.bfloat16)
        return carry

    lax.fori_loop(0, joined.shape[0] // tall, block, 0)
    for i, out in enumerate(outs):
        out[...] = made[i * each : (i + 1) * each, :]


def expert_rows(rows, halves):
    count = len(rows)
    each, width = rows[0].shape
    flops = 2 * count * each * width * halves[0].shape[1] * 2 * 3
    joined = pltpu.VMEM((count * each, width), jnp.bfloat16)
    return pl.pallas_call(
        partial(expert_kernel, count=count),
        out_shape=tuple(jax.ShapeDtypeStruct((each, width), jnp.bfloat16) for _ in rows),
        in_specs=[vmem] * (count + 2),
        out_specs=(vmem,) * count,
        scratch_shapes=[joined, joined],
        compiler_params=pltpu.CompilerParams(vmem_limit_bytes=16 << 20),
        cost_estimate=pl.CostEstimate(flops=flops, transcendentals=0, bytes_accessed=6 << 20),
    )(*rows, *halves)


def added(left, right):
    return (left.astype(jnp.float32) + right.astype(jnp.float32)).astype(jnp.bfloat16)


def expert_sum(own, weights):
    def up(array):
        return lax.ppermute(array, "tp", z_perm(1))

    def down(array):
        return lax.ppermute(array, "tp", z_perm(-1))

    half = own.shape[0] // 2
    top, end = own[:half], own[half:]
    up_top, down_end, up_end, down_top = [top], [end], [end], [top]
    for _ in range(1, 4):
        up_top.append(up(up_top[-1]))
        down_end.append(down(down_end[-1]))
        up_end.append(up(up_end[-1]))
        down_top.append(down(down_top[-1]))
    up_top.append(up(up_top[-1]))
    down_end.append(down(down_end[-1]))
    chains = (up_top, up_end, down_top, down_end)
    made = []
    for i in range(1, 4):
        rows = [chain[i] for chain in chains]
        made.append(expert_rows(([top, end] if i == 1 else []) + rows, weights))
    mine, done = made[0][:2], [made[0][2:], made[1], made[2]]
    far_top, far_end = expert_rows([up_top[4], down_end[4]], weights)

    low_top, high_end = down(done[2][0]), up(done[2][3])
    high_top, low_end = up(far_top), down(far_end)
    high_top = up(added(high_top, done[2][2]))
    low_end = down(added(low_end, done[2][1]))
    for i in (1, 0):
        low_top = down(added(low_top, done[i][0]))
        high_end = up(added(high_end, done[i][3]))
        high_top = up(added(high_top, done[i][2]))
        low_end = down(added(low_end, done[i][1]))
    sums = []
    for parts in ((low_top, high_top, mine[0]), (low_end, high_end, mine[1])):
        low, high, own_part = (part.astype(jnp.float32) for part in parts)
        sums.append((low + high + own_part).astype(jnp.bfloat16))
    return jnp.concatenate(sums)


def place_rows(routing, slot_count, capacity):
    expert_count, row_count = slot_count // capacity, routing.shape[1]
    expert_id = lax.broadcasted_iota(jnp.int32, (expert_count, row_count), 0)
    chosen = [(routing[k : k + 1, :] == expert_id).astype(jnp.float32) for k in range(TOP)]
    before = lax.broadcasted_iota(jnp.int32, (row_count, row_count), 0)
    before = before < lax.broadcasted_iota(jnp.int32, (row_count, row_count), 1)
    before = before.astype(jnp.float32).astype(jnp.bfloat16)
    counts = jnp.dot(
        sum(chosen).astype(jnp.bfloat16), before, preferred_element_type=jnp.float32
    )
    slot_id = lax.broadcasted_iota(jnp.int32, (slot_count, row_count), 0)
    here = []
    for k in range(TOP):
        rank = jnp.sum(counts * chosen[k], axis=0, keepdims=True).astype(jnp.int32)
        here.append(slot_id == routing[k : k + 1, :] * capacity + rank)
    return here


def project_kernel(
    heads, out_weight, stream, norm_gain, routing, route_weights, resid_sum, outgoing, mixing, joined
):
    for head in range(heads.shape[0]):
        joined[:, head * HD : (head + 1) * HD] = heads[head]
    slot_count = mixing.shape[0]
    experts = slot_count // max(2, 2 * TOP * stream.shape[0] // lax.axis_size("sp"))
    here = place_rows(routing[...], slot_count, slot_count // experts)
    mix = jnp.zeros(mixing.shape, jnp.float32)
    place = jnp.zeros(mixing.shape, jnp.float32)
    for k in range(TOP):
        mix = jnp.where(here[k], route_weights[k : k + 1, :], mix)
        place = jnp.where(here[k], 1.0, place)
    mixing[...] = mix
    wide = 512

    def column(j, carry):
        cols = pl.ds(pl.multiple_of(j * wide, wide), wide)
        mixed_rows = jnp.dot(joined[...], out_weight[:, cols], preferred_element_type=jnp.float32)
        resid_sum[:, cols] = stream[:, cols].astype(jnp.float32) + mixed_rows
        return carry

    lax.fori_loop(0, resid_sum.shape[1] // wide, column, 0)
    resid = resid_sum[...]
    center = resid - jnp.mean(resid, axis=1, keepdims=True)
    spread = jnp.mean(center * center, axis=1, keepdims=True)
    normed = (center * lax.rsqrt(spread + 1e-05) * norm_gain[...]).astype(jnp.bfloat16)
    outgoing[...] = jnp.dot(
        place.astype(jnp.bfloat16), normed, preferred_element_type=jnp.float32
    ).astype(jnp.bfloat16)


def project(heads, out_weight, stream, norm_gain, routing, route_weights, slot_count):
    rows, width = stream.shape
    return pl.pallas_call(
        project_kernel,
        out_shape=(
            jax.ShapeDtypeStruct((rows, width), jnp.float32),
            jax.ShapeDtypeStruct((slot_count, width), jnp.bfloat16),
            jax.ShapeDtypeStruct((slot_count, rows), jnp.float32),
        ),
        in_specs=[vmem] * 6,
        out_specs=(vmem,) * 3,
        scratch_shapes=[pltpu.VMEM((rows, heads.shape[0] * HD), jnp.bfloat16)],
        compiler_params=pltpu.CompilerParams(vmem_limit_bytes=14 << 20),
        name="project",
    )(
        heads,
        out_weight,
        stream,
        norm_gain.reshape(1, width),
        jnp.transpose(routing),
        jnp.transpose(route_weights),
    )


def combine_kernel(resid_sum, returned, mixing, out):
    total = resid_sum[...]
    for part in three_parts(mixing[...]):
        total = total + lax.dot_general(
            part, returned[...], (((0,), (0,)), ((), ())), preferred_element_type=jnp.float32
        )
    out[...] = total.astype(jnp.bfloat16)


def combine(resid_sum, returned, mixing):
    return pl.pallas_call(
        combine_kernel,
        out_shape=jax.ShapeDtypeStruct(resid_sum.shape, jnp.bfloat16),
        in_specs=[vmem] * 3,
        out_specs=vmem,
        compiler_params=pltpu.CompilerParams(vmem_limit_bytes=6 << 20),
        name="combine",
    )(resid_sum, returned, mixing)


def on_device(
    queries,
    key_vectors,
    value_vectors,
    forget_totals,
    head_gain,
    stream,
    out_weight,
    norm_gain,
    routing,
    route_weights,
    gate_weight,
    up_weight,
    down_weight,
):
    sp_count = lax.axis_size("sp")
    head_out, own_half = attention(
        queries,
        key_vectors,
        value_vectors,
        forget_totals,
        head_gain,
        (gate_weight[0], up_weight[0], down_weight[0]),
    )
    weights = own_half, lax.ppermute(own_half, "tp", core_swap)
    row_count, width = stream.shape
    capacity = max(2, 2 * TOP * row_count // sp_count)
    heads = head_out.reshape(-1, row_count, HD)
    heads = lax.all_to_all(heads, "tp", split_axis=0, concat_axis=0, tiled=True)
    resid_sum, outgoing, mixing = project(
        heads, out_weight, stream, norm_gain, routing, route_weights, sp_count * capacity
    )
    outgoing = outgoing.reshape(sp_count, capacity, width)
    arrived = lax.all_to_all(outgoing, "sp", split_axis=0, concat_axis=0, tiled=True)
    summed = expert_sum(arrived.reshape(-1, width), weights)
    expert_out = summed.reshape(sp_count, capacity, width)
    returned = lax.all_to_all(expert_out, "sp", split_axis=0, concat_axis=0, tiled=True)
    return combine(resid_sum, returned.reshape(-1, width), mixing)


def solution(mesh):
    in_specs = (
        P("sp", "tp"),
        P("sp", "tp"),
        P("sp", "tp"),
        P("sp", "tp"),
        P("tp"),
        P(("sp", "tp"), None),
        P(),
        P(),
        P(("sp", "tp"), None),
        P(("sp", "tp"), None),
        P("sp", None, "tp"),
        P("sp", None, "tp"),
        P("sp", "tp", None),
    )
    out_specs = P(("sp", "tp"), None)
    return jax.shard_map(
        on_device, mesh=mesh, in_specs=in_specs, out_specs=out_specs, check_vma=False
    )
```

```python
from functools import partial

import jax
import jax.numpy as jnp
from jax import lax
from jax.experimental import pallas as pl
from jax.experimental.pallas import tpu as pltpu
from jax.sharding import PartitionSpec as P


HD = 128
TOP = 2
LOG2E = 1.4426950408889634
low_score = -1e30
GATE_ROWS = 16
KEYS = 256
PIECE = KEYS + GATE_ROWS
BLOCK = 2 * PIECE
PACK = HD + GATE_ROWS


def sp_perm(dy, dx, needed):
    pairs = []
    for y in range(4):
        for x in range(4):
            into = (y + dy) % 4, (x + dx) % 4
            if needed(*into):
                pairs.append((y * 4 + x, into[0] * 4 + into[1]))
    return pairs


def z_perm(dz):
    return [(z * 2 + c, ((z + dz) % 8) * 2 + c) for z in range(8) for c in range(2)]


core_swap = [(i, i ^ 1) for i in range(16)]


vmem = pl.BlockSpec(memory_space=pltpu.VMEM)


def in_hbm(*arrays):
    return [pltpu.with_memory_space_constraint(array, pltpu.HBM) for array in arrays]


def three_parts(wide):
    first = wide.astype(jnp.bfloat16)
    rest = wide - first.astype(jnp.float32)
    second = rest.astype(jnp.bfloat16)
    third = (rest - second.astype(jnp.float32)).astype(jnp.bfloat16)
    return first, second, third


def piece_kernel(*refs):
    sources, outs, staged, sems = refs[:4], refs[4:6], refs[6:10], refs[10]
    copies = [
        pltpu.make_async_copy(source, into, sems.at[i])
        for i, (source, into) in enumerate(zip(sources, staged))
    ]
    for copy in copies:
        copy.start()
    for copy in copies:
        copy.wait()
    queries, keys, values, gates = staged
    keys_own, query_pack = outs
    stretched = gates[...] * HD**0.5
    tok_count = stretched.shape[1]
    row = lax.broadcasted_iota(jnp.int32, (GATE_ROWS, KEYS), 0)
    for i in range(2):
        at_row = i * PIECE
        rows = slice(i * KEYS, (i + 1) * KEYS)
        keys_own[at_row : at_row + HD, :] = jnp.transpose(values[rows, :])
        keys_own[at_row + HD : at_row + KEYS, 0:HD] = keys[i * KEYS : i * KEYS + HD, :]
        keys_own[at_row + HD : at_row + KEYS, HD:KEYS] = keys[i * KEYS + HD : (i + 1) * KEYS, :]
        parts = [part.astype(jnp.float32) for part in three_parts(-stretched[:, rows])]
        block = jnp.where((row >= 3) & (row < 6), 1.0, 0.0)
        for at, part in enumerate(parts):
            block = jnp.where(row == at, part, block)
        keys_own[at_row + KEYS : at_row + PIECE, :] = block.astype(jnp.bfloat16)
    wide_row = lax.broadcasted_iota(jnp.int32, (GATE_ROWS, tok_count), 0)
    mix = jnp.where(wide_row < 3, 1.0, 0.0)
    parts = [part.astype(jnp.float32) for part in three_parts(stretched[:, 0:1])]
    for at, part in enumerate(parts):
        mix = jnp.where(wide_row == 3 + at, part, mix)
    mix = jnp.where(wide_row == 6, low_score, mix)
    query_pack[HD:PACK, :] = mix.astype(jnp.bfloat16)
    query_pack[0:HD, :] = jnp.transpose(queries[...])


def make_pieces(queries, keys, values, gates):
    tok_count = queries.shape[0]
    return pl.pallas_call(
        piece_kernel,
        out_shape=(
            jax.ShapeDtypeStruct((BLOCK, 2 * HD), jnp.bfloat16),
            jax.ShapeDtypeStruct((PACK, tok_count), jnp.bfloat16),
        ),
        in_specs=[pl.BlockSpec(memory_space=pltpu.HBM)] * 4,
        out_specs=(vmem,) * 2,
        scratch_shapes=[pltpu.VMEM((tok_count, HD), jnp.bfloat16)] * 3
        + [pltpu.VMEM((1, tok_count), jnp.float32), pltpu.SemaphoreType.DMA((4,))],
        compiler_params=pltpu.CompilerParams(vmem_limit_bytes=6 << 20),
        name="make_pieces",
    )(*in_hbm(queries, keys, values, gates.reshape(1, tok_count)))


def fold(query_wide, state, stack, keys_wide, block, own_block=False):
    run_max, run_sum, run_acc = state
    tok_count = query_wide.shape[1]
    scale = HD ** (-0.5) * LOG2E
    scores = []
    for part in range(2 * KEYS // HD):
        spot = pl.ds(pl.multiple_of(block * (2 * KEYS) + part * HD, HD), HD)
        score = jnp.dot(
            keys_wide[spot, :], query_wide[...], preferred_element_type=jnp.float32
        )
        if own_block:
            key_at = lax.broadcasted_iota(jnp.int32, score.shape, 0) + part * HD
            query_at = lax.broadcasted_iota(jnp.int32, score.shape, 1)
            score = jnp.where(key_at <= query_at, score, low_score)
        scores.append(score)
    old_max = run_max[0:1, :]
    peak = scores[0]
    for score in scores[1:]:
        peak = jnp.maximum(peak, score)
    new_max = jnp.maximum(old_max, jnp.max(peak, axis=0, keepdims=True))
    rescale = jnp.exp2((old_max - new_max) * scale)
    scaled_max = new_max * scale
    total = run_sum[...] * rescale
    acc = run_acc[...] * rescale
    for i in range(2):
        at = pl.multiple_of(block * BLOCK + i * PIECE, GATE_ROWS)
        rounded = []
        for score in scores[2 * i : 2 * i + 2]:
            lifted = jnp.exp2(score * scale - scaled_max)
            total = total + jnp.sum(lifted.reshape(HD // 8, 8, tok_count), axis=0)
            rounded.append(lifted.astype(jnp.bfloat16))
        acc = acc + jnp.dot(
            stack[pl.ds(at, HD), :],
            jnp.concatenate(rounded, axis=0),
            preferred_element_type=jnp.float32,
        )
    run_sum[...] = total
    run_acc[...] = acc
    run_max[...] = jnp.broadcast_to(new_max, run_max.shape)


def clear(state):
    run_max, run_sum, run_acc = state
    run_max[...] = jnp.full(run_max.shape, low_score, jnp.float32)
    run_sum[...] = jnp.zeros(run_sum.shape, jnp.float32)
    run_acc[...] = jnp.zeros(run_acc.shape, jnp.float32)


def nth_state(state, i):
    found = []
    for ref in state:
        rows = ref.shape[0] // 2
        found.append(ref.at[pl.ds(pl.multiple_of(i * rows, 8), rows)])
    return found


def fold_blocks(query_wide, state, stack, keys_wide, first, count, seen=None):
    def block(i, carry):
        run = partial(fold, query_wide, state, stack, keys_wide, i)
        if seen is None:
            run()
        else:
            pl.when(seen(i))(run)
        return carry

    lax.fori_loop(first, first + count, block, 0)


def load_blocks(stack, keys_wide, parts):
    at = 0
    for part in parts:
        stack[at : at + part.shape[0], :] = part[...]
        at += part.shape[0]
    for piece in range(at // PIECE):
        row, at = piece * KEYS, piece * PIECE
        for half in range(KEYS // HD):
            keys_wide[row + half * HD : row + (half + 1) * HD, 0:HD] = stack[
                at + HD : at + 2 * HD, half * HD : (half + 1) * HD
            ]
        gates = stack[at + KEYS : at + PIECE, :].astype(jnp.float32)
        rest = jnp.zeros((HD - GATE_ROWS, KEYS), jnp.float32)
        columns = jnp.transpose(jnp.concatenate([gates, rest], axis=0))
        keys_wide[row : row + KEYS, HD : 2 * HD] = columns.astype(jnp.bfloat16)


def load_query(query_wide, pack):
    query_wide[0:PACK, :] = pack[...]
    query_wide[PACK : 2 * HD, :] = jnp.zeros((2 * HD - PACK, pack.shape[1]), jnp.bfloat16)


def pack_result(state, out):
    run_max, run_sum, run_acc = state
    total = jnp.sum(run_sum[...], axis=0, keepdims=True)
    out[0:HD, :] = (run_acc[...] / total).astype(jnp.bfloat16)
    row = lax.broadcasted_iota(jnp.int32, (GATE_ROWS, total.shape[1]), 0)
    block = jnp.zeros(row.shape, jnp.float32)
    for at, part in enumerate(three_parts(run_max[0:1, :]) + three_parts(total)):
        block = jnp.where(row == at, part.astype(jnp.float32), block)
    out[HD:PACK, :] = block.astype(jnp.bfloat16)


def distant_kernel(*refs):
    packs, keys, states = refs[:2], refs[2:5], refs[5:8]
    stack, keys_wide, query_wide = refs[8:]
    own_y = lax.axis_index("sp") >> 2

    @pl.when(own_y < 2)
    def _():
        load_blocks(stack, keys_wide, keys)

    def each(i, carry):
        @pl.when(own_y <= i)
        def _():
            for at, pack in enumerate(packs):
                pl.when(i == at)(partial(load_query, query_wide, pack))
            state = nth_state(states, i)
            clear(state)
            fold_blocks(query_wide, state, stack, keys_wide, 0, 3)

        return carry

    lax.fori_loop(0, 2, each, 0)


def distant_end_kernel(*refs):
    packs, far, states, outs = refs[:2], refs[2:4], refs[4:7], refs[7:9]
    state, (stack, keys_wide, query_wide) = refs[9:12], refs[12:]
    own_y = lax.axis_index("sp") >> 2

    @pl.when(own_y < 2)
    def _():
        load_blocks(stack, keys_wide, far)

    def each(i, carry):
        @pl.when(own_y <= i)
        def _():
            for into, came in zip(state, nth_state(states, i)):
                into[...] = came[...]
            for at, pack in enumerate(packs):
                pl.when(i == at)(partial(load_query, query_wide, pack))
            fold(query_wide, state, stack, keys_wide, 0)
            for at, out in enumerate(outs):
                pl.when(i == at)(partial(pack_result, state, out))

        return carry

    lax.fori_loop(0, 2, each, 0)


def next_kernel(*refs):
    pack, keys, out, state = refs[0], refs[1:6], refs[6], refs[7:10]
    stack, keys_wide, query_wide = refs[10:]

    @pl.when(lax.axis_index("sp") < 12)
    def _():
        load_blocks(stack, keys_wide, keys)
        load_query(query_wide, pack)
        clear(state)
        fold_blocks(query_wide, state, stack, keys_wide, 0, 4)
        pack_result(state, out)


def own_kernel(*refs):
    pack, keys, state = refs[0], refs[1:6], refs[6:9]
    stack, keys_wide, query_wide = refs[9:]
    own_x = lax.axis_index("sp") & 3
    load_blocks(stack, keys_wide, keys)
    load_query(query_wide, pack)
    clear(state)
    fold(query_wide, state, stack, keys_wide, 0, own_block=True)

    def seen(i):
        move = jnp.where(i == 1, -1, jnp.where(i == 2, 1, 2))
        return ((own_x + move) & 3) < own_x

    fold_blocks(query_wide, state, stack, keys_wide, 1, 3, seen)


def merge_kernel(*refs):
    came, own_state, gain, head_out = refs[:3], refs[3:6], refs[6], refs[7]
    own_y = lax.axis_index("sp") >> 2
    scale = HD ** (-0.5) * LOG2E
    peaks = [own_state[0][0:1, :]]
    totals = [jnp.sum(own_state[1][...], axis=0, keepdims=True)]
    for above, pack in enumerate(came):
        rows = pack[HD:PACK, :].astype(jnp.float32)
        parts = [rows[at : at + 1, :] for at in range(6)]
        valid = own_y > above
        peaks.append(jnp.where(valid, parts[0] + parts[1] + parts[2], low_score))
        totals.append(jnp.where(valid, parts[3] + parts[4] + parts[5], 0.0))
    top = peaks[0]
    for peak in peaks[1:]:
        top = jnp.maximum(top, peak)
    weight = jnp.exp2((peaks[0] - top) * scale)
    total = totals[0] * weight
    acc = own_state[2][...] * weight
    for pack, peak, share in zip(came, peaks[1:], totals[1:]):
        weight = share * jnp.exp2((peak - top) * scale)
        total = total + weight
        acc = acc + pack[0:HD, :].astype(jnp.float32) * weight
    attended = acc / total
    mean_square = jnp.mean(attended * attended, axis=0, keepdims=True)
    normed = jnp.transpose(attended * lax.rsqrt(mean_square + 1e-06))
    head_out[...] = (normed * gain[...]).astype(jnp.bfloat16)


def attend(kernel, operands, outs, scratch, folds):
    tok_count = 2 * KEYS
    return pl.pallas_call(
        kernel,
        out_shape=tuple(jax.ShapeDtypeStruct(*out) for out in outs),
        in_specs=[vmem] * len(operands),
        out_specs=(vmem,) * len(outs),
        scratch_shapes=[pltpu.VMEM(*shape) for shape in scratch],
        compiler_params=pltpu.CompilerParams(vmem_limit_bytes=12 << 20),
        cost_estimate=pl.CostEstimate(
            flops=8 * tok_count * tok_count * HD * folds,
            transcendentals=tok_count * tok_count * folds,
            bytes_accessed=1 << 20,
        ),
    )(*operands)


def attention(queries, key_vectors, value_vectors, forget_totals, head_gain):
    tok_count = queries.shape[0]

    def shift(array, dy, dx, needed):
        return lax.ppermute(array, "sp", sp_perm(dy, dx, needed))

    keys_own, own_pack = make_pieces(queries, key_vectors, value_vectors, forget_totals)
    low = shift(keys_own, 0, 1, lambda y, x: y < 3 or x > 0)
    high = shift(keys_own, 0, -1, lambda y, x: y < 3 or x in (0, 3))
    pack3 = shift(own_pack, 1, 0, lambda y, x: y == 0)
    pack2 = shift(own_pack, 2, 0, lambda y, x: y < 2)
    pack1 = shift(own_pack, -1, 0, lambda y, x: y < 3)
    far_a = shift(low[:PIECE], 0, 1, lambda y, x: y < 3 or x > 1)
    far_b = shift(high[PIECE:], 0, -1, lambda y, x: y < 3 or x > 1)

    narrow = ((8, tok_count), jnp.float32)
    state = [narrow, narrow, ((HD, tok_count), jnp.float32)]
    both = [((2 * shape[0], tok_count), kind) for shape, kind in state]
    result = ((PACK, tok_count), jnp.bfloat16)

    def loaded(count):
        shapes = (count * BLOCK, 2 * HD), (count * 2 * KEYS, 2 * HD), (2 * HD, tok_count)
        return [(shape, jnp.bfloat16) for shape in shapes]

    near = attend(distant_kernel, [pack3, pack2, keys_own, low, high], both, loaded(3), 6)
    far_a, far_b, near = lax.optimization_barrier((far_a, far_b, near))
    part3, part2 = attend(
        distant_end_kernel, [pack3, pack2, far_a, far_b, *near], [result] * 2, state + loaded(1), 2
    )
    part3, part2, pack1 = lax.optimization_barrier((part3, part2, pack1))
    back3 = shift(part3, -1, 0, lambda y, x: y == 3)
    back2 = shift(part2, 2, 0, lambda y, x: y > 1)
    keys = [keys_own, low, high, far_a, far_b]
    (part1,) = attend(next_kernel, [pack1, *keys], [result], state + loaded(4), 4)
    part1, own_pack, keys = lax.optimization_barrier((part1, own_pack, keys))
    back1 = shift(part1, 1, 0, lambda y, x: y > 0)
    own_state = attend(own_kernel, [own_pack, *keys], state, loaded(4), 4)
    (head_out,) = attend(
        merge_kernel,
        [back1, back2, back3, *own_state, head_gain.reshape(1, HD)],
        [((tok_count, HD), jnp.bfloat16)],
        [],
        0,
    )
    return head_out


def staging_kernel(gate, up, down, out, sems):
    tall, wide = gate.shape
    copies = [
        pltpu.make_async_copy(gate, out.at[pl.ds(0, tall)], sems.at[0]),
        pltpu.make_async_copy(up, out.at[pl.ds(tall, tall)], sems.at[1]),
    ]
    for i in range(down.shape[1] // wide):
        source = down.at[:, pl.ds(i * wide, wide)]
        into = out.at[pl.ds(2 * tall + i * down.shape[0], down.shape[0])]
        copies.append(pltpu.make_async_copy(source, into, sems.at[2 + i]))
    for copy in copies:
        copy.start()
    for copy in copies:
        copy.wait()


def stage_weights(gate, up, down):
    blocks = down.shape[1] // gate.shape[1]
    rows = 2 * gate.shape[0] + blocks * down.shape[0]
    return pl.pallas_call(
        staging_kernel,
        out_shape=jax.ShapeDtypeStruct((rows, gate.shape[1]), jnp.bfloat16),
        in_specs=[pl.BlockSpec(memory_space=pltpu.HBM)] * 3,
        out_specs=vmem,
        scratch_shapes=[pltpu.SemaphoreType.DMA((2 + blocks,))],
        compiler_params=pltpu.CompilerParams(vmem_limit_bytes=4 << 20),
        name="stage_weights",
    )(*in_hbm(gate, up, down))


def expert_kernel(*refs, count):
    rows, halves = refs[:count], refs[count : count + 2]
    outs = refs[count + 2 : 2 * count + 2]
    joined, made = refs[2 * count + 2 :]
    each, width = rows[0].shape
    units = halves[0].shape[1]
    for i, part in enumerate(rows):
        joined[i * each : (i + 1) * each, :] = part[...]
    tall = 128

    def block(i, carry):
        spot = pl.ds(pl.multiple_of(i * tall, tall), tall)
        mine = joined[spot, :]
        hidden = []
        for half in halves:
            gate_pre = jnp.dot(mine, half[0:width, :], preferred_element_type=jnp.float32)
            up_pre = jnp.dot(mine, half[width : 2 * width, :], preferred_element_type=jnp.float32)
            silu = gate_pre / (1.0 + jnp.exp(-gate_pre))
            hidden.append((silu * up_pre).astype(jnp.bfloat16))
        for col in range(0, width, units):
            at = 2 * width + col
            part = jnp.dot(
                hidden[0], halves[0][at : at + units, :], preferred_element_type=jnp.float32
            ) + jnp.dot(
                hidden[1], halves[1][at : at + units, :], preferred_element_type=jnp.float32
            )
            made[spot, col : col + units] = part.astype(jnp.bfloat16)
        return carry

    lax.fori_loop(0, joined.shape[0] // tall, block, 0)
    for i, out in enumerate(outs):
        out[...] = made[i * each : (i + 1) * each, :]


def expert_rows(rows, halves):
    count = len(rows)
    each, width = rows[0].shape
    flops = 2 * count * each * width * halves[0].shape[1] * 2 * 3
    joined = pltpu.VMEM((count * each, width), jnp.bfloat16)
    return pl.pallas_call(
        partial(expert_kernel, count=count),
        out_shape=tuple(jax.ShapeDtypeStruct((each, width), jnp.bfloat16) for _ in rows),
        in_specs=[vmem] * (count + 2),
        out_specs=(vmem,) * count,
        scratch_shapes=[joined, joined],
        compiler_params=pltpu.CompilerParams(vmem_limit_bytes=16 << 20),
        cost_estimate=pl.CostEstimate(flops=flops, transcendentals=0, bytes_accessed=6 << 20),
    )(*rows, *halves)


def added(left, right):
    return (left.astype(jnp.float32) + right.astype(jnp.float32)).astype(jnp.bfloat16)


def expert_sum(own, weights):
    def up(array):
        return lax.ppermute(array, "tp", z_perm(1))

    def down(array):
        return lax.ppermute(array, "tp", z_perm(-1))

    half = own.shape[0] // 2
    top, end = own[:half], own[half:]
    up_top, down_end, up_end, down_top = [top], [end], [end], [top]
    for _ in range(1, 4):
        up_top.append(up(up_top[-1]))
        down_end.append(down(down_end[-1]))
        up_end.append(up(up_end[-1]))
        down_top.append(down(down_top[-1]))
    up_top.append(up(up_top[-1]))
    down_end.append(down(down_end[-1]))
    chains = (up_top, up_end, down_top, down_end)
    rows = [top, end] + [chain[i] for i in (1, 2) for chain in chains]
    near = expert_rows(rows, weights)
    low_top, high_end = expert_rows([up_top[3], down_end[3]], weights)
    low_end3, high_top3 = expert_rows([up_end[3], down_top[3]], weights)
    far_top, far_end = expert_rows([up_top[4], down_end[4]], weights)
    mine, done = near[:2], [near[2:6], near[6:]]

    low_top, high_end = down(low_top), up(high_end)
    high_top, low_end = up(far_top), down(far_end)
    high_top = up(added(high_top, high_top3))
    low_end = down(added(low_end, low_end3))
    for i in (1, 0):
        low_top = down(added(low_top, done[i][0]))
        high_end = up(added(high_end, done[i][3]))
        high_top = up(added(high_top, done[i][2]))
        low_end = down(added(low_end, done[i][1]))
    sums = []
    for parts in ((low_top, high_top, mine[0]), (low_end, high_end, mine[1])):
        low, high, own_part = (part.astype(jnp.float32) for part in parts)
        sums.append((low + high + own_part).astype(jnp.bfloat16))
    return jnp.concatenate(sums)


def place_rows(routing, slot_count, capacity):
    expert_count, row_count = slot_count // capacity, routing.shape[1]
    expert_id = lax.broadcasted_iota(jnp.int32, (expert_count, row_count), 0)
    chosen = [(routing[k : k + 1, :] == expert_id).astype(jnp.float32) for k in range(TOP)]
    before = lax.broadcasted_iota(jnp.int32, (row_count, row_count), 0)
    before = before < lax.broadcasted_iota(jnp.int32, (row_count, row_count), 1)
    before = before.astype(jnp.float32).astype(jnp.bfloat16)
    counts = jnp.dot(
        sum(chosen).astype(jnp.bfloat16), before, preferred_element_type=jnp.float32
    )
    slot_id = lax.broadcasted_iota(jnp.int32, (slot_count, row_count), 0)
    here = []
    for k in range(TOP):
        rank = jnp.sum(counts * chosen[k], axis=0, keepdims=True).astype(jnp.int32)
        here.append(slot_id == routing[k : k + 1, :] * capacity + rank)
    return here


def project_kernel(
    heads, out_weight, stream, norm_gain, routing, route_weights, resid_sum, outgoing, mixing, joined
):
    for head in range(heads.shape[0]):
        joined[:, head * HD : (head + 1) * HD] = heads[head]
    slot_count = mixing.shape[0]
    experts = slot_count // max(2, 2 * TOP * stream.shape[0] // lax.axis_size("sp"))
    here = place_rows(routing[...], slot_count, slot_count // experts)
    mix = jnp.zeros(mixing.shape, jnp.float32)
    place = jnp.zeros(mixing.shape, jnp.float32)
    for k in range(TOP):
        mix = jnp.where(here[k], route_weights[k : k + 1, :], mix)
        place = jnp.where(here[k], 1.0, place)
    mixing[...] = mix
    wide = 512

    def column(j, carry):
        cols = pl.ds(pl.multiple_of(j * wide, wide), wide)
        mixed_rows = jnp.dot(joined[...], out_weight[:, cols], preferred_element_type=jnp.float32)
        resid_sum[:, cols] = stream[:, cols].astype(jnp.float32) + mixed_rows
        return carry

    lax.fori_loop(0, resid_sum.shape[1] // wide, column, 0)
    resid = resid_sum[...]
    center = resid - jnp.mean(resid, axis=1, keepdims=True)
    spread = jnp.mean(center * center, axis=1, keepdims=True)
    normed = (center * lax.rsqrt(spread + 1e-05) * norm_gain[...]).astype(jnp.bfloat16)
    outgoing[...] = jnp.dot(
        place.astype(jnp.bfloat16), normed, preferred_element_type=jnp.float32
    ).astype(jnp.bfloat16)


def project(heads, out_weight, stream, norm_gain, routing, route_weights, slot_count):
    rows, width = stream.shape
    return pl.pallas_call(
        project_kernel,
        out_shape=(
            jax.ShapeDtypeStruct((rows, width), jnp.float32),
            jax.ShapeDtypeStruct((slot_count, width), jnp.bfloat16),
            jax.ShapeDtypeStruct((slot_count, rows), jnp.float32),
        ),
        in_specs=[vmem] * 6,
        out_specs=(vmem,) * 3,
        scratch_shapes=[pltpu.VMEM((rows, heads.shape[0] * HD), jnp.bfloat16)],
        compiler_params=pltpu.CompilerParams(vmem_limit_bytes=14 << 20),
        name="project",
    )(
        heads,
        out_weight,
        stream,
        norm_gain.reshape(1, width),
        jnp.transpose(routing),
        jnp.transpose(route_weights),
    )


def combine_kernel(resid_sum, returned, mixing, out):
    total = resid_sum[...]
    for part in three_parts(mixing[...]):
        total = total + lax.dot_general(
            part, returned[...], (((0,), (0,)), ((), ())), preferred_element_type=jnp.float32
        )
    out[...] = total.astype(jnp.bfloat16)


def combine(resid_sum, returned, mixing):
    return pl.pallas_call(
        combine_kernel,
        out_shape=jax.ShapeDtypeStruct(resid_sum.shape, jnp.bfloat16),
        in_specs=[vmem] * 3,
        out_specs=vmem,
        compiler_params=pltpu.CompilerParams(vmem_limit_bytes=6 << 20),
        name="combine",
    )(resid_sum, returned, mixing)


def on_device(
    queries,
    key_vectors,
    value_vectors,
    forget_totals,
    head_gain,
    stream,
    out_weight,
    norm_gain,
    routing,
    route_weights,
    gate_weight,
    up_weight,
    down_weight,
):
    sp_count = lax.axis_size("sp")
    head_out = attention(queries, key_vectors, value_vectors, forget_totals, head_gain)
    row_count, width = stream.shape
    capacity = max(2, 2 * TOP * row_count // sp_count)
    heads = head_out.reshape(-1, row_count, HD)
    heads = lax.all_to_all(heads, "tp", split_axis=0, concat_axis=0, tiled=True)
    resid_sum, outgoing, mixing = project(
        heads, out_weight, stream, norm_gain, routing, route_weights, sp_count * capacity
    )
    outgoing = outgoing.reshape(sp_count, capacity, width)
    arrived = lax.all_to_all(outgoing, "sp", split_axis=0, concat_axis=0, tiled=True)
    own_weights = gate_weight[0], up_weight[0], down_weight[0]
    arrived, own_weights = lax.optimization_barrier((arrived, own_weights))
    own_half = stage_weights(*own_weights)
    weights = own_half, lax.ppermute(own_half, "tp", core_swap)
    summed = expert_sum(arrived.reshape(-1, width), weights)
    expert_out = summed.reshape(sp_count, capacity, width)
    returned = lax.all_to_all(expert_out, "sp", split_axis=0, concat_axis=0, tiled=True)
    return combine(resid_sum, returned.reshape(-1, width), mixing)


def solution(mesh):
    in_specs = (
        P("sp", "tp"),
        P("sp", "tp"),
        P("sp", "tp"),
        P("sp", "tp"),
        P("tp"),
        P(("sp", "tp"), None),
        P(),
        P(),
        P(("sp", "tp"), None),
        P(("sp", "tp"), None),
        P("sp", None, "tp"),
        P("sp", None, "tp"),
        P("sp", "tp", None),
    )
    out_specs = P(("sp", "tp"), None)
    return jax.shard_map(
        on_device, mesh=mesh, in_specs=in_specs, out_specs=out_specs, check_vma=False
    )
```

```python
from functools import partial

import jax
import jax.numpy as jnp
from jax import lax
from jax.experimental import pallas as pl
from jax.experimental.pallas import tpu as pltpu
from jax.sharding import PartitionSpec as P


HD = 128
TOP = 2
LOG2E = 1.4426950408889634
low_score = -1e30
GATE_ROWS = 16
KEYS = 256
PIECE = KEYS + GATE_ROWS
BLOCK = 2 * PIECE
PACK = HD + GATE_ROWS


def sp_perm(dy, dx, needed):
    pairs = []
    for y in range(4):
        for x in range(4):
            into = (y + dy) % 4, (x + dx) % 4
            if needed(*into):
                pairs.append((y * 4 + x, into[0] * 4 + into[1]))
    return pairs


def z_perm(dz):
    return [(z * 2 + c, ((z + dz) % 8) * 2 + c) for z in range(8) for c in range(2)]


core_swap = [(i, i ^ 1) for i in range(16)]


vmem = pl.BlockSpec(memory_space=pltpu.VMEM)


def in_hbm(*arrays):
    return [pltpu.with_memory_space_constraint(array, pltpu.HBM) for array in arrays]


def three_parts(wide):
    first = wide.astype(jnp.bfloat16)
    rest = wide - first.astype(jnp.float32)
    second = rest.astype(jnp.bfloat16)
    third = (rest - second.astype(jnp.float32)).astype(jnp.bfloat16)
    return first, second, third


def piece_kernel(*refs):
    sources, outs, staged, sems = refs[:4], refs[4:6], refs[6:10], refs[10]
    copies = [
        pltpu.make_async_copy(source, into, sems.at[i])
        for i, (source, into) in enumerate(zip(sources, staged))
    ]
    for copy in copies:
        copy.start()
    for copy in copies:
        copy.wait()
    queries, keys, values, gates = staged
    keys_own, query_pack = outs
    stretched = gates[...] * HD**0.5
    tok_count = stretched.shape[1]
    row = lax.broadcasted_iota(jnp.int32, (GATE_ROWS, KEYS), 0)
    for i in range(2):
        at_row = i * PIECE
        rows = slice(i * KEYS, (i + 1) * KEYS)
        keys_own[at_row : at_row + HD, :] = jnp.transpose(values[rows, :])
        keys_own[at_row + HD : at_row + KEYS, 0:HD] = keys[i * KEYS : i * KEYS + HD, :]
        keys_own[at_row + HD : at_row + KEYS, HD:KEYS] = keys[i * KEYS + HD : (i + 1) * KEYS, :]
        parts = [part.astype(jnp.float32) for part in three_parts(-stretched[:, rows])]
        block = jnp.where((row >= 3) & (row < 6), 1.0, 0.0)
        for at, part in enumerate(parts):
            block = jnp.where(row == at, part, block)
        keys_own[at_row + KEYS : at_row + PIECE, :] = block.astype(jnp.bfloat16)
    wide_row = lax.broadcasted_iota(jnp.int32, (GATE_ROWS, tok_count), 0)
    mix = jnp.where(wide_row < 3, 1.0, 0.0)
    parts = [part.astype(jnp.float32) for part in three_parts(stretched[:, 0:1])]
    for at, part in enumerate(parts):
        mix = jnp.where(wide_row == 3 + at, part, mix)
    mix = jnp.where(wide_row == 6, low_score, mix)
    query_pack[HD:PACK, :] = mix.astype(jnp.bfloat16)
    query_pack[0:HD, :] = jnp.transpose(queries[...])


def make_pieces(queries, keys, values, gates):
    tok_count = queries.shape[0]
    return pl.pallas_call(
        piece_kernel,
        out_shape=(
            jax.ShapeDtypeStruct((BLOCK, 2 * HD), jnp.bfloat16),
            jax.ShapeDtypeStruct((PACK, tok_count), jnp.bfloat16),
        ),
        in_specs=[pl.BlockSpec(memory_space=pltpu.HBM)] * 4,
        out_specs=(vmem,) * 2,
        scratch_shapes=[pltpu.VMEM((tok_count, HD), jnp.bfloat16)] * 3
        + [pltpu.VMEM((1, tok_count), jnp.float32), pltpu.SemaphoreType.DMA((4,))],
        compiler_params=pltpu.CompilerParams(vmem_limit_bytes=6 << 20),
        name="make_pieces",
    )(*in_hbm(queries, keys, values, gates.reshape(1, tok_count)))


def fold(query_wide, state, stack, keys_wide, block, own_block=False):
    run_max, run_sum, run_acc = state
    tok_count = query_wide.shape[1]
    scale = HD ** (-0.5) * LOG2E
    scores = []
    for part in range(2 * KEYS // HD):
        spot = pl.ds(pl.multiple_of(block * (2 * KEYS) + part * HD, HD), HD)
        score = jnp.dot(
            keys_wide[spot, :], query_wide[...], preferred_element_type=jnp.float32
        )
        if own_block:
            key_at = lax.broadcasted_iota(jnp.int32, score.shape, 0) + part * HD
            query_at = lax.broadcasted_iota(jnp.int32, score.shape, 1)
            score = jnp.where(key_at <= query_at, score, low_score)
        scores.append(score)
    old_max = run_max[0:1, :]
    peak = scores[0]
    for score in scores[1:]:
        peak = jnp.maximum(peak, score)
    new_max = jnp.maximum(old_max, jnp.max(peak, axis=0, keepdims=True))
    rescale = jnp.exp2((old_max - new_max) * scale)
    scaled_max = new_max * scale
    total = run_sum[...] * rescale
    acc = run_acc[...] * rescale
    for i in range(2):
        at = pl.multiple_of(block * BLOCK + i * PIECE, GATE_ROWS)
        rounded = []
        for score in scores[2 * i : 2 * i + 2]:
            lifted = jnp.exp2(score * scale - scaled_max)
            total = total + jnp.sum(lifted.reshape(HD // 8, 8, tok_count), axis=0)
            rounded.append(lifted.astype(jnp.bfloat16))
        acc = acc + jnp.dot(
            stack[pl.ds(at, HD), :],
            jnp.concatenate(rounded, axis=0),
            preferred_element_type=jnp.float32,
        )
    run_sum[...] = total
    run_acc[...] = acc
    run_max[...] = jnp.broadcast_to(new_max, run_max.shape)


def clear(state):
    run_max, run_sum, run_acc = state
    run_max[...] = jnp.full(run_max.shape, low_score, jnp.float32)
    run_sum[...] = jnp.zeros(run_sum.shape, jnp.float32)
    run_acc[...] = jnp.zeros(run_acc.shape, jnp.float32)


def nth_state(state, i):
    found = []
    for ref in state:
        rows = ref.shape[0] // 4
        found.append(ref.at[pl.ds(pl.multiple_of(i * rows, 8), rows)])
    return found


def fold_blocks(query_wide, state, stack, keys_wide, first, count, seen=None):
    def block(i, carry):
        run = partial(fold, query_wide, state, stack, keys_wide, i)
        if seen is None:
            run()
        else:
            pl.when(seen(i))(run)
        return carry

    lax.fori_loop(first, first + count, block, 0)


def load_blocks(stack, keys_wide, parts):
    at = 0
    for part in parts:
        stack[at : at + part.shape[0], :] = part[...]
        at += part.shape[0]
    for piece in range(at // PIECE):
        row, at = piece * KEYS, piece * PIECE
        for half in range(KEYS // HD):
            keys_wide[row + half * HD : row + (half + 1) * HD, 0:HD] = stack[
                at + HD : at + 2 * HD, half * HD : (half + 1) * HD
            ]
        gates = stack[at + KEYS : at + PIECE, :].astype(jnp.float32)
        rest = jnp.zeros((HD - GATE_ROWS, KEYS), jnp.float32)
        columns = jnp.transpose(jnp.concatenate([gates, rest], axis=0))
        keys_wide[row : row + KEYS, HD : 2 * HD] = columns.astype(jnp.bfloat16)


def load_query(query_wide, pack):
    query_wide[0:PACK, :] = pack[...]
    query_wide[PACK : 2 * HD, :] = jnp.zeros((2 * HD - PACK, pack.shape[1]), jnp.bfloat16)


def pack_result(state, out):
    run_max, run_sum, run_acc = state
    total = jnp.sum(run_sum[...], axis=0, keepdims=True)
    out[0:HD, :] = (run_acc[...] / total).astype(jnp.bfloat16)
    row = lax.broadcasted_iota(jnp.int32, (GATE_ROWS, total.shape[1]), 0)
    block = jnp.zeros(row.shape, jnp.float32)
    for at, part in enumerate(three_parts(run_max[0:1, :]) + three_parts(total)):
        block = jnp.where(row == at, part.astype(jnp.float32), block)
    out[HD:PACK, :] = block.astype(jnp.bfloat16)


def near_kernel(*refs):
    packs, keys, states = refs[:4], refs[4:7], refs[7:10]
    stack, keys_wide, query_wide = refs[10:]
    own = lax.axis_index("sp")
    own_y, own_x = own >> 2, own & 3
    load_blocks(stack, keys_wide, keys)

    def each(i, carry):
        @pl.when(own_y <= i)
        def _():
            for at, pack in enumerate(packs[:3]):
                pl.when(i == at)(partial(load_query, query_wide, pack))
            state = nth_state(states, i)
            clear(state)
            fold_blocks(query_wide, state, stack, keys_wide, 0, 3)

        return carry

    lax.fori_loop(0, 3, each, 0)
    state = nth_state(states, 3)
    load_query(query_wide, packs[3])
    clear(state)
    fold(query_wide, state, stack, keys_wide, 0, own_block=True)

    def seen(i):
        return ((own_x + jnp.where(i == 1, -1, 1)) & 3) < own_x

    fold_blocks(query_wide, state, stack, keys_wide, 1, 2, seen)


def end_kernel(*refs, first):
    packs, far, states, outs = refs[:2], refs[2:4], refs[4:7], refs[7:-6]
    state, (stack, keys_wide, query_wide) = refs[-6:-3], refs[-3:]
    own = lax.axis_index("sp")
    own_y, own_x = own >> 2, own & 3
    load_blocks(stack, keys_wide, far)

    def each(i, carry):
        needed = own_y <= first + i
        if first == 2:
            needed = jnp.where(i == 0, needed, ((own_x + 2) & 3) < own_x)
        for into, came in zip(state, nth_state(states, first + i)):
            into[...] = came[...]

        @pl.when(needed)
        def _():
            for at, pack in enumerate(packs):
                pl.when(i == at)(partial(load_query, query_wide, pack))
            fold(query_wide, state, stack, keys_wide, 0)

        for at in range(1 if first == 2 else 2):
            pl.when(jnp.logical_and(i == at, needed))(partial(pack_result, state, outs[at]))
        return carry

    lax.fori_loop(0, 2, each, 0)
    if first == 2:
        for out, ref in zip(outs[1:], state):
            out[...] = ref[...]


def merge_kernel(*refs):
    came, own_state, gain, head_out = refs[:3], refs[3:6], refs[6], refs[7]
    own_y = lax.axis_index("sp") >> 2
    scale = HD ** (-0.5) * LOG2E
    peaks = [own_state[0][0:1, :]]
    totals = [jnp.sum(own_state[1][...], axis=0, keepdims=True)]
    for above, pack in enumerate(came):
        rows = pack[HD:PACK, :].astype(jnp.float32)
        parts = [rows[at : at + 1, :] for at in range(6)]
        valid = own_y > above
        peaks.append(jnp.where(valid, parts[0] + parts[1] + parts[2], low_score))
        totals.append(jnp.where(valid, parts[3] + parts[4] + parts[5], 0.0))
    top = peaks[0]
    for peak in peaks[1:]:
        top = jnp.maximum(top, peak)
    weight = jnp.exp2((peaks[0] - top) * scale)
    total = totals[0] * weight
    acc = own_state[2][...] * weight
    for pack, peak, share in zip(came, peaks[1:], totals[1:]):
        weight = share * jnp.exp2((peak - top) * scale)
        total = total + weight
        acc = acc + pack[0:HD, :].astype(jnp.float32) * weight
    attended = acc / total
    mean_square = jnp.mean(attended * attended, axis=0, keepdims=True)
    normed = jnp.transpose(attended * lax.rsqrt(mean_square + 1e-06))
    head_out[...] = (normed * gain[...]).astype(jnp.bfloat16)


def attend(kernel, operands, outs, scratch, folds):
    tok_count = 2 * KEYS
    return pl.pallas_call(
        kernel,
        out_shape=tuple(jax.ShapeDtypeStruct(*out) for out in outs),
        in_specs=[vmem] * len(operands),
        out_specs=(vmem,) * len(outs),
        scratch_shapes=[pltpu.VMEM(*shape) for shape in scratch],
        compiler_params=pltpu.CompilerParams(vmem_limit_bytes=12 << 20),
        cost_estimate=pl.CostEstimate(
            flops=8 * tok_count * tok_count * HD * folds,
            transcendentals=tok_count * tok_count * folds,
            bytes_accessed=1 << 20,
        ),
    )(*operands)


def attention(queries, key_vectors, value_vectors, forget_totals, head_gain, weights):
    tok_count = queries.shape[0]

    def shift(array, dy, dx, needed):
        return lax.ppermute(array, "sp", sp_perm(dy, dx, needed))

    keys_own, own_pack = make_pieces(queries, key_vectors, value_vectors, forget_totals)
    low = shift(keys_own, 0, 1, lambda y, x: y < 3 or x > 0)
    high = shift(keys_own, 0, -1, lambda y, x: y < 3 or x in (0, 3))
    pack3 = shift(own_pack, 1, 0, lambda y, x: y == 0)
    pack2 = shift(own_pack, 2, 0, lambda y, x: y < 2)
    pack1 = shift(own_pack, -1, 0, lambda y, x: y < 3)
    far_a = shift(low[:PIECE], 0, 1, lambda y, x: y < 3 or x > 1)
    far_b = shift(high[PIECE:], 0, -1, lambda y, x: y < 3 or x > 1)

    narrow = ((8, tok_count), jnp.float32)
    state = [narrow, narrow, ((HD, tok_count), jnp.float32)]
    all_states = [((4 * shape[0], tok_count), kind) for shape, kind in state]
    result = ((PACK, tok_count), jnp.bfloat16)

    def loaded(count):
        shapes = (count * BLOCK, 2 * HD), (count * 2 * KEYS, 2 * HD), (2 * HD, tok_count)
        return [(shape, jnp.bfloat16) for shape in shapes]

    packs = [pack3, pack2, pack1, own_pack]
    near = attend(near_kernel, [*packs, keys_own, low, high], all_states, loaded(3), 12)
    weights, near = lax.optimization_barrier((weights, near))
    staged = stage_weights(*weights)

    def end(first, outs):
        operands = [*packs[first : first + 2], far_a, far_b, *near]
        return attend(partial(end_kernel, first=first), operands, outs, state + loaded(1), 2)

    part3, part2 = end(0, [result] * 2)
    part3, part2, near = lax.optimization_barrier((part3, part2, near))
    back3 = shift(part3, -1, 0, lambda y, x: y == 3)
    back2 = shift(part2, 2, 0, lambda y, x: y > 1)
    part1, *own_state = end(2, [result] + state)
    back1 = shift(part1, 1, 0, lambda y, x: y > 0)
    (head_out,) = attend(
        merge_kernel,
        [back1, back2, back3, *own_state, head_gain.reshape(1, HD)],
        [((tok_count, HD), jnp.bfloat16)],
        [],
        0,
    )
    return head_out, staged


def staging_kernel(gate, up, down, out, sems):
    tall, wide = gate.shape
    copies = [
        pltpu.make_async_copy(gate, out.at[pl.ds(0, tall)], sems.at[0]),
        pltpu.make_async_copy(up, out.at[pl.ds(tall, tall)], sems.at[1]),
    ]
    for i in range(down.shape[1] // wide):
        source = down.at[:, pl.ds(i * wide, wide)]
        into = out.at[pl.ds(2 * tall + i * down.shape[0], down.shape[0])]
        copies.append(pltpu.make_async_copy(source, into, sems.at[2 + i]))
    for copy in copies:
        copy.start()
    for copy in copies:
        copy.wait()


def stage_weights(gate, up, down):
    blocks = down.shape[1] // gate.shape[1]
    rows = 2 * gate.shape[0] + blocks * down.shape[0]
    return pl.pallas_call(
        staging_kernel,
        out_shape=jax.ShapeDtypeStruct((rows, gate.shape[1]), jnp.bfloat16),
        in_specs=[pl.BlockSpec(memory_space=pltpu.HBM)] * 3,
        out_specs=vmem,
        scratch_shapes=[pltpu.SemaphoreType.DMA((2 + blocks,))],
        compiler_params=pltpu.CompilerParams(vmem_limit_bytes=4 << 20),
        name="stage_weights",
    )(*in_hbm(gate, up, down))


def expert_kernel(*refs, count):
    rows, halves = refs[:count], refs[count : count + 2]
    outs = refs[count + 2 : 2 * count + 2]
    joined, made = refs[2 * count + 2 :]
    each, width = rows[0].shape
    units = halves[0].shape[1]
    for i, part in enumerate(rows):
        joined[i * each : (i + 1) * each, :] = part[...]
    tall = 128

    def block(i, carry):
        spot = pl.ds(pl.multiple_of(i * tall, tall), tall)
        mine = joined[spot, :]
        hidden = []
        for half in halves:
            gate_pre = jnp.dot(mine, half[0:width, :], preferred_element_type=jnp.float32)
            up_pre = jnp.dot(mine, half[width : 2 * width, :], preferred_element_type=jnp.float32)
            silu = gate_pre / (1.0 + jnp.exp(-gate_pre))
            hidden.append((silu * up_pre).astype(jnp.bfloat16))
        for col in range(0, width, units):
            at = 2 * width + col
            part = jnp.dot(
                hidden[0], halves[0][at : at + units, :], preferred_element_type=jnp.float32
            ) + jnp.dot(
                hidden[1], halves[1][at : at + units, :], preferred_element_type=jnp.float32
            )
            made[spot, col : col + units] = part.astype(jnp.bfloat16)
        return carry

    lax.fori_loop(0, joined.shape[0] // tall, block, 0)
    for i, out in enumerate(outs):
        out[...] = made[i * each : (i + 1) * each, :]


def expert_rows(rows, halves):
    count = len(rows)
    each, width = rows[0].shape
    flops = 2 * count * each * width * halves[0].shape[1] * 2 * 3
    joined = pltpu.VMEM((count * each, width), jnp.bfloat16)
    return pl.pallas_call(
        partial(expert_kernel, count=count),
        out_shape=tuple(jax.ShapeDtypeStruct((each, width), jnp.bfloat16) for _ in rows),
        in_specs=[vmem] * (count + 2),
        out_specs=(vmem,) * count,
        scratch_shapes=[joined, joined],
        compiler_params=pltpu.CompilerParams(vmem_limit_bytes=16 << 20),
        cost_estimate=pl.CostEstimate(flops=flops, transcendentals=0, bytes_accessed=6 << 20),
    )(*rows, *halves)


def added(left, right):
    return (left.astype(jnp.float32) + right.astype(jnp.float32)).astype(jnp.bfloat16)


def expert_sum(own, weights):
    def up(array):
        return lax.ppermute(array, "tp", z_perm(1))

    def down(array):
        return lax.ppermute(array, "tp", z_perm(-1))

    half = own.shape[0] // 2
    top, end = own[:half], own[half:]
    up_top, down_end, up_end, down_top = [top], [end], [end], [top]
    for _ in range(1, 4):
        up_top.append(up(up_top[-1]))
        down_end.append(down(down_end[-1]))
        up_end.append(up(up_end[-1]))
        down_top.append(down(down_top[-1]))
    up_top.append(up(up_top[-1]))
    down_end.append(down(down_end[-1]))
    chains = (up_top, up_end, down_top, down_end)
    made = []
    for i in range(1, 4):
        rows = [chain[i] for chain in chains]
        made.append(expert_rows(([top, end] if i == 1 else []) + rows, weights))
    mine, done = made[0][:2], [made[0][2:], made[1], made[2]]
    far_top, far_end = expert_rows([up_top[4], down_end[4]], weights)

    low_top, high_end = down(done[2][0]), up(done[2][3])
    high_top, low_end = up(far_top), down(far_end)
    high_top = up(added(high_top, done[2][2]))
    low_end = down(added(low_end, done[2][1]))
    for i in (1, 0):
        low_top = down(added(low_top, done[i][0]))
        high_end = up(added(high_end, done[i][3]))
        high_top = up(added(high_top, done[i][2]))
        low_end = down(added(low_end, done[i][1]))
    sums = []
    for parts in ((low_top, high_top, mine[0]), (low_end, high_end, mine[1])):
        low, high, own_part = (part.astype(jnp.float32) for part in parts)
        sums.append((low + high + own_part).astype(jnp.bfloat16))
    return jnp.concatenate(sums)


def place_rows(routing, slot_count, capacity):
    expert_count, row_count = slot_count // capacity, routing.shape[1]
    expert_id = lax.broadcasted_iota(jnp.int32, (expert_count, row_count), 0)
    chosen = [(routing[k : k + 1, :] == expert_id).astype(jnp.float32) for k in range(TOP)]
    before = lax.broadcasted_iota(jnp.int32, (row_count, row_count), 0)
    before = before < lax.broadcasted_iota(jnp.int32, (row_count, row_count), 1)
    before = before.astype(jnp.float32).astype(jnp.bfloat16)
    counts = jnp.dot(
        sum(chosen).astype(jnp.bfloat16), before, preferred_element_type=jnp.float32
    )
    slot_id = lax.broadcasted_iota(jnp.int32, (slot_count, row_count), 0)
    here = []
    for k in range(TOP):
        rank = jnp.sum(counts * chosen[k], axis=0, keepdims=True).astype(jnp.int32)
        here.append(slot_id == routing[k : k + 1, :] * capacity + rank)
    return here


def project_kernel(
    heads, out_weight, stream, norm_gain, routing, route_weights, resid_sum, outgoing, mixing, joined
):
    for head in range(heads.shape[0]):
        joined[:, head * HD : (head + 1) * HD] = heads[head]
    slot_count = mixing.shape[0]
    experts = slot_count // max(2, 2 * TOP * stream.shape[0] // lax.axis_size("sp"))
    here = place_rows(routing[...], slot_count, slot_count // experts)
    mix = jnp.zeros(mixing.shape, jnp.float32)
    place = jnp.zeros(mixing.shape, jnp.float32)
    for k in range(TOP):
        mix = jnp.where(here[k], route_weights[k : k + 1, :], mix)
        place = jnp.where(here[k], 1.0, place)
    mixing[...] = mix
    wide = 512

    def column(j, carry):
        cols = pl.ds(pl.multiple_of(j * wide, wide), wide)
        mixed_rows = jnp.dot(joined[...], out_weight[:, cols], preferred_element_type=jnp.float32)
        resid_sum[:, cols] = stream[:, cols].astype(jnp.float32) + mixed_rows
        return carry

    lax.fori_loop(0, resid_sum.shape[1] // wide, column, 0)
    resid = resid_sum[...]
    center = resid - jnp.mean(resid, axis=1, keepdims=True)
    spread = jnp.mean(center * center, axis=1, keepdims=True)
    normed = (center * lax.rsqrt(spread + 1e-05) * norm_gain[...]).astype(jnp.bfloat16)
    outgoing[...] = jnp.dot(
        place.astype(jnp.bfloat16), normed, preferred_element_type=jnp.float32
    ).astype(jnp.bfloat16)


def project(heads, out_weight, stream, norm_gain, routing, route_weights, slot_count):
    rows, width = stream.shape
    return pl.pallas_call(
        project_kernel,
        out_shape=(
            jax.ShapeDtypeStruct((rows, width), jnp.float32),
            jax.ShapeDtypeStruct((slot_count, width), jnp.bfloat16),
            jax.ShapeDtypeStruct((slot_count, rows), jnp.float32),
        ),
        in_specs=[vmem] * 6,
        out_specs=(vmem,) * 3,
        scratch_shapes=[pltpu.VMEM((rows, heads.shape[0] * HD), jnp.bfloat16)],
        compiler_params=pltpu.CompilerParams(vmem_limit_bytes=14 << 20),
        name="project",
    )(
        heads,
        out_weight,
        stream,
        norm_gain.reshape(1, width),
        jnp.transpose(routing),
        jnp.transpose(route_weights),
    )


def combine_kernel(resid_sum, returned, mixing, out):
    total = resid_sum[...]
    for part in three_parts(mixing[...]):
        total = total + lax.dot_general(
            part, returned[...], (((0,), (0,)), ((), ())), preferred_element_type=jnp.float32
        )
    out[...] = total.astype(jnp.bfloat16)


def combine(resid_sum, returned, mixing):
    return pl.pallas_call(
        combine_kernel,
        out_shape=jax.ShapeDtypeStruct(resid_sum.shape, jnp.bfloat16),
        in_specs=[vmem] * 3,
        out_specs=vmem,
        compiler_params=pltpu.CompilerParams(vmem_limit_bytes=6 << 20),
        name="combine",
    )(resid_sum, returned, mixing)


def on_device(
    queries,
    key_vectors,
    value_vectors,
    forget_totals,
    head_gain,
    stream,
    out_weight,
    norm_gain,
    routing,
    route_weights,
    gate_weight,
    up_weight,
    down_weight,
):
    sp_count = lax.axis_size("sp")
    head_out, own_half = attention(
        queries,
        key_vectors,
        value_vectors,
        forget_totals,
        head_gain,
        (gate_weight[0], up_weight[0], down_weight[0]),
    )
    weights = own_half, lax.ppermute(own_half, "tp", core_swap)
    row_count, width = stream.shape
    capacity = max(2, 2 * TOP * row_count // sp_count)
    heads = head_out.reshape(-1, row_count, HD)
    heads = lax.all_to_all(heads, "tp", split_axis=0, concat_axis=0, tiled=True)
    resid_sum, outgoing, mixing = project(
        heads, out_weight, stream, norm_gain, routing, route_weights, sp_count * capacity
    )
    outgoing = outgoing.reshape(sp_count, capacity, width)
    arrived = lax.all_to_all(outgoing, "sp", split_axis=0, concat_axis=0, tiled=True)
    summed = expert_sum(arrived.reshape(-1, width), weights)
    expert_out = summed.reshape(sp_count, capacity, width)
    returned = lax.all_to_all(expert_out, "sp", split_axis=0, concat_axis=0, tiled=True)
    return combine(resid_sum, returned.reshape(-1, width), mixing)


def solution(mesh):
    in_specs = (
        P("sp", "tp"),
        P("sp", "tp"),
        P("sp", "tp"),
        P("sp", "tp"),
        P("tp"),
        P(("sp", "tp"), None),
        P(),
        P(),
        P(("sp", "tp"), None),
        P(("sp", "tp"), None),
        P("sp", None, "tp"),
        P("sp", None, "tp"),
        P("sp", "tp", None),
    )
    out_specs = P(("sp", "tp"), None)
    return jax.shard_map(
        on_device, mesh=mesh, in_specs=in_specs, out_specs=out_specs, check_vma=False
    )
```

```python
from functools import partial

import jax
import jax.numpy as jnp
from jax import lax
from jax.experimental import pallas as pl
from jax.experimental.pallas import tpu as pltpu
from jax.sharding import PartitionSpec as P


HD = 128
TOP = 2
LOG2E = 1.4426950408889634
low_score = -1e30
GATE_ROWS = 16
KEYS = 256
PIECE = KEYS + GATE_ROWS
BLOCK = 2 * PIECE
PACK = HD + GATE_ROWS


def sp_perm(dy, dx, needed):
    pairs = []
    for y in range(4):
        for x in range(4):
            into = (y + dy) % 4, (x + dx) % 4
            if needed(*into):
                pairs.append((y * 4 + x, into[0] * 4 + into[1]))
    return pairs


def z_perm(dz):
    return [(z * 2 + c, ((z + dz) % 8) * 2 + c) for z in range(8) for c in range(2)]


core_swap = [(i, i ^ 1) for i in range(16)]


vmem = pl.BlockSpec(memory_space=pltpu.VMEM)


def in_hbm(*arrays):
    return [pltpu.with_memory_space_constraint(array, pltpu.HBM) for array in arrays]


def three_parts(wide):
    first = wide.astype(jnp.bfloat16)
    rest = wide - first.astype(jnp.float32)
    second = rest.astype(jnp.bfloat16)
    third = (rest - second.astype(jnp.float32)).astype(jnp.bfloat16)
    return first, second, third


def piece_kernel(*refs):
    sources, outs, staged, sems = refs[:4], refs[4:6], refs[6:10], refs[10]
    copies = [
        pltpu.make_async_copy(source, into, sems.at[i])
        for i, (source, into) in enumerate(zip(sources, staged))
    ]
    for copy in copies:
        copy.start()
    for copy in copies:
        copy.wait()
    queries, keys, values, gates = staged
    keys_own, query_pack = outs
    stretched = gates[...] * HD**0.5
    tok_count = stretched.shape[1]
    row = lax.broadcasted_iota(jnp.int32, (GATE_ROWS, KEYS), 0)
    for i in range(2):
        at_row = i * PIECE
        rows = slice(i * KEYS, (i + 1) * KEYS)
        keys_own[at_row : at_row + HD, :] = jnp.transpose(values[rows, :])
        keys_own[at_row + HD : at_row + KEYS, 0:HD] = keys[i * KEYS : i * KEYS + HD, :]
        keys_own[at_row + HD : at_row + KEYS, HD:KEYS] = keys[i * KEYS + HD : (i + 1) * KEYS, :]
        parts = [part.astype(jnp.float32) for part in three_parts(-stretched[:, rows])]
        block = jnp.where((row >= 3) & (row < 6), 1.0, 0.0)
        for at, part in enumerate(parts):
            block = jnp.where(row == at, part, block)
        keys_own[at_row + KEYS : at_row + PIECE, :] = block.astype(jnp.bfloat16)
    wide_row = lax.broadcasted_iota(jnp.int32, (GATE_ROWS, tok_count), 0)
    mix = jnp.where(wide_row < 3, 1.0, 0.0)
    parts = [part.astype(jnp.float32) for part in three_parts(stretched[:, 0:1])]
    for at, part in enumerate(parts):
        mix = jnp.where(wide_row == 3 + at, part, mix)
    mix = jnp.where(wide_row == 6, low_score, mix)
    query_pack[HD:PACK, :] = mix.astype(jnp.bfloat16)
    query_pack[0:HD, :] = jnp.transpose(queries[...])


def make_pieces(queries, keys, values, gates):
    tok_count = queries.shape[0]
    return pl.pallas_call(
        piece_kernel,
        out_shape=(
            jax.ShapeDtypeStruct((BLOCK, 2 * HD), jnp.bfloat16),
            jax.ShapeDtypeStruct((PACK, tok_count), jnp.bfloat16),
        ),
        in_specs=[pl.BlockSpec(memory_space=pltpu.HBM)] * 4,
        out_specs=(vmem,) * 2,
        scratch_shapes=[pltpu.VMEM((tok_count, HD), jnp.bfloat16)] * 3
        + [pltpu.VMEM((1, tok_count), jnp.float32), pltpu.SemaphoreType.DMA((4,))],
        compiler_params=pltpu.CompilerParams(vmem_limit_bytes=6 << 20),
        name="make_pieces",
    )(*in_hbm(queries, keys, values, gates.reshape(1, tok_count)))


def fold(query_wide, state, stack, keys_wide, block, own_block=False):
    run_max, run_sum, run_acc = state
    tok_count = query_wide.shape[1]
    scale = HD ** (-0.5) * LOG2E
    scores = []
    for part in range(2 * KEYS // HD):
        spot = pl.ds(pl.multiple_of(block * (2 * KEYS) + part * HD, HD), HD)
        score = jnp.dot(
            keys_wide[spot, :], query_wide[...], preferred_element_type=jnp.float32
        )
        if own_block:
            key_at = lax.broadcasted_iota(jnp.int32, score.shape, 0) + part * HD
            query_at = lax.broadcasted_iota(jnp.int32, score.shape, 1)
            score = jnp.where(key_at <= query_at, score, low_score)
        scores.append(score)
    old_max = run_max[0:1, :]
    peak = scores[0]
    for score in scores[1:]:
        peak = jnp.maximum(peak, score)
    new_max = jnp.maximum(old_max, jnp.max(peak, axis=0, keepdims=True))
    rescale = jnp.exp2((old_max - new_max) * scale)
    scaled_max = new_max * scale
    total = run_sum[...] * rescale
    acc = run_acc[...] * rescale
    for i in range(2):
        at = pl.multiple_of(block * BLOCK + i * PIECE, GATE_ROWS)
        rounded = []
        for score in scores[2 * i : 2 * i + 2]:
            lifted = jnp.exp2(score * scale - scaled_max)
            total = total + jnp.sum(lifted.reshape(HD // 8, 8, tok_count), axis=0)
            rounded.append(lifted.astype(jnp.bfloat16))
        acc = acc + jnp.dot(
            stack[pl.ds(at, HD), :],
            jnp.concatenate(rounded, axis=0),
            preferred_element_type=jnp.float32,
        )
    run_sum[...] = total
    run_acc[...] = acc
    run_max[...] = jnp.broadcast_to(new_max, run_max.shape)


def clear(state):
    run_max, run_sum, run_acc = state
    run_max[...] = jnp.full(run_max.shape, low_score, jnp.float32)
    run_sum[...] = jnp.zeros(run_sum.shape, jnp.float32)
    run_acc[...] = jnp.zeros(run_acc.shape, jnp.float32)


def nth_state(state, i):
    found = []
    for ref in state:
        rows = ref.shape[0] // 3
        found.append(ref.at[pl.ds(pl.multiple_of(i * rows, 8), rows)])
    return found


def fold_blocks(query_wide, state, stack, keys_wide, first, count, seen=None):
    def block(i, carry):
        run = partial(fold, query_wide, state, stack, keys_wide, i)
        if seen is None:
            run()
        else:
            pl.when(seen(i))(run)
        return carry

    lax.fori_loop(first, first + count, block, 0)


def load_blocks(stack, keys_wide, parts):
    at = 0
    for part in parts:
        stack[at : at + part.shape[0], :] = part[...]
        at += part.shape[0]
    for piece in range(at // PIECE):
        row, at = piece * KEYS, piece * PIECE
        for half in range(KEYS // HD):
            keys_wide[row + half * HD : row + (half + 1) * HD, 0:HD] = stack[
                at + HD : at + 2 * HD, half * HD : (half + 1) * HD
            ]
        gates = stack[at + KEYS : at + PIECE, :].astype(jnp.float32)
        rest = jnp.zeros((HD - GATE_ROWS, KEYS), jnp.float32)
        columns = jnp.transpose(jnp.concatenate([gates, rest], axis=0))
        keys_wide[row : row + KEYS, HD : 2 * HD] = columns.astype(jnp.bfloat16)


def load_query(query_wide, pack):
    query_wide[0:PACK, :] = pack[...]
    query_wide[PACK : 2 * HD, :] = jnp.zeros((2 * HD - PACK, pack.shape[1]), jnp.bfloat16)


def pack_result(state, out):
    run_max, run_sum, run_acc = state
    total = jnp.sum(run_sum[...], axis=0, keepdims=True)
    out[0:HD, :] = (run_acc[...] / total).astype(jnp.bfloat16)
    row = lax.broadcasted_iota(jnp.int32, (GATE_ROWS, total.shape[1]), 0)
    block = jnp.zeros(row.shape, jnp.float32)
    for at, part in enumerate(three_parts(run_max[0:1, :]) + three_parts(total)):
        block = jnp.where(row == at, part.astype(jnp.float32), block)
    out[HD:PACK, :] = block.astype(jnp.bfloat16)


def near_kernel(*refs):
    packs, keys, states = refs[:3], refs[3:6], refs[6:9]
    stack, keys_wide, query_wide = refs[9:]
    own_y = lax.axis_index("sp") >> 2

    @pl.when(own_y < 3)
    def _():
        load_blocks(stack, keys_wide, keys)

    def each(i, carry):
        @pl.when(own_y <= i)
        def _():
            for at, pack in enumerate(packs):
                pl.when(i == at)(partial(load_query, query_wide, pack))
            state = nth_state(states, i)
            clear(state)
            fold_blocks(query_wide, state, stack, keys_wide, 0, 3)

        return carry

    lax.fori_loop(0, 3, each, 0)


def end_kernel(*refs, first, count):
    packs, far, states = refs[:count], refs[count : count + 2], refs[count + 2 : count + 5]
    outs = refs[count + 5 : 2 * count + 5]
    state, (stack, keys_wide, query_wide) = refs[-6:-3], refs[-3:]
    own_y = lax.axis_index("sp") >> 2

    @pl.when(own_y < first + count)
    def _():
        load_blocks(stack, keys_wide, far)

    def each(i, carry):
        @pl.when(own_y <= first + i)
        def _():
            for into, came in zip(state, nth_state(states, first + i)):
                into[...] = came[...]
            for at, pack in enumerate(packs):
                pl.when(i == at)(partial(load_query, query_wide, pack))
            fold(query_wide, state, stack, keys_wide, 0)
            for at, out in enumerate(outs):
                pl.when(i == at)(partial(pack_result, state, out))

        return carry

    lax.fori_loop(0, count, each, 0)


def own_kernel(*refs):
    pack, keys, state = refs[0], refs[1:6], refs[6:9]
    stack, keys_wide, query_wide = refs[9:]
    own_x = lax.axis_index("sp") & 3
    load_blocks(stack, keys_wide, keys)
    load_query(query_wide, pack)
    clear(state)
    fold(query_wide, state, stack, keys_wide, 0, own_block=True)

    def seen(i):
        move = jnp.where(i == 1, -1, jnp.where(i == 2, 1, 2))
        return ((own_x + move) & 3) < own_x

    fold_blocks(query_wide, state, stack, keys_wide, 1, 3, seen)


def merge_kernel(*refs):
    came, own_state, gain, head_out = refs[:3], refs[3:6], refs[6], refs[7]
    own_y = lax.axis_index("sp") >> 2
    scale = HD ** (-0.5) * LOG2E
    peaks = [own_state[0][0:1, :]]
    totals = [jnp.sum(own_state[1][...], axis=0, keepdims=True)]
    for above, pack in enumerate(came):
        rows = pack[HD:PACK, :].astype(jnp.float32)
        parts = [rows[at : at + 1, :] for at in range(6)]
        valid = own_y > above
        peaks.append(jnp.where(valid, parts[0] + parts[1] + parts[2], low_score))
        totals.append(jnp.where(valid, parts[3] + parts[4] + parts[5], 0.0))
    top = peaks[0]
    for peak in peaks[1:]:
        top = jnp.maximum(top, peak)
    weight = jnp.exp2((peaks[0] - top) * scale)
    total = totals[0] * weight
    acc = own_state[2][...] * weight
    for pack, peak, share in zip(came, peaks[1:], totals[1:]):
        weight = share * jnp.exp2((peak - top) * scale)
        total = total + weight
        acc = acc + pack[0:HD, :].astype(jnp.float32) * weight
    attended = acc / total
    mean_square = jnp.mean(attended * attended, axis=0, keepdims=True)
    normed = jnp.transpose(attended * lax.rsqrt(mean_square + 1e-06))
    head_out[...] = (normed * gain[...]).astype(jnp.bfloat16)


def attend(kernel, operands, outs, scratch, folds):
    tok_count = 2 * KEYS
    return pl.pallas_call(
        kernel,
        out_shape=tuple(jax.ShapeDtypeStruct(*out) for out in outs),
        in_specs=[vmem] * len(operands),
        out_specs=(vmem,) * len(outs),
        scratch_shapes=[pltpu.VMEM(*shape) for shape in scratch],
        compiler_params=pltpu.CompilerParams(vmem_limit_bytes=12 << 20),
        cost_estimate=pl.CostEstimate(
            flops=8 * tok_count * tok_count * HD * folds,
            transcendentals=tok_count * tok_count * folds,
            bytes_accessed=1 << 20,
        ),
    )(*operands)


def attention(queries, key_vectors, value_vectors, forget_totals, head_gain, weights):
    tok_count = queries.shape[0]

    def shift(array, dy, dx, needed):
        return lax.ppermute(array, "sp", sp_perm(dy, dx, needed))

    keys_own, own_pack = make_pieces(queries, key_vectors, value_vectors, forget_totals)
    low = shift(keys_own, 0, 1, lambda y, x: y < 3 or x > 0)
    high = shift(keys_own, 0, -1, lambda y, x: y < 3 or x in (0, 3))
    pack3 = shift(own_pack, 1, 0, lambda y, x: y == 0)
    pack2 = shift(own_pack, 2, 0, lambda y, x: y < 2)
    pack1 = shift(own_pack, -1, 0, lambda y, x: y < 3)
    far_a = shift(low[:PIECE], 0, 1, lambda y, x: y < 3 or x > 1)
    far_b = shift(high[PIECE:], 0, -1, lambda y, x: y < 3 or x > 1)

    narrow = ((8, tok_count), jnp.float32)
    state = [narrow, narrow, ((HD, tok_count), jnp.float32)]
    all_states = [((3 * shape[0], tok_count), kind) for shape, kind in state]
    result = ((PACK, tok_count), jnp.bfloat16)

    def loaded(count):
        shapes = (count * BLOCK, 2 * HD), (count * 2 * KEYS, 2 * HD), (2 * HD, tok_count)
        return [(shape, jnp.bfloat16) for shape in shapes]

    packs = [pack3, pack2, pack1]
    near = attend(near_kernel, [*packs, keys_own, low, high], all_states, loaded(3), 9)

    def end(first, count):
        operands = [*packs[first : first + count], far_a, far_b, *near]
        kernel = partial(end_kernel, first=first, count=count)
        return attend(kernel, operands, [result] * count, state + loaded(1), count)

    part3, part2 = end(0, 2)
    part3, part2, near = lax.optimization_barrier((part3, part2, near))
    back3 = shift(part3, -1, 0, lambda y, x: y == 3)
    back2 = shift(part2, 2, 0, lambda y, x: y > 1)
    (part1,) = end(2, 1)
    keys = [keys_own, low, high, far_a, far_b]
    part1, own_pack, keys, weights = lax.optimization_barrier((part1, own_pack, keys, weights))
    back1 = shift(part1, 1, 0, lambda y, x: y > 0)
    own_state = attend(own_kernel, [own_pack, *keys], state, loaded(4), 4)
    staged = stage_weights(*weights)
    (head_out,) = attend(
        merge_kernel,
        [back1, back2, back3, *own_state, head_gain.reshape(1, HD)],
        [((tok_count, HD), jnp.bfloat16)],
        [],
        0,
    )
    return head_out, staged


def staging_kernel(gate, up, down, out, sems):
    tall, wide = gate.shape
    copies = [
        pltpu.make_async_copy(gate, out.at[pl.ds(0, tall)], sems.at[0]),
        pltpu.make_async_copy(up, out.at[pl.ds(tall, tall)], sems.at[1]),
    ]
    for i in range(down.shape[1] // wide):
        source = down.at[:, pl.ds(i * wide, wide)]
        into = out.at[pl.ds(2 * tall + i * down.shape[0], down.shape[0])]
        copies.append(pltpu.make_async_copy(source, into, sems.at[2 + i]))
    for copy in copies:
        copy.start()
    for copy in copies:
        copy.wait()


def stage_weights(gate, up, down):
    blocks = down.shape[1] // gate.shape[1]
    rows = 2 * gate.shape[0] + blocks * down.shape[0]
    return pl.pallas_call(
        staging_kernel,
        out_shape=jax.ShapeDtypeStruct((rows, gate.shape[1]), jnp.bfloat16),
        in_specs=[pl.BlockSpec(memory_space=pltpu.HBM)] * 3,
        out_specs=vmem,
        scratch_shapes=[pltpu.SemaphoreType.DMA((2 + blocks,))],
        compiler_params=pltpu.CompilerParams(vmem_limit_bytes=4 << 20),
        name="stage_weights",
    )(*in_hbm(gate, up, down))


def expert_kernel(*refs, count):
    rows, halves = refs[:count], refs[count : count + 2]
    outs = refs[count + 2 : 2 * count + 2]
    joined, made = refs[2 * count + 2 :]
    each, width = rows[0].shape
    units = halves[0].shape[1]
    for i, part in enumerate(rows):
        joined[i * each : (i + 1) * each, :] = part[...]
    tall = 128

    def block(i, carry):
        spot = pl.ds(pl.multiple_of(i * tall, tall), tall)
        mine = joined[spot, :]
        hidden = []
        for half in halves:
            gate_pre = jnp.dot(mine, half[0:width, :], preferred_element_type=jnp.float32)
            up_pre = jnp.dot(mine, half[width : 2 * width, :], preferred_element_type=jnp.float32)
            silu = gate_pre / (1.0 + jnp.exp(-gate_pre))
            hidden.append((silu * up_pre).astype(jnp.bfloat16))
        for col in range(0, width, units):
            at = 2 * width + col
            part = jnp.dot(
                hidden[0], halves[0][at : at + units, :], preferred_element_type=jnp.float32
            ) + jnp.dot(
                hidden[1], halves[1][at : at + units, :], preferred_element_type=jnp.float32
            )
            made[spot, col : col + units] = part.astype(jnp.bfloat16)
        return carry

    lax.fori_loop(0, joined.shape[0] // tall, block, 0)
    for i, out in enumerate(outs):
        out[...] = made[i * each : (i + 1) * each, :]


def expert_rows(rows, halves):
    count = len(rows)
    each, width = rows[0].shape
    flops = 2 * count * each * width * halves[0].shape[1] * 2 * 3
    joined = pltpu.VMEM((count * each, width), jnp.bfloat16)
    return pl.pallas_call(
        partial(expert_kernel, count=count),
        out_shape=tuple(jax.ShapeDtypeStruct((each, width), jnp.bfloat16) for _ in rows),
        in_specs=[vmem] * (count + 2),
        out_specs=(vmem,) * count,
        scratch_shapes=[joined, joined],
        compiler_params=pltpu.CompilerParams(vmem_limit_bytes=16 << 20),
        cost_estimate=pl.CostEstimate(flops=flops, transcendentals=0, bytes_accessed=6 << 20),
    )(*rows, *halves)


def added(left, right):
    return (left.astype(jnp.float32) + right.astype(jnp.float32)).astype(jnp.bfloat16)


def expert_sum(own, weights):
    def up(array):
        return lax.ppermute(array, "tp", z_perm(1))

    def down(array):
        return lax.ppermute(array, "tp", z_perm(-1))

    half = own.shape[0] // 2
    top, end = own[:half], own[half:]
    up_top, down_end, up_end, down_top = [top], [end], [end], [top]
    for _ in range(1, 4):
        up_top.append(up(up_top[-1]))
        down_end.append(down(down_end[-1]))
        up_end.append(up(up_end[-1]))
        down_top.append(down(down_top[-1]))
    up_top.append(up(up_top[-1]))
    down_end.append(down(down_end[-1]))
    chains = (up_top, up_end, down_top, down_end)
    made = []
    for i in range(1, 4):
        rows = [chain[i] for chain in chains]
        made.append(expert_rows(([top, end] if i == 1 else []) + rows, weights))
    mine, done = made[0][:2], [made[0][2:], made[1], made[2]]
    far_top, far_end = expert_rows([up_top[4], down_end[4]], weights)

    low_top, high_end = down(done[2][0]), up(done[2][3])
    high_top, low_end = up(far_top), down(far_end)
    high_top = up(added(high_top, done[2][2]))
    low_end = down(added(low_end, done[2][1]))
    for i in (1, 0):
        low_top = down(added(low_top, done[i][0]))
        high_end = up(added(high_end, done[i][3]))
        high_top = up(added(high_top, done[i][2]))
        low_end = down(added(low_end, done[i][1]))
    sums = []
    for parts in ((low_top, high_top, mine[0]), (low_end, high_end, mine[1])):
        low, high, own_part = (part.astype(jnp.float32) for part in parts)
        sums.append((low + high + own_part).astype(jnp.bfloat16))
    return jnp.concatenate(sums)


def place_rows(routing, slot_count, capacity):
    expert_count, row_count = slot_count // capacity, routing.shape[1]
    expert_id = lax.broadcasted_iota(jnp.int32, (expert_count, row_count), 0)
    chosen = [(routing[k : k + 1, :] == expert_id).astype(jnp.float32) for k in range(TOP)]
    before = lax.broadcasted_iota(jnp.int32, (row_count, row_count), 0)
    before = before < lax.broadcasted_iota(jnp.int32, (row_count, row_count), 1)
    before = before.astype(jnp.float32).astype(jnp.bfloat16)
    counts = jnp.dot(
        sum(chosen).astype(jnp.bfloat16), before, preferred_element_type=jnp.float32
    )
    slot_id = lax.broadcasted_iota(jnp.int32, (slot_count, row_count), 0)
    here = []
    for k in range(TOP):
        rank = jnp.sum(counts * chosen[k], axis=0, keepdims=True).astype(jnp.int32)
        here.append(slot_id == routing[k : k + 1, :] * capacity + rank)
    return here


def project_kernel(
    heads, out_weight, stream, norm_gain, routing, route_weights, resid_sum, outgoing, mixing, joined
):
    for head in range(heads.shape[0]):
        joined[:, head * HD : (head + 1) * HD] = heads[head]
    slot_count = mixing.shape[0]
    experts = slot_count // max(2, 2 * TOP * stream.shape[0] // lax.axis_size("sp"))
    here = place_rows(routing[...], slot_count, slot_count // experts)
    mix = jnp.zeros(mixing.shape, jnp.float32)
    place = jnp.zeros(mixing.shape, jnp.float32)
    for k in range(TOP):
        mix = jnp.where(here[k], route_weights[k : k + 1, :], mix)
        place = jnp.where(here[k], 1.0, place)
    mixing[...] = mix
    wide = 512

    def column(j, carry):
        cols = pl.ds(pl.multiple_of(j * wide, wide), wide)
        mixed_rows = jnp.dot(joined[...], out_weight[:, cols], preferred_element_type=jnp.float32)
        resid_sum[:, cols] = stream[:, cols].astype(jnp.float32) + mixed_rows
        return carry

    lax.fori_loop(0, resid_sum.shape[1] // wide, column, 0)
    resid = resid_sum[...]
    center = resid - jnp.mean(resid, axis=1, keepdims=True)
    spread = jnp.mean(center * center, axis=1, keepdims=True)
    normed = (center * lax.rsqrt(spread + 1e-05) * norm_gain[...]).astype(jnp.bfloat16)
    outgoing[...] = jnp.dot(
        place.astype(jnp.bfloat16), normed, preferred_element_type=jnp.float32
    ).astype(jnp.bfloat16)


def project(heads, out_weight, stream, norm_gain, routing, route_weights, slot_count):
    rows, width = stream.shape
    return pl.pallas_call(
        project_kernel,
        out_shape=(
            jax.ShapeDtypeStruct((rows, width), jnp.float32),
            jax.ShapeDtypeStruct((slot_count, width), jnp.bfloat16),
            jax.ShapeDtypeStruct((slot_count, rows), jnp.float32),
        ),
        in_specs=[vmem] * 6,
        out_specs=(vmem,) * 3,
        scratch_shapes=[pltpu.VMEM((rows, heads.shape[0] * HD), jnp.bfloat16)],
        compiler_params=pltpu.CompilerParams(vmem_limit_bytes=14 << 20),
        name="project",
    )(
        heads,
        out_weight,
        stream,
        norm_gain.reshape(1, width),
        jnp.transpose(routing),
        jnp.transpose(route_weights),
    )


def combine_kernel(resid_sum, returned, mixing, out):
    total = resid_sum[...]
    for part in three_parts(mixing[...]):
        total = total + lax.dot_general(
            part, returned[...], (((0,), (0,)), ((), ())), preferred_element_type=jnp.float32
        )
    out[...] = total.astype(jnp.bfloat16)


def combine(resid_sum, returned, mixing):
    return pl.pallas_call(
        combine_kernel,
        out_shape=jax.ShapeDtypeStruct(resid_sum.shape, jnp.bfloat16),
        in_specs=[vmem] * 3,
        out_specs=vmem,
        compiler_params=pltpu.CompilerParams(vmem_limit_bytes=6 << 20),
        name="combine",
    )(resid_sum, returned, mixing)


def on_device(
    queries,
    key_vectors,
    value_vectors,
    forget_totals,
    head_gain,
    stream,
    out_weight,
    norm_gain,
    routing,
    route_weights,
    gate_weight,
    up_weight,
    down_weight,
):
    sp_count = lax.axis_size("sp")
    head_out, own_half = attention(
        queries,
        key_vectors,
        value_vectors,
        forget_totals,
        head_gain,
        (gate_weight[0], up_weight[0], down_weight[0]),
    )
    weights = own_half, lax.ppermute(own_half, "tp", core_swap)
    row_count, width = stream.shape
    capacity = max(2, 2 * TOP * row_count // sp_count)
    heads = head_out.reshape(-1, row_count, HD)
    heads = lax.all_to_all(heads, "tp", split_axis=0, concat_axis=0, tiled=True)
    resid_sum, outgoing, mixing = project(
        heads, out_weight, stream, norm_gain, routing, route_weights, sp_count * capacity
    )
    outgoing = outgoing.reshape(sp_count, capacity, width)
    arrived = lax.all_to_all(outgoing, "sp", split_axis=0, concat_axis=0, tiled=True)
    summed = expert_sum(arrived.reshape(-1, width), weights)
    expert_out = summed.reshape(sp_count, capacity, width)
    returned = lax.all_to_all(expert_out, "sp", split_axis=0, concat_axis=0, tiled=True)
    return combine(resid_sum, returned.reshape(-1, width), mixing)


def solution(mesh):
    in_specs = (
        P("sp", "tp"),
        P("sp", "tp"),
        P("sp", "tp"),
        P("sp", "tp"),
        P("tp"),
        P(("sp", "tp"), None),
        P(),
        P(),
        P(("sp", "tp"), None),
        P(("sp", "tp"), None),
        P("sp", None, "tp"),
        P("sp", None, "tp"),
        P("sp", "tp", None),
    )
    out_specs = P(("sp", "tp"), None)
    return jax.shard_map(
        on_device, mesh=mesh, in_specs=in_specs, out_specs=out_specs, check_vma=False
    )
```

```python
from functools import partial

import jax
import jax.numpy as jnp
from jax import lax
from jax.experimental import pallas as pl
from jax.experimental.pallas import tpu as pltpu
from jax.sharding import PartitionSpec as P


HD = 128
TOP = 2
LOG2E = 1.4426950408889634
low_score = -1e30
GATE_ROWS = 16
KEYS = 256
PIECE = KEYS + GATE_ROWS
BLOCK = 2 * PIECE
PACK = HD + GATE_ROWS


def sp_perm(dy, dx, needed):
    pairs = []
    for y in range(4):
        for x in range(4):
            into = (y + dy) % 4, (x + dx) % 4
            if needed(*into):
                pairs.append((y * 4 + x, into[0] * 4 + into[1]))
    return pairs


def z_perm(dz):
    return [(z * 2 + c, ((z + dz) % 8) * 2 + c) for z in range(8) for c in range(2)]


core_swap = [(i, i ^ 1) for i in range(16)]


vmem = pl.BlockSpec(memory_space=pltpu.VMEM)


def in_hbm(*arrays):
    return [pltpu.with_memory_space_constraint(array, pltpu.HBM) for array in arrays]


def three_parts(wide):
    first = wide.astype(jnp.bfloat16)
    rest = wide - first.astype(jnp.float32)
    second = rest.astype(jnp.bfloat16)
    third = (rest - second.astype(jnp.float32)).astype(jnp.bfloat16)
    return first, second, third


def piece_kernel(*refs):
    sources, outs, staged, sems = refs[:4], refs[4:6], refs[6:10], refs[10]
    copies = [
        pltpu.make_async_copy(source, into, sems.at[i])
        for i, (source, into) in enumerate(zip(sources, staged))
    ]
    for copy in copies:
        copy.start()
    for copy in copies:
        copy.wait()
    queries, keys, values, gates = staged
    keys_own, query_pack = outs
    stretched = gates[...] * HD**0.5
    tok_count = stretched.shape[1]
    row = lax.broadcasted_iota(jnp.int32, (GATE_ROWS, KEYS), 0)
    for i in range(2):
        at_row = i * PIECE
        rows = slice(i * KEYS, (i + 1) * KEYS)
        keys_own[at_row : at_row + HD, :] = jnp.transpose(values[rows, :])
        keys_own[at_row + HD : at_row + KEYS, 0:HD] = keys[i * KEYS : i * KEYS + HD, :]
        keys_own[at_row + HD : at_row + KEYS, HD:KEYS] = keys[i * KEYS + HD : (i + 1) * KEYS, :]
        parts = [part.astype(jnp.float32) for part in three_parts(-stretched[:, rows])]
        block = jnp.where((row >= 3) & (row < 6), 1.0, 0.0)
        for at, part in enumerate(parts):
            block = jnp.where(row == at, part, block)
        keys_own[at_row + KEYS : at_row + PIECE, :] = block.astype(jnp.bfloat16)
    wide_row = lax.broadcasted_iota(jnp.int32, (GATE_ROWS, tok_count), 0)
    mix = jnp.where(wide_row < 3, 1.0, 0.0)
    parts = [part.astype(jnp.float32) for part in three_parts(stretched[:, 0:1])]
    for at, part in enumerate(parts):
        mix = jnp.where(wide_row == 3 + at, part, mix)
    mix = jnp.where(wide_row == 6, low_score, mix)
    query_pack[HD:PACK, :] = mix.astype(jnp.bfloat16)
    query_pack[0:HD, :] = jnp.transpose(queries[...])


def make_pieces(queries, keys, values, gates):
    tok_count = queries.shape[0]
    return pl.pallas_call(
        piece_kernel,
        out_shape=(
            jax.ShapeDtypeStruct((BLOCK, 2 * HD), jnp.bfloat16),
            jax.ShapeDtypeStruct((PACK, tok_count), jnp.bfloat16),
        ),
        in_specs=[pl.BlockSpec(memory_space=pltpu.HBM)] * 4,
        out_specs=(vmem,) * 2,
        scratch_shapes=[pltpu.VMEM((tok_count, HD), jnp.bfloat16)] * 3
        + [pltpu.VMEM((1, tok_count), jnp.float32), pltpu.SemaphoreType.DMA((4,))],
        compiler_params=pltpu.CompilerParams(vmem_limit_bytes=6 << 20),
        name="make_pieces",
    )(*in_hbm(queries, keys, values, gates.reshape(1, tok_count)))


def fold(query_wide, state, stack, keys_wide, block, own_block=False):
    run_max, run_sum, run_acc = state
    tok_count = query_wide.shape[1]
    scale = HD ** (-0.5) * LOG2E
    scores = []
    for part in range(2 * KEYS // HD):
        spot = pl.ds(pl.multiple_of(block * (2 * KEYS) + part * HD, HD), HD)
        score = jnp.dot(
            keys_wide[spot, :], query_wide[...], preferred_element_type=jnp.float32
        )
        if own_block:
            key_at = lax.broadcasted_iota(jnp.int32, score.shape, 0) + part * HD
            query_at = lax.broadcasted_iota(jnp.int32, score.shape, 1)
            score = jnp.where(key_at <= query_at, score, low_score)
        scores.append(score)
    old_max = run_max[0:1, :]
    peak = scores[0]
    for score in scores[1:]:
        peak = jnp.maximum(peak, score)
    new_max = jnp.maximum(old_max, jnp.max(peak, axis=0, keepdims=True))
    rescale = jnp.exp2((old_max - new_max) * scale)
    scaled_max = new_max * scale
    total = run_sum[...] * rescale
    acc = run_acc[...] * rescale
    for i in range(2):
        at = pl.multiple_of(block * BLOCK + i * PIECE, GATE_ROWS)
        rounded = []
        for score in scores[2 * i : 2 * i + 2]:
            lifted = jnp.exp2(score * scale - scaled_max)
            total = total + jnp.sum(lifted.reshape(HD // 8, 8, tok_count), axis=0)
            rounded.append(lifted.astype(jnp.bfloat16))
        acc = acc + jnp.dot(
            stack[pl.ds(at, HD), :],
            jnp.concatenate(rounded, axis=0),
            preferred_element_type=jnp.float32,
        )
    run_sum[...] = total
    run_acc[...] = acc
    run_max[...] = jnp.broadcast_to(new_max, run_max.shape)


def clear(state):
    run_max, run_sum, run_acc = state
    run_max[...] = jnp.full(run_max.shape, low_score, jnp.float32)
    run_sum[...] = jnp.zeros(run_sum.shape, jnp.float32)
    run_acc[...] = jnp.zeros(run_acc.shape, jnp.float32)


def nth_state(state, i):
    found = []
    for ref in state:
        rows = ref.shape[0] // 3
        found.append(ref.at[pl.ds(pl.multiple_of(i * rows, 8), rows)])
    return found


def fold_blocks(query_wide, state, stack, keys_wide, first, count, seen=None):
    def block(i, carry):
        run = partial(fold, query_wide, state, stack, keys_wide, i)
        if seen is None:
            run()
        else:
            pl.when(seen(i))(run)
        return carry

    lax.fori_loop(first, first + count, block, 0)


def load_blocks(stack, keys_wide, parts):
    at = 0
    for part in parts:
        stack[at : at + part.shape[0], :] = part[...]
        at += part.shape[0]
    for piece in range(at // PIECE):
        row, at = piece * KEYS, piece * PIECE
        for half in range(KEYS // HD):
            keys_wide[row + half * HD : row + (half + 1) * HD, 0:HD] = stack[
                at + HD : at + 2 * HD, half * HD : (half + 1) * HD
            ]
        gates = stack[at + KEYS : at + PIECE, :].astype(jnp.float32)
        rest = jnp.zeros((HD - GATE_ROWS, KEYS), jnp.float32)
        columns = jnp.transpose(jnp.concatenate([gates, rest], axis=0))
        keys_wide[row : row + KEYS, HD : 2 * HD] = columns.astype(jnp.bfloat16)


def load_query(query_wide, pack):
    query_wide[0:PACK, :] = pack[...]
    query_wide[PACK : 2 * HD, :] = jnp.zeros((2 * HD - PACK, pack.shape[1]), jnp.bfloat16)


def pack_result(state, out):
    run_max, run_sum, run_acc = state
    total = jnp.sum(run_sum[...], axis=0, keepdims=True)
    out[0:HD, :] = (run_acc[...] / total).astype(jnp.bfloat16)
    row = lax.broadcasted_iota(jnp.int32, (GATE_ROWS, total.shape[1]), 0)
    block = jnp.zeros(row.shape, jnp.float32)
    for at, part in enumerate(three_parts(run_max[0:1, :]) + three_parts(total)):
        block = jnp.where(row == at, part.astype(jnp.float32), block)
    out[HD:PACK, :] = block.astype(jnp.bfloat16)


def near_kernel(*refs):
    packs, keys, states = refs[:3], refs[3:6], refs[6:9]
    stack, keys_wide, query_wide = refs[9:]
    own_y = lax.axis_index("sp") >> 2

    @pl.when(own_y < 3)
    def _():
        load_blocks(stack, keys_wide, keys)

    def each(i, carry):
        @pl.when(own_y <= i)
        def _():
            for at, pack in enumerate(packs):
                pl.when(i == at)(partial(load_query, query_wide, pack))
            state = nth_state(states, i)
            clear(state)
            fold_blocks(query_wide, state, stack, keys_wide, 0, 3)

        return carry

    lax.fori_loop(0, 3, each, 0)


def end_kernel(*refs):
    packs, far, states, outs = refs[:3], refs[3:5], refs[5:8], refs[8:11]
    state, (stack, keys_wide, query_wide) = refs[11:14], refs[14:]
    own_y = lax.axis_index("sp") >> 2

    @pl.when(own_y < 3)
    def _():
        load_blocks(stack, keys_wide, far)

    def each(i, carry):
        @pl.when(own_y <= i)
        def _():
            for into, came in zip(state, nth_state(states, i)):
                into[...] = came[...]
            for at, pack in enumerate(packs):
                pl.when(i == at)(partial(load_query, query_wide, pack))
            fold(query_wide, state, stack, keys_wide, 0)
            for at, out in enumerate(outs):
                pl.when(i == at)(partial(pack_result, state, out))

        return carry

    lax.fori_loop(0, 3, each, 0)


def own_kernel(*refs):
    pack, keys, state = refs[0], refs[1:6], refs[6:9]
    stack, keys_wide, query_wide = refs[9:]
    own_x = lax.axis_index("sp") & 3
    load_blocks(stack, keys_wide, keys)
    load_query(query_wide, pack)
    clear(state)
    fold(query_wide, state, stack, keys_wide, 0, own_block=True)

    def seen(i):
        move = jnp.where(i == 1, -1, jnp.where(i == 2, 1, 2))
        return ((own_x + move) & 3) < own_x

    fold_blocks(query_wide, state, stack, keys_wide, 1, 3, seen)


def merge_kernel(*refs):
    came, own_state, gain, head_out = refs[:3], refs[3:6], refs[6], refs[7]
    own_y = lax.axis_index("sp") >> 2
    scale = HD ** (-0.5) * LOG2E
    peaks = [own_state[0][0:1, :]]
    totals = [jnp.sum(own_state[1][...], axis=0, keepdims=True)]
    for above, pack in enumerate(came):
        rows = pack[HD:PACK, :].astype(jnp.float32)
        parts = [rows[at : at + 1, :] for at in range(6)]
        valid = own_y > above
        peaks.append(jnp.where(valid, parts[0] + parts[1] + parts[2], low_score))
        totals.append(jnp.where(valid, parts[3] + parts[4] + parts[5], 0.0))
    top = peaks[0]
    for peak in peaks[1:]:
        top = jnp.maximum(top, peak)
    weight = jnp.exp2((peaks[0] - top) * scale)
    total = totals[0] * weight
    acc = own_state[2][...] * weight
    for pack, peak, share in zip(came, peaks[1:], totals[1:]):
        weight = share * jnp.exp2((peak - top) * scale)
        total = total + weight
        acc = acc + pack[0:HD, :].astype(jnp.float32) * weight
    attended = acc / total
    mean_square = jnp.mean(attended * attended, axis=0, keepdims=True)
    normed = jnp.transpose(attended * lax.rsqrt(mean_square + 1e-06))
    head_out[...] = (normed * gain[...]).astype(jnp.bfloat16)


def attend(kernel, operands, outs, scratch, folds):
    tok_count = 2 * KEYS
    return pl.pallas_call(
        kernel,
        out_shape=tuple(jax.ShapeDtypeStruct(*out) for out in outs),
        in_specs=[vmem] * len(operands),
        out_specs=(vmem,) * len(outs),
        scratch_shapes=[pltpu.VMEM(*shape) for shape in scratch],
        compiler_params=pltpu.CompilerParams(vmem_limit_bytes=12 << 20),
        cost_estimate=pl.CostEstimate(
            flops=8 * tok_count * tok_count * HD * folds,
            transcendentals=tok_count * tok_count * folds,
            bytes_accessed=1 << 20,
        ),
    )(*operands)


def attention(queries, key_vectors, value_vectors, forget_totals, head_gain, weights):
    tok_count = queries.shape[0]

    def shift(array, dy, dx, needed):
        return lax.ppermute(array, "sp", sp_perm(dy, dx, needed))

    keys_own, own_pack = make_pieces(queries, key_vectors, value_vectors, forget_totals)
    low = shift(keys_own, 0, 1, lambda y, x: y < 3 or x > 0)
    high = shift(keys_own, 0, -1, lambda y, x: y < 3 or x in (0, 3))
    pack3 = shift(own_pack, 1, 0, lambda y, x: y == 0)
    pack2 = shift(own_pack, 2, 0, lambda y, x: y < 2)
    pack1 = shift(own_pack, -1, 0, lambda y, x: y < 3)
    far_a = shift(low[:PIECE], 0, 1, lambda y, x: y < 3 or x > 1)
    far_b = shift(high[PIECE:], 0, -1, lambda y, x: y < 3 or x > 1)

    narrow = ((8, tok_count), jnp.float32)
    state = [narrow, narrow, ((HD, tok_count), jnp.float32)]
    all_states = [((3 * shape[0], tok_count), kind) for shape, kind in state]
    result = ((PACK, tok_count), jnp.bfloat16)

    def loaded(count):
        shapes = (count * BLOCK, 2 * HD), (count * 2 * KEYS, 2 * HD), (2 * HD, tok_count)
        return [(shape, jnp.bfloat16) for shape in shapes]

    packs = [pack3, pack2, pack1]
    near = attend(near_kernel, [*packs, keys_own, low, high], all_states, loaded(3), 9)
    part3, part2, part1 = attend(
        end_kernel, [*packs, far_a, far_b, *near], [result] * 3, state + loaded(1), 3
    )
    keys = [keys_own, low, high, far_a, far_b]
    part3, part2, part1, own_pack, keys, weights = lax.optimization_barrier(
        (part3, part2, part1, own_pack, keys, weights)
    )
    back3 = shift(part3, -1, 0, lambda y, x: y == 3)
    back2 = shift(part2, 2, 0, lambda y, x: y > 1)
    back1 = shift(part1, 1, 0, lambda y, x: y > 0)
    own_state = attend(own_kernel, [own_pack, *keys], state, loaded(4), 4)
    staged = stage_weights(*weights)
    (head_out,) = attend(
        merge_kernel,
        [back1, back2, back3, *own_state, head_gain.reshape(1, HD)],
        [((tok_count, HD), jnp.bfloat16)],
        [],
        0,
    )
    return head_out, staged


def staging_kernel(gate, up, down, out, sems):
    tall, wide = gate.shape
    copies = [
        pltpu.make_async_copy(gate, out.at[pl.ds(0, tall)], sems.at[0]),
        pltpu.make_async_copy(up, out.at[pl.ds(tall, tall)], sems.at[1]),
    ]
    for i in range(down.shape[1] // wide):
        source = down.at[:, pl.ds(i * wide, wide)]
        into = out.at[pl.ds(2 * tall + i * down.shape[0], down.shape[0])]
        copies.append(pltpu.make_async_copy(source, into, sems.at[2 + i]))
    for copy in copies:
        copy.start()
    for copy in copies:
        copy.wait()


def stage_weights(gate, up, down):
    blocks = down.shape[1] // gate.shape[1]
    rows = 2 * gate.shape[0] + blocks * down.shape[0]
    return pl.pallas_call(
        staging_kernel,
        out_shape=jax.ShapeDtypeStruct((rows, gate.shape[1]), jnp.bfloat16),
        in_specs=[pl.BlockSpec(memory_space=pltpu.HBM)] * 3,
        out_specs=vmem,
        scratch_shapes=[pltpu.SemaphoreType.DMA((2 + blocks,))],
        compiler_params=pltpu.CompilerParams(vmem_limit_bytes=4 << 20),
        name="stage_weights",
    )(*in_hbm(gate, up, down))


def expert_kernel(*refs, count):
    rows, halves = refs[:count], refs[count : count + 2]
    outs = refs[count + 2 : 2 * count + 2]
    joined, made = refs[2 * count + 2 :]
    each, width = rows[0].shape
    units = halves[0].shape[1]
    for i, part in enumerate(rows):
        joined[i * each : (i + 1) * each, :] = part[...]
    tall = 128

    def block(i, carry):
        spot = pl.ds(pl.multiple_of(i * tall, tall), tall)
        mine = joined[spot, :]
        hidden = []
        for half in halves:
            gate_pre = jnp.dot(mine, half[0:width, :], preferred_element_type=jnp.float32)
            up_pre = jnp.dot(mine, half[width : 2 * width, :], preferred_element_type=jnp.float32)
            silu = gate_pre / (1.0 + jnp.exp(-gate_pre))
            hidden.append((silu * up_pre).astype(jnp.bfloat16))
        for col in range(0, width, units):
            at = 2 * width + col
            part = jnp.dot(
                hidden[0], halves[0][at : at + units, :], preferred_element_type=jnp.float32
            ) + jnp.dot(
                hidden[1], halves[1][at : at + units, :], preferred_element_type=jnp.float32
            )
            made[spot, col : col + units] = part.astype(jnp.bfloat16)
        return carry

    lax.fori_loop(0, joined.shape[0] // tall, block, 0)
    for i, out in enumerate(outs):
        out[...] = made[i * each : (i + 1) * each, :]


def expert_rows(rows, halves):
    count = len(rows)
    each, width = rows[0].shape
    flops = 2 * count * each * width * halves[0].shape[1] * 2 * 3
    joined = pltpu.VMEM((count * each, width), jnp.bfloat16)
    return pl.pallas_call(
        partial(expert_kernel, count=count),
        out_shape=tuple(jax.ShapeDtypeStruct((each, width), jnp.bfloat16) for _ in rows),
        in_specs=[vmem] * (count + 2),
        out_specs=(vmem,) * count,
        scratch_shapes=[joined, joined],
        compiler_params=pltpu.CompilerParams(vmem_limit_bytes=16 << 20),
        cost_estimate=pl.CostEstimate(flops=flops, transcendentals=0, bytes_accessed=6 << 20),
    )(*rows, *halves)


def added(left, right):
    return (left.astype(jnp.float32) + right.astype(jnp.float32)).astype(jnp.bfloat16)


def expert_sum(own, weights):
    def up(array):
        return lax.ppermute(array, "tp", z_perm(1))

    def down(array):
        return lax.ppermute(array, "tp", z_perm(-1))

    half = own.shape[0] // 2
    top, end = own[:half], own[half:]
    up_top, down_end, up_end, down_top = [top], [end], [end], [top]
    for _ in range(1, 4):
        up_top.append(up(up_top[-1]))
        down_end.append(down(down_end[-1]))
        up_end.append(up(up_end[-1]))
        down_top.append(down(down_top[-1]))
    up_top.append(up(up_top[-1]))
    down_end.append(down(down_end[-1]))
    chains = (up_top, up_end, down_top, down_end)
    made = []
    for i in range(1, 4):
        rows = [chain[i] for chain in chains]
        made.append(expert_rows(([top, end] if i == 1 else []) + rows, weights))
    mine, done = made[0][:2], [made[0][2:], made[1], made[2]]
    far_top, far_end = expert_rows([up_top[4], down_end[4]], weights)

    low_top, high_end = down(done[2][0]), up(done[2][3])
    high_top, low_end = up(far_top), down(far_end)
    high_top = up(added(high_top, done[2][2]))
    low_end = down(added(low_end, done[2][1]))
    for i in (1, 0):
        low_top = down(added(low_top, done[i][0]))
        high_end = up(added(high_end, done[i][3]))
        high_top = up(added(high_top, done[i][2]))
        low_end = down(added(low_end, done[i][1]))
    sums = []
    for parts in ((low_top, high_top, mine[0]), (low_end, high_end, mine[1])):
        low, high, own_part = (part.astype(jnp.float32) for part in parts)
        sums.append((low + high + own_part).astype(jnp.bfloat16))
    return jnp.concatenate(sums)


def place_rows(routing, slot_count, capacity):
    expert_count, row_count = slot_count // capacity, routing.shape[1]
    expert_id = lax.broadcasted_iota(jnp.int32, (expert_count, row_count), 0)
    chosen = [(routing[k : k + 1, :] == expert_id).astype(jnp.float32) for k in range(TOP)]
    before = lax.broadcasted_iota(jnp.int32, (row_count, row_count), 0)
    before = before < lax.broadcasted_iota(jnp.int32, (row_count, row_count), 1)
    before = before.astype(jnp.float32).astype(jnp.bfloat16)
    counts = jnp.dot(
        sum(chosen).astype(jnp.bfloat16), before, preferred_element_type=jnp.float32
    )
    slot_id = lax.broadcasted_iota(jnp.int32, (slot_count, row_count), 0)
    here = []
    for k in range(TOP):
        rank = jnp.sum(counts * chosen[k], axis=0, keepdims=True).astype(jnp.int32)
        here.append(slot_id == routing[k : k + 1, :] * capacity + rank)
    return here


def project_kernel(
    heads, out_weight, stream, norm_gain, routing, route_weights, resid_sum, outgoing, mixing, joined
):
    for head in range(heads.shape[0]):
        joined[:, head * HD : (head + 1) * HD] = heads[head]
    slot_count = mixing.shape[0]
    experts = slot_count // max(2, 2 * TOP * stream.shape[0] // lax.axis_size("sp"))
    here = place_rows(routing[...], slot_count, slot_count // experts)
    mix = jnp.zeros(mixing.shape, jnp.float32)
    place = jnp.zeros(mixing.shape, jnp.float32)
    for k in range(TOP):
        mix = jnp.where(here[k], route_weights[k : k + 1, :], mix)
        place = jnp.where(here[k], 1.0, place)
    mixing[...] = mix
    wide = 512

    def column(j, carry):
        cols = pl.ds(pl.multiple_of(j * wide, wide), wide)
        mixed_rows = jnp.dot(joined[...], out_weight[:, cols], preferred_element_type=jnp.float32)
        resid_sum[:, cols] = stream[:, cols].astype(jnp.float32) + mixed_rows
        return carry

    lax.fori_loop(0, resid_sum.shape[1] // wide, column, 0)
    resid = resid_sum[...]
    center = resid - jnp.mean(resid, axis=1, keepdims=True)
    spread = jnp.mean(center * center, axis=1, keepdims=True)
    normed = (center * lax.rsqrt(spread + 1e-05) * norm_gain[...]).astype(jnp.bfloat16)
    outgoing[...] = jnp.dot(
        place.astype(jnp.bfloat16), normed, preferred_element_type=jnp.float32
    ).astype(jnp.bfloat16)


def project(heads, out_weight, stream, norm_gain, routing, route_weights, slot_count):
    rows, width = stream.shape
    return pl.pallas_call(
        project_kernel,
        out_shape=(
            jax.ShapeDtypeStruct((rows, width), jnp.float32),
            jax.ShapeDtypeStruct((slot_count, width), jnp.bfloat16),
            jax.ShapeDtypeStruct((slot_count, rows), jnp.float32),
        ),
        in_specs=[vmem] * 6,
        out_specs=(vmem,) * 3,
        scratch_shapes=[pltpu.VMEM((rows, heads.shape[0] * HD), jnp.bfloat16)],
        compiler_params=pltpu.CompilerParams(vmem_limit_bytes=14 << 20),
        name="project",
    )(
        heads,
        out_weight,
        stream,
        norm_gain.reshape(1, width),
        jnp.transpose(routing),
        jnp.transpose(route_weights),
    )


def combine_kernel(resid_sum, returned, mixing, out):
    total = resid_sum[...]
    for part in three_parts(mixing[...]):
        total = total + lax.dot_general(
            part, returned[...], (((0,), (0,)), ((), ())), preferred_element_type=jnp.float32
        )
    out[...] = total.astype(jnp.bfloat16)


def combine(resid_sum, returned, mixing):
    return pl.pallas_call(
        combine_kernel,
        out_shape=jax.ShapeDtypeStruct(resid_sum.shape, jnp.bfloat16),
        in_specs=[vmem] * 3,
        out_specs=vmem,
        compiler_params=pltpu.CompilerParams(vmem_limit_bytes=6 << 20),
        name="combine",
    )(resid_sum, returned, mixing)


def on_device(
    queries,
    key_vectors,
    value_vectors,
    forget_totals,
    head_gain,
    stream,
    out_weight,
    norm_gain,
    routing,
    route_weights,
    gate_weight,
    up_weight,
    down_weight,
):
    sp_count = lax.axis_size("sp")
    head_out, own_half = attention(
        queries,
        key_vectors,
        value_vectors,
        forget_totals,
        head_gain,
        (gate_weight[0], up_weight[0], down_weight[0]),
    )
    weights = own_half, lax.ppermute(own_half, "tp", core_swap)
    row_count, width = stream.shape
    capacity = max(2, 2 * TOP * row_count // sp_count)
    heads = head_out.reshape(-1, row_count, HD)
    heads = lax.all_to_all(heads, "tp", split_axis=0, concat_axis=0, tiled=True)
    resid_sum, outgoing, mixing = project(
        heads, out_weight, stream, norm_gain, routing, route_weights, sp_count * capacity
    )
    outgoing = outgoing.reshape(sp_count, capacity, width)
    arrived = lax.all_to_all(outgoing, "sp", split_axis=0, concat_axis=0, tiled=True)
    summed = expert_sum(arrived.reshape(-1, width), weights)
    expert_out = summed.reshape(sp_count, capacity, width)
    returned = lax.all_to_all(expert_out, "sp", split_axis=0, concat_axis=0, tiled=True)
    return combine(resid_sum, returned.reshape(-1, width), mixing)


def solution(mesh):
    in_specs = (
        P("sp", "tp"),
        P("sp", "tp"),
        P("sp", "tp"),
        P("sp", "tp"),
        P("tp"),
        P(("sp", "tp"), None),
        P(),
        P(),
        P(("sp", "tp"), None),
        P(("sp", "tp"), None),
        P("sp", None, "tp"),
        P("sp", None, "tp"),
        P("sp", "tp", None),
    )
    out_specs = P(("sp", "tp"), None)
    return jax.shard_map(
        on_device, mesh=mesh, in_specs=in_specs, out_specs=out_specs, check_vma=False
    )
```
